32 devices in a mesh: fs: 4 (over z), tp: 8 (over y, x, core).
Axes of the slice: x: 2, y: 2, z: 4, core: 2. Of those that a mesh axis runs over, the one named last changes fastest.
Arguments:
- tokens: bfloat16 [1024, 1344], P('fs'), may hold values from -6 to 6
- cotangent: bfloat16 [1024, 1344], P('fs'), may hold values from -8 to 8
- gate_weight: bfloat16 [1344, 3072], P('fs', 'tp'), may hold values from -0.15625 to 0.15625
- up_weight: bfloat16 [1344, 3072], P('fs', 'tp'), may hold values from -0.15625 to 0.15625
- down_weight: bfloat16 [3072, 1344], P('tp', 'fs'), may hold values from -0.109375 to 0.109375
Outputs:
- input_grad: bfloat16 [1024, 1344], P('fs')
- down_grad: float32 [3072, 1344], P('tp', 'fs')
The draws below stay inside these ranges and needn't reach their ends.
All inputs are finite; a program needn't handle non-finite values.
Results may differ from the reference program's by a relative error of at most 0.013.
Values may be sent and summed in bfloat16 or wider, within the bound.
A program may use at most 64 MiB of HBM per device.

```python
import jax
import jax.numpy as jnp
from jax import lax

D = 1344
FF = 3072
TOKENS = 1024
N_TP = 8


def with_spikes(values, key, source, target, blocks, factor):
    owner, partner = [(jnp.arange(values.shape[position]) // (values.shape[position] // blocks)).reshape([-1 if axis == position else 1 for axis in range(values.ndim)]) for position in (source, target)]
    chosen = jax.random.permutation(key, blocks)[partner]
    strong = (owner == chosen) | (owner == (partner + blocks // 2) % blocks)
    return jnp.where(strong, factor * values, values)


def steps_of(stream_key, dims, split, least, largest):
    factor_of, own = 1.0, jax.random.fold_in(stream_key, 6)
    for axis_at, blocks in split:
        heights = jnp.exp(jax.random.uniform(jax.random.fold_in(own, axis_at), (blocks,), jnp.float32, least / len(split), largest / len(split)))
        factor_of = factor_of * jnp.repeat(heights, dims[axis_at] // blocks).reshape([-1 if axis == axis_at else 1 for axis in range(len(dims))])
    return factor_of


def scatter_about(rng, shape, width, limit, split=(), held_as=jnp.bfloat16):
    level = steps_of(rng, shape, split, -0.22, 0.18) if split else 1.0
    values = jax.random.normal(rng, shape, jnp.float32) * width * level
    return jnp.minimum(jnp.maximum(values, -limit), limit).astype(held_as)


def bell_draw_with(key, extent, spread, limit, shards, heavy, dtype=jnp.bfloat16):
    result = spread * jax.random.normal(key, extent, jnp.float32)
    if shards:
        result = result * steps_of(key, extent, shards, -0.22, 0.18)
    return jnp.clip(with_spikes(result, jax.random.fold_in(key, 3), *heavy), -limit, limit).astype(dtype)


def setup_inputs(seed: int = 0) -> dict:
    streams_of = jax.random.split(jax.random.key(seed), 6)
    tokens = scatter_about(streams_of[0], (TOKENS, D), 1.0, 6.0, ((0, 4),))
    cotangent = bell_draw_with(streams_of[1], (TOKENS, D), 1.0, 8.0, ((0, 4),), (0, 1, 4, 2.0))
    gate_weight = scatter_about(streams_of[2], (D, FF), D ** -0.5, 0.15625, ((0, 4), (1, 8)))
    up_weight = scatter_about(streams_of[3], (D, FF), D ** -0.5, 0.15625, ((0, 4), (1, 8)))
    down_weight = scatter_about(streams_of[4], (FF, D), FF ** -0.5, 0.109375, ((0, 8), (1, 4)))
    return dict(tokens=tokens, cotangent=cotangent, gate_weight=gate_weight, up_weight=up_weight, down_weight=down_weight)


def contract_rows(left, right):
    return lax.dot_general(left, right, (((0,), (0,)), ((), ())), preferred_element_type=jnp.float32)


def contract_cols(left, right):
    return lax.dot_general(left, right, (((1,), (1,)), ((), ())), preferred_element_type=jnp.float32)


def reference(tokens, cotangent, gate_weight, up_weight, down_weight):
    gate_pre = jnp.dot(tokens, gate_weight, preferred_element_type=jnp.float32)
    up_pre = jnp.dot(tokens, up_weight, preferred_element_type=jnp.float32)
    sigmoid_gate = jax.nn.sigmoid(gate_pre)
    activated = gate_pre * sigmoid_gate
    hidden = (activated * up_pre).astype(jnp.bfloat16)
    hidden_grad = contract_cols(cotangent, down_weight)
    gate_pre_grad = (hidden_grad * up_pre * sigmoid_gate * (1.0 + gate_pre * (1.0 - sigmoid_gate))).astype(jnp.bfloat16)
    up_pre_grad = (hidden_grad * activated).astype(jnp.bfloat16)
    block_width = FF // N_TP
    summed = jnp.zeros(tokens.shape, jnp.float32)
    for member in range(N_TP):
        lower = member * block_width
        upper = lower + block_width
        partial_value = contract_cols(gate_pre_grad[:, lower:upper], gate_weight[:, lower:upper])
        partial_value = partial_value + contract_cols(up_pre_grad[:, lower:upper], up_weight[:, lower:upper])
        summed = summed + partial_value.astype(jnp.bfloat16).astype(jnp.float32)
    input_grad = summed.astype(jnp.bfloat16)
    down_grad = contract_rows(hidden, cotangent)
    return input_grad, down_grad
```

```python
import functools

import jax
import jax.numpy as jnp
from jax import lax
from jax.experimental import pallas as pl
from jax.experimental.pallas import tpu as pltpu
from jax.sharding import PartitionSpec as P

LANES = 128
SUB = 16
BF16 = jnp.bfloat16
F32 = jnp.float32


def contract_rows(left, right):
    return lax.dot_general(
        left, right, (((0,), (0,)), ((), ())), preferred_element_type=jnp.float32
    )


def contract_cols(left, right):
    return lax.dot_general(
        left, right, (((1,), (1,)), ((), ())), preferred_element_type=jnp.float32
    )


def send_down(hidden, cotangent):
    return lax.psum_scatter(
        contract_rows(cotangent, hidden), "fs", scatter_dimension=0, tiled=True
    ).T


def per_device_plain(tokens, cotangent, gate_weight, up_weight, down_weight):
    whole_gate, whole_up, whole_down = (
        lax.all_gather(gate_weight, "fs", axis=0, tiled=True),
        lax.all_gather(up_weight, "fs", axis=0, tiled=True),
        lax.all_gather(down_weight, "fs", axis=1, tiled=True),
    )
    gate_pre = jnp.dot(tokens, whole_gate, preferred_element_type=jnp.float32)
    up_pre = jnp.dot(tokens, whole_up, preferred_element_type=jnp.float32)
    hidden_grad = contract_cols(cotangent, whole_down)
    sigmoid_gate = jax.nn.sigmoid(gate_pre)
    activated = gate_pre * sigmoid_gate
    hidden = (activated * up_pre).astype(jnp.bfloat16)
    gate_pre_grad = (
        hidden_grad * up_pre * sigmoid_gate * (1.0 + gate_pre * (1.0 - sigmoid_gate))
    ).astype(jnp.bfloat16)
    up_pre_grad = (hidden_grad * activated).astype(jnp.bfloat16)
    partial_value = contract_cols(gate_pre_grad, whole_gate) + contract_cols(up_pre_grad, whole_up)
    input_grad = lax.psum(partial_value.astype(jnp.bfloat16), "tp")
    down_grad = send_down(hidden, cotangent)
    return (input_grad, down_grad)


def kernel(n, tok_ref, cot_ref, gate_ref, up_ref, down_ref, dx_out, dg_out,
           weights, tok, cot, ptok, pcot, dxacc, hid, dgp, dgs, dgr, dgf,
           t1s, t1r, t2s, t2r, t3s, t3r, ybuf,
           z_send, s_send, w_recv, loc_sem, tk_send, tk_recv, hid_send, hid_recv,
           dg_send, dg_recv, dgf_send, dgf_recv, t1_send, t1_recv, t2_send, t2_recv,
           t3_send, t3_recv, y_send, y_recv, yd_send, yd_recv):
    z = lax.axis_index("fs")
    b = lax.axis_index("tp")
    depth, rows = tok_ref.shape
    shard, ff = gate_ref.shape
    chunks = ff // LANES
    parts = t2s.shape[1]
    piece = shard // parts
    half_rows = rows // 2
    core = lax.rem(b, 2)
    col = lax.div(b, 2)
    cx = lax.rem(col, 2)
    cy = lax.div(col, 2)
    side = lax.div(z, 2)
    home = core == side
    away = core != side
    near = jnp.logical_or(z == 1, z == 2)
    end = jnp.logical_not(near)
    zodd = lax.rem(z, 2)
    sib = b + 1 - 2 * core
    bx = b + 2 * (1 - 2 * cx)
    by = b + 4 * (1 - 2 * cy)
    zs = z + 1 - 2 * zodd
    zp = lax.rem(z + 2, 4)
    zn = 2 - side
    zf = 3 - 3 * side
    me = jnp.where(home, 0, 1)
    col_x = 2 * cy + 1 - cx
    col_y = 2 * (1 - cy) + cx
    col_d = 2 * (1 - cy) + 1 - cx

    barrier = pltpu.get_barrier_semaphore()

    def greet(fs, tp):
        pl.semaphore_signal(barrier, inc=1, device_id={"fs": fs, "tp": tp},
                            device_id_type=pl.DeviceIdType.MESH)

    greet(z, sib)
    greet(z, bx)
    greet(z, by)
    for step in range(1, n):
        greet(lax.rem(z + step, n), b)
        greet(lax.rem(z + step, n), sib)
    pl.semaphore_wait(barrier, 3 + 2 * (n - 1))

    def remote(src, dst, send, recv, fs, tp):
        return pltpu.make_async_remote_copy(
            src_ref=src, dst_ref=dst, send_sem=send, recv_sem=recv,
            device_id={"fs": fs, "tp": tp}, device_id_type=pl.DeviceIdType.MESH)

    def rows_of(k, count=1):
        return pl.ds(pl.multiple_of(k * shard, SUB), count * shard)

    def slot(c, k, kind):
        return weights.at[rows_of(k), pl.ds((3 * c + kind) * LANES, LANES)]

    def own(c, kind):
        return (gate_ref, up_ref, down_ref)[kind].at[:, pl.ds(c * LANES, LANES)]

    def w_copy(src, c, k, kind, fs):
        return remote(src, slot(c, k, kind), z_send.at[c, k, kind], w_recv.at[c, k, kind], fs, b)

    def sib_copy(src, c, k, kind):
        return remote(src, slot(c, k, kind), s_send.at[c, k, kind], w_recv.at[c, k, kind], z, sib)

    def local_copy(c, kind):
        return pltpu.make_async_copy(own(c, kind), slot(c, z, kind), loc_sem.at[c, kind])

    every = [(c, kind) for c in range(chunks) for kind in range(3)]
    mine_q = rows_of(col)
    far_rows = rows_of(2 * side, 2)

    def tk_copy(i, src, dst, fs, tp):
        return remote(src, dst, tk_send.at[i], tk_recv.at[i], fs, tp)

    tok_hop = tk_copy(0, tok_ref.at[mine_q], ptok.at[mine_q], zp, b)
    cot_hop = tk_copy(1, cot_ref.at[mine_q], pcot.at[mine_q], zp, sib)

    def spread(i, buf, q, tp):
        return tk_copy(i, buf.at[rows_of(q)], buf.at[rows_of(q)], z, tp)

    give = tk_copy(8, pcot.at[far_rows], pcot.at[far_rows], z, sib)

    @pl.when(home)
    def _():
        remote(tok_ref.at[mine_q], ptok.at[mine_q], tk_send.at[0], tk_recv.at[0], zp, b).start()
        for c, kind in every:
            w_copy(own(c, kind), c, z, kind, zs).start()
            sib_copy(own(c, kind), c, z, kind).start()
            local_copy(c, kind).start()
        tok[...] = tok_ref[...].T
        cot[...] = cot_ref[...].T

    @pl.when(away)
    def _():
        remote(cot_ref.at[mine_q], pcot.at[mine_q], tk_send.at[1], tk_recv.at[1], zp, sib).start()
        for c, kind in every:
            w_copy(own(c, kind), c, z, kind, zn).start()
        tok_hop.wait_recv()
        spread(2, ptok, col, bx).start()
        spread(3, ptok, col, by).start()
        cot_hop.wait_recv()
        spread(4, pcot, col, bx).start()
        spread(5, pcot, col, by).start()
        spread(2, ptok, col_x, bx).wait_recv()
        spread(6, ptok, col_x, by).start()
        spread(5, pcot, col_y, by).wait_recv()
        spread(7, pcot, col_y, bx).start()
        spread(3, ptok, col_y, by).wait_recv()
        spread(6, ptok, col_d, by).wait_recv()
        tok[...] = ptok[...].T
        spread(4, pcot, col_x, bx).wait_recv()
        spread(7, pcot, col_d, bx).wait_recv()
        give.start()
        cot[...] = pcot[...].T

    others = (zs, zn, zf)

    def gather(c):
        @pl.when(home)
        def _():
            for kind in range(3):
                for i, k in enumerate(others):
                    w_copy(slot(c, k, kind), c, k, kind, zs).wait_recv()
                    if i:
                        @pl.when(near)
                        def _():
                            w_copy(slot(c, k, kind), c, k, kind, zs).start()
                    sib_copy(slot(c, k, kind), c, k, kind).start()
            for kind in range(3):
                local_copy(c, kind).wait()

        @pl.when(away)
        def _():
            for kind in range(3):
                for k in range(n):
                    sib_copy(slot(c, k, kind), c, k, kind).wait_recv()

    def hid_copy(c):
        return remote(hid.at[me, c], hid.at[me, c], hid_send.at[c], hid_recv.at[c], z, sib)

    def dg_home(c):
        return remote(dgs.at[c, 0], dgr.at[c, 0], dg_send.at[c], dg_recv.at[c], zs, b)

    def dg_away(c):
        return remote(dgs.at[c], dgr.at[c], dg_send.at[c], dg_recv.at[c], zs, b)

    def dg_far(c, i):
        return remote(dgs.at[c, i], dgf.at[c], dgf_send.at[c, i], dgf_recv.at[c],
                      2 * (1 - side) + i, sib)

    def lanes_of(c):
        return pl.ds(c * LANES, LANES)

    def down_part(c):
        hid_copy(c).wait_recv()
        for i in range(2):
            k = rows_of(2 * core + i)
            value = (jnp.dot(cot_ref[k, :], hid[0, c], preferred_element_type=F32)
                     + jnp.dot(pcot[k, :], hid[1, c], preferred_element_type=F32))

            @pl.when(jnp.logical_and(home, zodd == i))
            def _():
                dg_out[:, lanes_of(c)] = value

            @pl.when(jnp.logical_and(home, zodd != i))
            def _():
                dgs[c, 0] = value.astype(BF16)

            @pl.when(jnp.logical_and(away, near))
            def _():
                dgp[c, i] = value

            @pl.when(jnp.logical_and(away, end))
            def _():
                dgs[c, i] = value.astype(BF16)

        @pl.when(home)
        def _():
            dg_home(c).start()

        @pl.when(jnp.logical_and(away, end))
        def _():
            dg_away(c).start()

    def down_mid(c):
        @pl.when(jnp.logical_and(away, near))
        def _():
            dg_away(c).wait_recv()
            for i in range(2):
                dgs[c, i] = (dgp[c, i] + dgr[c, i].astype(F32)).astype(BF16)
                dg_far(c, i).start()

    def down_final(c):
        @pl.when(home)
        def _():
            dg_home(c).wait_recv()
            dg_out[:, lanes_of(c)] += dgr[c, 0].astype(F32)

        @pl.when(away)
        def _():
            dg_far(c, 0).wait_recv()
            dg_out[:, lanes_of(c)] = dgf[c].astype(F32)

    low, high = slice(0, half_rows), slice(half_rows, rows)
    halves = (low, high)

    def t1_copy(i, step):
        return remote(t1s.at[i, step], t1r.at[i, step], t1_send.at[i, step], t1_recv.at[i, step],
                      z, bx if i == 0 else by)

    def t2_copy(i, q):
        return remote(t2s.at[i, q], t2r.at[i, q], t2_send.at[i, q], t2_recv.at[i, q],
                      z, by if i == 0 else bx)

    def t3_copy(q):
        return remote(t3s.at[q], t3r.at[q], t3_send.at[q], t3_recv.at[q], zp, b)

    def strip(k, q):
        return pl.ds(pl.multiple_of(k * shard + q * piece, SUB), piece)

    def y_copy(i, k, q, tp):
        ref = ybuf.at[strip(k, q)]
        return remote(ref, ref, y_send.at[i, q], y_recv.at[i, q], z, tp)

    def y_half(i, k, q, tp):
        ref = ybuf.at[strip(k, q), pl.ds(i * half_rows, half_rows)]
        return remote(ref, ref, yd_send.at[i, q], yd_recv.at[i, q], z, tp)

    def y_sib(i, k, q):
        ref = ybuf.at[strip(k, q)]
        return remote(ref, ref, y_send.at[2 + i, q], y_recv.at[2 + i, q], z, sib)

    for c in range(chunks):
        gather(c)
        w = weights[:, 3 * c * LANES:(3 * c + 2) * LANES]
        pre = jnp.dot(tok[...], w, preferred_element_type=F32)
        hg = jnp.dot(cot[...], weights[:, (3 * c + 2) * LANES:(3 * c + 3) * LANES],
                     preferred_element_type=F32)
        gate_pre, up_pre = pre[:, :LANES], pre[:, LANES:]
        sig = jax.nn.sigmoid(gate_pre)
        act = gate_pre * sig
        hid[me, c] = (act * up_pre).astype(BF16)
        hid_copy(c).start()
        dgu = jnp.concatenate(
            [(hg * up_pre * sig * (1.0 + gate_pre * (1.0 - sig))).astype(BF16),
             (hg * act).astype(BF16)], axis=1)
        if c == 0:
            dxacc[...] = contract_cols(w, dgu)
        elif c < chunks - 1:
            dxacc[...] += contract_cols(w, dgu)
        if c == 0:
            @pl.when(home)
            def _():
                give.wait_recv()
        if c < chunks - 1:
            down_part(c)
        if 0 < c < chunks - 1:
            down_mid(c - 1)
        if c == chunks - 1:
            for k, sends in ((col_d, ((0, 0), (1, 0))), (col_x, ((0, 1),)), (col_y, ((1, 1),)), (col, ())):
                r = rows_of(k)
                value = contract_cols(weights[r, 3 * c * LANES:(3 * c + 2) * LANES], dgu)
                if c:
                    value = value + dxacc[r, :]
                if k is not col_d:
                    dxacc[r, :] = value
                for i, step in sends:
                    t1s[i, step] = value[:, halves[i]].astype(BF16)
                    t1_copy(i, step).start()

    down_part(chunks - 1)
    t1_copy(0, 0).wait_recv()
    t1_copy(1, 0).wait_recv()
    for q in range(parts):
        inner = slice(q * piece, (q + 1) * piece)
        for i, k in ((0, col_y), (1, col_x)):
            t2s[i, q] = (dxacc[strip(k, q), halves[i]] + t1r[i, 0, inner].astype(F32)).astype(BF16)
            t2_copy(i, q).start()
    t1_copy(0, 1).wait_recv()
    t1_copy(1, 1).wait_recv()
    for q in range(parts):
        inner = slice(q * piece, (q + 1) * piece)
        for i in range(2):
            dxacc[strip(col, q), halves[i]] += t1r[i, 1, inner].astype(F32)
    for q in range(parts):
        for i in range(2):
            t2_copy(i, q).wait_recv()
            dxacc[strip(col, q), halves[i]] += t2r[i, q].astype(F32)

        @pl.when(away)
        def _():
            t3s[q] = dxacc[strip(col, q), :].astype(BF16)
            t3_copy(q).start()
    for c in range(max(0, chunks - 2), chunks):
        down_mid(c)

    @pl.when(home)
    def _():
        for q in range(parts):
            t3_copy(q).wait_recv()
            ybuf[strip(col, q), :] = (dxacc[strip(col, q), :] + t3r[q].astype(F32)).astype(BF16)
            y_copy(0, col, q, bx).start()
            y_copy(1, col, q, by).start()
            y_sib(0, col, q).start()
        for q in range(parts):
            y_copy(0, col_x, q, bx).wait_recv()
            y_half(0, col_x, q, by).start()
            y_sib(1, col_x, q).start()
            y_copy(1, col_y, q, by).wait_recv()
            y_half(1, col_y, q, bx).start()
            y_sib(2, col_y, q).start()
        for q in range(parts):
            y_half(0, col_d, q, by).wait_recv()
            y_half(1, col_d, q, bx).wait_recv()
            y_sib(3, col_d, q).start()

    for c in range(chunks):
        down_final(c)

    @pl.when(away)
    def _():
        for q in range(parts):
            for i, k in enumerate((col, col_x, col_y, col_d)):
                y_sib(i, k, q).wait_recv()
    dx_out[...] = ybuf[...]

    @pl.when(home)
    def _():
        tok_hop.wait_send()
        for c, kind in every:
            w_copy(own(c, kind), c, z, kind, zs).wait_send()
            sib_copy(own(c, kind), c, z, kind).wait_send()
            for i, k in enumerate(others):
                sib_copy(slot(c, k, kind), c, k, kind).wait_send()
                if i:
                    @pl.when(near)
                    def _():
                        w_copy(slot(c, k, kind), c, k, kind, zs).wait_send()
        for c in range(chunks):
            dg_home(c).wait_send()
        for q in range(parts):
            y_copy(0, col, q, bx).wait_send()
            y_copy(1, col, q, by).wait_send()
            y_half(0, col_x, q, by).wait_send()
            y_half(1, col_y, q, bx).wait_send()
            for i, k in enumerate((col, col_x, col_y, col_d)):
                y_sib(i, k, q).wait_send()

    @pl.when(away)
    def _():
        cot_hop.wait_send()
        for c, kind in every:
            w_copy(own(c, kind), c, z, kind, zn).wait_send()
        spread(2, ptok, col, bx).wait_send()
        spread(3, ptok, col, by).wait_send()
        spread(4, pcot, col, bx).wait_send()
        spread(5, pcot, col, by).wait_send()
        spread(6, ptok, col_x, by).wait_send()
        spread(7, pcot, col_y, bx).wait_send()
        give.wait_send()
        for q in range(parts):
            t3_copy(q).wait_send()
        for c in range(chunks):
            @pl.when(end)
            def _():
                dg_away(c).wait_send()

            @pl.when(near)
            def _():
                for i in range(2):
                    dg_far(c, i).wait_send()

    for c in range(chunks):
        hid_copy(c).wait_send()
    for i in range(2):
        for step in range(2):
            t1_copy(i, step).wait_send()
        for q in range(parts):
            t2_copy(i, q).wait_send()


def per_device_kernel(n, tokens, cotangent, gate_weight, up_weight, down_weight):
    rows, depth = tokens.shape
    shard, ff = gate_weight.shape
    chunks = ff // LANES
    parts = next(p for p in (3, 2, 1) if shard % (p * SUB) == 0)
    piece = shard // parts
    vmem = pl.BlockSpec(memory_space=pltpu.VMEM)
    dma = pltpu.SemaphoreType.DMA
    dx, dg = pl.pallas_call(
        functools.partial(kernel, n),
        out_shape=(jax.ShapeDtypeStruct((depth, rows), BF16),
                   jax.ShapeDtypeStruct((shard, ff), F32)),
        in_specs=[vmem] * 5,
        out_specs=(vmem, vmem),
        scratch_shapes=[
            pltpu.VMEM((depth, 3 * ff), BF16),
            pltpu.VMEM((rows, depth), BF16),
            pltpu.VMEM((rows, depth), BF16),
            pltpu.VMEM((depth, rows), BF16),
            pltpu.VMEM((depth, rows), BF16),
            pltpu.VMEM((depth, rows), F32),
            pltpu.VMEM((2, chunks, rows, LANES), BF16),
            pltpu.VMEM((chunks, 2, shard, LANES), F32),
            pltpu.VMEM((chunks, 2, shard, LANES), BF16),
            pltpu.VMEM((chunks, 2, shard, LANES), BF16),
            pltpu.VMEM((chunks, shard, LANES), BF16),
            pltpu.VMEM((2, 2, shard, rows // 2), BF16),
            pltpu.VMEM((2, 2, shard, rows // 2), BF16),
            pltpu.VMEM((2, parts, piece, rows // 2), BF16),
            pltpu.VMEM((2, parts, piece, rows // 2), BF16),
            pltpu.VMEM((parts, piece, rows), BF16),
            pltpu.VMEM((parts, piece, rows), BF16),
            pltpu.VMEM((depth, rows), BF16),
            dma((chunks, n, 3)), dma((chunks, n, 3)), dma((chunks, n, 3)), dma((chunks, 3)),
            dma((9,)), dma((9,)), dma((chunks,)), dma((chunks,)),
            dma((chunks,)), dma((chunks,)), dma((chunks, 2)), dma((chunks,)),
            dma((2, 2)), dma((2, 2)), dma((2, parts)), dma((2, parts)),
            dma((parts,)), dma((parts,)), dma((6, parts)), dma((6, parts)),
            dma((2, parts)), dma((2, parts)),
        ],
        compiler_params=pltpu.CompilerParams(
            collective_id=0, has_side_effects=True, vmem_limit_bytes=56 * 2**20),
    )(tokens.T, cotangent.T, gate_weight, up_weight, down_weight.T)
    return dx.T, dg.T


def solution(mesh):
    n, tp = mesh.shape["fs"], mesh.shape["tp"]

    def per_device(tokens, cotangent, gate_weight, up_weight, down_weight):
        rows, depth = tokens.shape
        shard, ff = gate_weight.shape
        args = (tokens, cotangent, gate_weight, up_weight, down_weight)
        fits = (tp == 8 and n == 4 and rows % (2 * LANES) == 0 and rows <= 512
                and depth == n * shard and shard % SUB == 0 and ff % LANES == 0 and ff <= 512)
        return per_device_kernel(n, *args) if fits else per_device_plain(*args)

    placed = (P("fs", None), P("fs", None), P("fs", "tp"), P("fs", "tp"), P("tp", "fs"))
    return jax.shard_map(
        per_device,
        mesh=mesh,
        in_specs=placed,
        out_specs=(P("fs", None), P("tp", "fs")),
        check_vma=False,
    )
```

```python
import functools

import jax
import jax.numpy as jnp
from jax import lax
from jax.experimental import pallas as pl
from jax.experimental.pallas import tpu as pltpu
from jax.sharding import PartitionSpec as P

LANES = 128
SUB = 16
BF16 = jnp.bfloat16
F32 = jnp.float32


def contract_rows(left, right):
    return lax.dot_general(
        left, right, (((0,), (0,)), ((), ())), preferred_element_type=jnp.float32
    )


def contract_cols(left, right):
    return lax.dot_general(
        left, right, (((1,), (1,)), ((), ())), preferred_element_type=jnp.float32
    )


def send_down(hidden, cotangent):
    return lax.psum_scatter(
        contract_rows(cotangent, hidden), "fs", scatter_dimension=0, tiled=True
    ).T


def per_device_plain(tokens, cotangent, gate_weight, up_weight, down_weight):
    whole_gate, whole_up, whole_down = (
        lax.all_gather(gate_weight, "fs", axis=0, tiled=True),
        lax.all_gather(up_weight, "fs", axis=0, tiled=True),
        lax.all_gather(down_weight, "fs", axis=1, tiled=True),
    )
    gate_pre = jnp.dot(tokens, whole_gate, preferred_element_type=jnp.float32)
    up_pre = jnp.dot(tokens, whole_up, preferred_element_type=jnp.float32)
    hidden_grad = contract_cols(cotangent, whole_down)
    sigmoid_gate = jax.nn.sigmoid(gate_pre)
    activated = gate_pre * sigmoid_gate
    hidden = (activated * up_pre).astype(jnp.bfloat16)
    gate_pre_grad = (
        hidden_grad * up_pre * sigmoid_gate * (1.0 + gate_pre * (1.0 - sigmoid_gate))
    ).astype(jnp.bfloat16)
    up_pre_grad = (hidden_grad * activated).astype(jnp.bfloat16)
    partial_value = contract_cols(gate_pre_grad, whole_gate) + contract_cols(up_pre_grad, whole_up)
    input_grad = lax.psum(partial_value.astype(jnp.bfloat16), "tp")
    down_grad = send_down(hidden, cotangent)
    return (input_grad, down_grad)


def kernel(n, tok_hbm, cot_hbm, gate_hbm, up_hbm, down_hbm, dx_out, dg_out,
           tok_ref, cot_ref, gate_ref, up_ref, down_ref, dgacc, weights, tok, cot, ptok, pcot, dxacc, hid, dgp, dgs, dgr, dgf,
           t1s, t1r, t2s, t2r, t3s, t3r, ybuf,
           z_send, s_send, w_recv, loc_sem, tk_send, tk_recv, hid_send, hid_recv,
           dg_send, dg_recv, dgf_send, dgf_recv, t1_send, t1_recv, t2_send, t2_recv,
           t3_send, t3_recv, y_send, y_recv, yd_send, yd_recv, in_sem, out_sem):
    z = lax.axis_index("fs")
    b = lax.axis_index("tp")
    depth, rows = tok_ref.shape
    shard, ff = gate_ref.shape
    chunks = ff // LANES
    parts = t2s.shape[1]
    piece = shard // parts
    half_rows = rows // 2
    core = lax.rem(b, 2)
    col = lax.div(b, 2)
    cx = lax.rem(col, 2)
    cy = lax.div(col, 2)
    side = lax.div(z, 2)
    home = core == side
    away = core != side
    near = jnp.logical_or(z == 1, z == 2)
    end = jnp.logical_not(near)
    zodd = lax.rem(z, 2)
    sib = b + 1 - 2 * core
    bx = b + 2 * (1 - 2 * cx)
    by = b + 4 * (1 - 2 * cy)
    zs = z + 1 - 2 * zodd
    zp = lax.rem(z + 2, 4)
    zn = 2 - side
    zf = 3 - 3 * side
    me = jnp.where(home, 0, 1)
    col_x = 2 * cy + 1 - cx
    col_y = 2 * (1 - cy) + cx
    col_d = 2 * (1 - cy) + 1 - cx

    loads = [pltpu.make_async_copy(src, dst, in_sem.at[i]) for i, (src, dst) in enumerate((
        (tok_hbm, tok_ref), (cot_hbm, cot_ref), (gate_hbm, gate_ref), (up_hbm, up_ref),
        (down_hbm, down_ref)))]
    for load in loads:
        load.start()
    barrier = pltpu.get_barrier_semaphore()

    def greet(fs, tp):
        pl.semaphore_signal(barrier, inc=1, device_id={"fs": fs, "tp": tp},
                            device_id_type=pl.DeviceIdType.MESH)

    greet(z, sib)
    greet(z, bx)
    greet(z, by)
    for step in range(1, n):
        greet(lax.rem(z + step, n), b)
        greet(lax.rem(z + step, n), sib)
    pl.semaphore_wait(barrier, 3 + 2 * (n - 1))
    for load in loads:
        load.wait()

    def remote(src, dst, send, recv, fs, tp):
        return pltpu.make_async_remote_copy(
            src_ref=src, dst_ref=dst, send_sem=send, recv_sem=recv,
            device_id={"fs": fs, "tp": tp}, device_id_type=pl.DeviceIdType.MESH)

    def rows_of(k, count=1):
        return pl.ds(pl.multiple_of(k * shard, SUB), count * shard)

    def slot(c, k, kind):
        return weights.at[rows_of(k), pl.ds((3 * c + kind) * LANES, LANES)]

    def own(c, kind):
        return (gate_ref, up_ref, down_ref)[kind].at[:, pl.ds(c * LANES, LANES)]

    def w_copy(src, c, k, kind, fs):
        return remote(src, slot(c, k, kind), z_send.at[c, k, kind], w_recv.at[c, k, kind], fs, b)

    def sib_copy(src, c, k, kind):
        return remote(src, slot(c, k, kind), s_send.at[c, k, kind], w_recv.at[c, k, kind], z, sib)

    def local_copy(c, kind):
        return pltpu.make_async_copy(own(c, kind), slot(c, z, kind), loc_sem.at[c, kind])

    every = [(c, kind) for c in range(chunks) for kind in range(3)]
    mine_q = rows_of(col)
    far_rows = rows_of(2 * side, 2)

    def tk_copy(i, src, dst, fs, tp):
        return remote(src, dst, tk_send.at[i], tk_recv.at[i], fs, tp)

    tok_hop = tk_copy(0, tok_ref.at[mine_q], ptok.at[mine_q], zp, b)
    cot_hop = tk_copy(1, cot_ref.at[mine_q], pcot.at[mine_q], zp, sib)

    def spread(i, buf, q, tp):
        return tk_copy(i, buf.at[rows_of(q)], buf.at[rows_of(q)], z, tp)

    give = tk_copy(8, pcot.at[far_rows], pcot.at[far_rows], z, sib)

    @pl.when(home)
    def _():
        remote(tok_ref.at[mine_q], ptok.at[mine_q], tk_send.at[0], tk_recv.at[0], zp, b).start()
        for c, kind in every:
            w_copy(own(c, kind), c, z, kind, zs).start()
            sib_copy(own(c, kind), c, z, kind).start()
            local_copy(c, kind).start()
        tok[...] = tok_ref[...].T
        cot[...] = cot_ref[...].T

    @pl.when(away)
    def _():
        remote(cot_ref.at[mine_q], pcot.at[mine_q], tk_send.at[1], tk_recv.at[1], zp, sib).start()
        for c, kind in every:
            w_copy(own(c, kind), c, z, kind, zn).start()
        tok_hop.wait_recv()
        spread(2, ptok, col, bx).start()
        spread(3, ptok, col, by).start()
        cot_hop.wait_recv()
        spread(4, pcot, col, bx).start()
        spread(5, pcot, col, by).start()
        spread(2, ptok, col_x, bx).wait_recv()
        spread(6, ptok, col_x, by).start()
        spread(5, pcot, col_y, by).wait_recv()
        spread(7, pcot, col_y, bx).start()
        spread(3, ptok, col_y, by).wait_recv()
        spread(6, ptok, col_d, by).wait_recv()
        tok[...] = ptok[...].T
        spread(4, pcot, col_x, bx).wait_recv()
        spread(7, pcot, col_d, bx).wait_recv()
        give.start()
        cot[...] = pcot[...].T

    others = (zs, zn, zf)

    def gather(c):
        @pl.when(home)
        def _():
            for kind in range(3):
                for i, k in enumerate(others):
                    w_copy(slot(c, k, kind), c, k, kind, zs).wait_recv()
                    if i:
                        @pl.when(near)
                        def _():
                            w_copy(slot(c, k, kind), c, k, kind, zs).start()
                    sib_copy(slot(c, k, kind), c, k, kind).start()
            for kind in range(3):
                local_copy(c, kind).wait()

        @pl.when(away)
        def _():
            for kind in range(3):
                for k in range(n):
                    sib_copy(slot(c, k, kind), c, k, kind).wait_recv()

    def hid_copy(c):
        return remote(hid.at[me, c], hid.at[me, c], hid_send.at[c], hid_recv.at[c], z, sib)

    def dg_home(c):
        return remote(dgs.at[c, 0], dgr.at[c, 0], dg_send.at[c], dg_recv.at[c], zs, b)

    def dg_away(c):
        return remote(dgs.at[c], dgr.at[c], dg_send.at[c], dg_recv.at[c], zs, b)

    def dg_far(c, i):
        return remote(dgs.at[c, i], dgf.at[c], dgf_send.at[c, i], dgf_recv.at[c],
                      2 * (1 - side) + i, sib)

    def lanes_of(c):
        return pl.ds(c * LANES, LANES)

    def down_part(c):
        hid_copy(c).wait_recv()
        for i in range(2):
            k = rows_of(2 * core + i)
            value = (jnp.dot(cot_ref[k, :], hid[0, c], preferred_element_type=F32)
                     + jnp.dot(pcot[k, :], hid[1, c], preferred_element_type=F32))

            @pl.when(jnp.logical_and(home, zodd == i))
            def _():
                dgacc[:, lanes_of(c)] = value

            @pl.when(jnp.logical_and(home, zodd != i))
            def _():
                dgs[c, 0] = value.astype(BF16)

            @pl.when(jnp.logical_and(away, near))
            def _():
                dgp[c, i] = value

            @pl.when(jnp.logical_and(away, end))
            def _():
                dgs[c, i] = value.astype(BF16)

        @pl.when(home)
        def _():
            dg_home(c).start()

        @pl.when(jnp.logical_and(away, end))
        def _():
            dg_away(c).start()

    def down_mid(c):
        @pl.when(jnp.logical_and(away, near))
        def _():
            dg_away(c).wait_recv()
            for i in range(2):
                dgs[c, i] = (dgp[c, i] + dgr[c, i].astype(F32)).astype(BF16)
                dg_far(c, i).start()

    def down_final(c):
        @pl.when(home)
        def _():
            dg_home(c).wait_recv()
            dgacc[:, lanes_of(c)] += dgr[c, 0].astype(F32)

        @pl.when(away)
        def _():
            dg_far(c, 0).wait_recv()
            dgacc[:, lanes_of(c)] = dgf[c].astype(F32)

    low, high = slice(0, half_rows), slice(half_rows, rows)
    halves = (low, high)

    def t1_copy(i, step):
        return remote(t1s.at[i, step], t1r.at[i, step], t1_send.at[i, step], t1_recv.at[i, step],
                      z, bx if i == 0 else by)

    def t2_copy(i, q):
        return remote(t2s.at[i, q], t2r.at[i, q], t2_send.at[i, q], t2_recv.at[i, q],
                      z, by if i == 0 else bx)

    def t3_copy(q):
        return remote(t3s.at[q], t3r.at[q], t3_send.at[q], t3_recv.at[q], zp, b)

    def strip(k, q):
        return pl.ds(pl.multiple_of(k * shard + q * piece, SUB), piece)

    def y_copy(i, k, q, tp):
        ref = ybuf.at[strip(k, q)]
        return remote(ref, ref, y_send.at[i, q], y_recv.at[i, q], z, tp)

    def y_half(i, k, q, tp):
        ref = ybuf.at[strip(k, q), pl.ds(i * half_rows, half_rows)]
        return remote(ref, ref, yd_send.at[i, q], yd_recv.at[i, q], z, tp)

    def put(i, k, q):
        r = strip(k, q)
        return pltpu.make_async_copy(ybuf.at[r], dx_out.at[r], out_sem.at[i, q])

    dg_put = pltpu.make_async_copy(dgacc, dg_out, out_sem.at[4, 0])

    def y_sib(i, k, q):
        ref = ybuf.at[strip(k, q)]
        return remote(ref, ref, y_send.at[2 + i, q], y_recv.at[2 + i, q], z, sib)

    for c in range(chunks):
        gather(c)
        w = weights[:, 3 * c * LANES:(3 * c + 2) * LANES]
        pre = jnp.dot(tok[...], w, preferred_element_type=F32)
        hg = jnp.dot(cot[...], weights[:, (3 * c + 2) * LANES:(3 * c + 3) * LANES],
                     preferred_element_type=F32)
        gate_pre, up_pre = pre[:, :LANES], pre[:, LANES:]
        sig = jax.nn.sigmoid(gate_pre)
        act = gate_pre * sig
        hid[me, c] = (act * up_pre).astype(BF16)
        hid_copy(c).start()
        dgu = jnp.concatenate(
            [(hg * up_pre * sig * (1.0 + gate_pre * (1.0 - sig))).astype(BF16),
             (hg * act).astype(BF16)], axis=1)
        if c == 0:
            dxacc[...] = contract_cols(w, dgu)
        elif c < chunks - 1:
            dxacc[...] += contract_cols(w, dgu)
        if c:
            @pl.when(end)
            def _():
                if c == 1:
                    @pl.when(home)
                    def _():
                        give.wait_recv()
                down_part(c - 1)
        if c == chunks - 1:
            for k, sends in ((col_d, ((0, 0), (1, 0))), (col_x, ((0, 1),)), (col_y, ((1, 1),)), (col, ())):
                r = rows_of(k)
                value = contract_cols(weights[r, 3 * c * LANES:(3 * c + 2) * LANES], dgu)
                if c:
                    value = value + dxacc[r, :]
                if k is not col_d:
                    dxacc[r, :] = value
                for i, step in sends:
                    t1s[i, step] = value[:, halves[i]].astype(BF16)
                    t1_copy(i, step).start()

    @pl.when(end)
    def _():
        if chunks == 1:
            @pl.when(home)
            def _():
                give.wait_recv()
        down_part(chunks - 1)

    @pl.when(near)
    def _():
        @pl.when(home)
        def _():
            give.wait_recv()
        for c in range(chunks):
            down_part(c)
    t1_copy(0, 0).wait_recv()
    t1_copy(1, 0).wait_recv()
    for q in range(parts):
        inner = slice(q * piece, (q + 1) * piece)
        for i, k in ((0, col_y), (1, col_x)):
            t2s[i, q] = (dxacc[strip(k, q), halves[i]] + t1r[i, 0, inner].astype(F32)).astype(BF16)
            t2_copy(i, q).start()
    t1_copy(0, 1).wait_recv()
    t1_copy(1, 1).wait_recv()
    for q in range(parts):
        inner = slice(q * piece, (q + 1) * piece)
        for i in range(2):
            dxacc[strip(col, q), halves[i]] += t1r[i, 1, inner].astype(F32)
    for q in range(parts):
        for i in range(2):
            t2_copy(i, q).wait_recv()
            dxacc[strip(col, q), halves[i]] += t2r[i, q].astype(F32)

        @pl.when(away)
        def _():
            t3s[q] = dxacc[strip(col, q), :].astype(BF16)
            t3_copy(q).start()
    for c in range(chunks):
        down_mid(c)

    @pl.when(home)
    def _():
        for q in range(parts):
            t3_copy(q).wait_recv()
            ybuf[strip(col, q), :] = (dxacc[strip(col, q), :] + t3r[q].astype(F32)).astype(BF16)
            y_copy(0, col, q, bx).start()
            y_copy(1, col, q, by).start()
            y_sib(0, col, q).start()
            put(0, col, q).start()
        for q in range(parts):
            y_copy(0, col_x, q, bx).wait_recv()
            y_half(0, col_x, q, by).start()
            y_sib(1, col_x, q).start()
            put(1, col_x, q).start()
            y_copy(1, col_y, q, by).wait_recv()
            y_half(1, col_y, q, bx).start()
            y_sib(2, col_y, q).start()
            put(2, col_y, q).start()
        for q in range(parts):
            y_half(0, col_d, q, by).wait_recv()
            y_half(1, col_d, q, bx).wait_recv()
            y_sib(3, col_d, q).start()
            put(3, col_d, q).start()

    for c in range(chunks):
        down_final(c)
    dg_put.start()

    @pl.when(away)
    def _():
        for q in range(parts):
            for i, k in enumerate((col, col_x, col_y, col_d)):
                y_sib(i, k, q).wait_recv()
                put(i, k, q).start()

    @pl.when(home)
    def _():
        tok_hop.wait_send()
        for c, kind in every:
            w_copy(own(c, kind), c, z, kind, zs).wait_send()
            sib_copy(own(c, kind), c, z, kind).wait_send()
            for i, k in enumerate(others):
                sib_copy(slot(c, k, kind), c, k, kind).wait_send()
                if i:
                    @pl.when(near)
                    def _():
                        w_copy(slot(c, k, kind), c, k, kind, zs).wait_send()
        for c in range(chunks):
            dg_home(c).wait_send()
        for q in range(parts):
            y_copy(0, col, q, bx).wait_send()
            y_copy(1, col, q, by).wait_send()
            y_half(0, col_x, q, by).wait_send()
            y_half(1, col_y, q, bx).wait_send()
            for i, k in enumerate((col, col_x, col_y, col_d)):
                y_sib(i, k, q).wait_send()

    @pl.when(away)
    def _():
        cot_hop.wait_send()
        for c, kind in every:
            w_copy(own(c, kind), c, z, kind, zn).wait_send()
        spread(2, ptok, col, bx).wait_send()
        spread(3, ptok, col, by).wait_send()
        spread(4, pcot, col, bx).wait_send()
        spread(5, pcot, col, by).wait_send()
        spread(6, ptok, col_x, by).wait_send()
        spread(7, pcot, col_y, bx).wait_send()
        give.wait_send()
        for q in range(parts):
            t3_copy(q).wait_send()
        for c in range(chunks):
            @pl.when(end)
            def _():
                dg_away(c).wait_send()

            @pl.when(near)
            def _():
                for i in range(2):
                    dg_far(c, i).wait_send()

    for q in range(parts):
        for i, k in enumerate((col, col_x, col_y, col_d)):
            put(i, k, q).wait()
    dg_put.wait()
    for c in range(chunks):
        hid_copy(c).wait_send()
    for i in range(2):
        for step in range(2):
            t1_copy(i, step).wait_send()
        for q in range(parts):
            t2_copy(i, q).wait_send()


def per_device_kernel(n, tokens, cotangent, gate_weight, up_weight, down_weight):
    rows, depth = tokens.shape
    shard, ff = gate_weight.shape
    chunks = ff // LANES
    parts = next(p for p in (3, 2, 1) if shard % (p * SUB) == 0)
    piece = shard // parts
    vmem = pl.BlockSpec(memory_space=pltpu.VMEM)
    dma = pltpu.SemaphoreType.DMA
    dx, dg = pl.pallas_call(
        functools.partial(kernel, n),
        out_shape=(pltpu.VMEM((depth, rows), BF16), pltpu.VMEM((shard, ff), F32)),
        in_specs=[pl.BlockSpec(memory_space=pltpu.HBM)] * 5,
        out_specs=[pl.BlockSpec(memory_space=pl.ANY)] * 2,
        scratch_shapes=[
            pltpu.VMEM((depth, rows), BF16),
            pltpu.VMEM((depth, rows), BF16),
            pltpu.VMEM((shard, ff), BF16),
            pltpu.VMEM((shard, ff), BF16),
            pltpu.VMEM((shard, ff), BF16),
            pltpu.VMEM((shard, ff), F32),
            pltpu.VMEM((depth, 3 * ff), BF16),
            pltpu.VMEM((rows, depth), BF16),
            pltpu.VMEM((rows, depth), BF16),
            pltpu.VMEM((depth, rows), BF16),
            pltpu.VMEM((depth, rows), BF16),
            pltpu.VMEM((depth, rows), F32),
            pltpu.VMEM((2, chunks, rows, LANES), BF16),
            pltpu.VMEM((chunks, 2, shard, LANES), F32),
            pltpu.VMEM((chunks, 2, shard, LANES), BF16),
            pltpu.VMEM((chunks, 2, shard, LANES), BF16),
            pltpu.VMEM((chunks, shard, LANES), BF16),
            pltpu.VMEM((2, 2, shard, rows // 2), BF16),
            pltpu.VMEM((2, 2, shard, rows // 2), BF16),
            pltpu.VMEM((2, parts, piece, rows // 2), BF16),
            pltpu.VMEM((2, parts, piece, rows // 2), BF16),
            pltpu.VMEM((parts, piece, rows), BF16),
            pltpu.VMEM((parts, piece, rows), BF16),
            pltpu.VMEM((depth, rows), BF16),
            dma((chunks, n, 3)), dma((chunks, n, 3)), dma((chunks, n, 3)), dma((chunks, 3)),
            dma((9,)), dma((9,)), dma((chunks,)), dma((chunks,)),
            dma((chunks,)), dma((chunks,)), dma((chunks, 2)), dma((chunks,)),
            dma((2, 2)), dma((2, 2)), dma((2, parts)), dma((2, parts)),
            dma((parts,)), dma((parts,)), dma((6, parts)), dma((6, parts)),
            dma((2, parts)), dma((2, parts)), dma((5,)), dma((5, parts)),
        ],
        compiler_params=pltpu.CompilerParams(
            collective_id=0, has_side_effects=True, vmem_limit_bytes=28 * 2**20),
    )(*(pltpu.with_memory_space_constraint(a, pltpu.HBM) for a in (
        tokens.T, cotangent.T, gate_weight, up_weight, down_weight.T)))
    return dx.T, dg.T


def solution(mesh):
    n, tp = mesh.shape["fs"], mesh.shape["tp"]

    def per_device(tokens, cotangent, gate_weight, up_weight, down_weight):
        rows, depth = tokens.shape
        shard, ff = gate_weight.shape
        args = (tokens, cotangent, gate_weight, up_weight, down_weight)
        fits = (tp == 8 and n == 4 and rows % (2 * LANES) == 0 and rows <= 512
                and depth == n * shard and shard % SUB == 0 and ff % LANES == 0 and ff <= 512)
        return per_device_kernel(n, *args) if fits else per_device_plain(*args)

    placed = (P("fs", None), P("fs", None), P("fs", "tp"), P("fs", "tp"), P("tp", "fs"))
    return jax.shard_map(
        per_device,
        mesh=mesh,
        in_specs=placed,
        out_specs=(P("fs", None), P("tp", "fs")),
        check_vma=False,
    )
```

```python
import functools

import jax
import jax.numpy as jnp
from jax import lax
from jax.experimental import pallas as pl
from jax.experimental.pallas import tpu as pltpu
from jax.sharding import PartitionSpec as P

LANES = 128
SUB = 16
BF16 = jnp.bfloat16
F32 = jnp.float32


def contract_rows(left, right):
    return lax.dot_general(
        left, right, (((0,), (0,)), ((), ())), preferred_element_type=jnp.float32
    )


def contract_cols(left, right):
    return lax.dot_general(
        left, right, (((1,), (1,)), ((), ())), preferred_element_type=jnp.float32
    )


def send_down(hidden, cotangent):
    return lax.psum_scatter(
        contract_rows(cotangent, hidden), "fs", scatter_dimension=0, tiled=True
    ).T


def per_device_plain(tokens, cotangent, gate_weight, up_weight, down_weight):
    whole_gate, whole_up, whole_down = (
        lax.all_gather(gate_weight, "fs", axis=0, tiled=True),
        lax.all_gather(up_weight, "fs", axis=0, tiled=True),
        lax.all_gather(down_weight, "fs", axis=1, tiled=True),
    )
    gate_pre = jnp.dot(tokens, whole_gate, preferred_element_type=jnp.float32)
    up_pre = jnp.dot(tokens, whole_up, preferred_element_type=jnp.float32)
    hidden_grad = contract_cols(cotangent, whole_down)
    sigmoid_gate = jax.nn.sigmoid(gate_pre)
    activated = gate_pre * sigmoid_gate
    hidden = (activated * up_pre).astype(jnp.bfloat16)
    gate_pre_grad = (
        hidden_grad * up_pre * sigmoid_gate * (1.0 + gate_pre * (1.0 - sigmoid_gate))
    ).astype(jnp.bfloat16)
    up_pre_grad = (hidden_grad * activated).astype(jnp.bfloat16)
    partial_value = contract_cols(gate_pre_grad, whole_gate) + contract_cols(up_pre_grad, whole_up)
    input_grad = lax.psum(partial_value.astype(jnp.bfloat16), "tp")
    down_grad = send_down(hidden, cotangent)
    return (input_grad, down_grad)


def kernel(n, tok_hbm, cot_hbm, gate_hbm, up_hbm, down_hbm, dx_out, dg_out,
           tok_ref, cot_ref, gate_ref, up_ref, down_ref, dgacc, weights, tok, cot, ptok, pcot, dxacc, hid, dgp, dgs, dgr, dgf,
           t1s, t1r, t2s, t2r, t3s, t3r, ownr, ybuf, tally,
           sent, w_recv, tk_recv, hid_recv, dg_recv, dgf_recv, t1_recv, t2_recv,
           t3_recv, own_recv, y_recv, local_sem):
    z = lax.axis_index("fs")
    b = lax.axis_index("tp")
    depth, rows = tok_ref.shape
    shard, ff = gate_ref.shape
    chunks = ff // LANES
    parts = t2s.shape[1]
    piece = shard // parts
    half_rows = rows // 2
    core = lax.rem(b, 2)
    col = lax.div(b, 2)
    cx = lax.rem(col, 2)
    cy = lax.div(col, 2)
    side = lax.div(z, 2)
    home = core == side
    away = core != side
    near = jnp.logical_or(z == 1, z == 2)
    end = jnp.logical_not(near)
    zodd = lax.rem(z, 2)
    sib = b + 1 - 2 * core
    bx = b + 2 * (1 - 2 * cx)
    by = b + 4 * (1 - 2 * cy)
    bd = bx + by - b
    last = 2 * col + 1
    lead = core == 1
    zs = z + 1 - 2 * zodd
    zp = 3 - z
    zn = 2 - side
    zf = 3 - 3 * side
    me = jnp.where(home, 0, 1)
    col_x = 2 * cy + 1 - cx
    col_y = 2 * (1 - cy) + cx
    col_d = 2 * (1 - cy) + 1 - cx

    for src, dst, i in ((tok_hbm, tok_ref, 0), (cot_hbm, cot_ref, 0), (gate_hbm, gate_ref, 1),
                        (up_hbm, up_ref, 1), (down_hbm, down_ref, 1)):
        pltpu.make_async_copy(src, dst, local_sem.at[i]).start()

    def drain(ref, sem):
        pltpu.make_async_copy(ref, ref, sem).wait()

    barrier = pltpu.get_barrier_semaphore()

    def greet(fs, tp):
        pl.semaphore_signal(barrier, inc=1, device_id={"fs": fs, "tp": tp},
                            device_id_type=pl.DeviceIdType.MESH)

    greet(z, sib)
    greet(z, bx)
    greet(z, by)
    greet(z, bd)
    for step in range(1, n):
        greet(lax.rem(z + step, n), b)
        greet(lax.rem(z + step, n), sib)
    pl.semaphore_wait(barrier, 4 + 2 * (n - 1))
    drain(tally.at[pl.ds(0, 2 * depth)], local_sem.at[0])
    drain(weights.at[pl.ds(0, shard)], local_sem.at[1])

    def remote(src, dst, send, recv, fs, tp):
        return pltpu.make_async_remote_copy(
            src_ref=src, dst_ref=dst, send_sem=send, recv_sem=recv,
            device_id={"fs": fs, "tp": tp}, device_id_type=pl.DeviceIdType.MESH)

    def rows_of(k, count=1):
        return pl.ds(pl.multiple_of(k * shard, SUB), count * shard)

    def slot(c, k, kind):
        return weights.at[rows_of(k), pl.ds((3 * c + kind) * LANES, LANES)]

    def own(c, kind):
        return (gate_ref, up_ref, down_ref)[kind].at[:, pl.ds(c * LANES, LANES)]

    def w_copy(src, c, k, kind, i, fs):
        return remote(src, slot(c, k, kind), sent.at[0], w_recv.at[c, i, kind], fs, b)

    def sib_copy(src, c, k, kind):
        return remote(src, slot(c, k, kind), sent.at[1], w_recv.at[c, 0, 0], z, sib)

    def local_copy(c, kind):
        return pltpu.make_async_copy(own(c, kind), slot(c, z, kind), local_sem.at[2])

    every = [(c, kind) for c in range(chunks) for kind in range(3)]
    mine_q = rows_of(col)
    far_rows = rows_of(2 * side, 2)

    def tk_copy(i, src, dst, fs, tp):
        return remote(src, dst, sent.at[2], tk_recv.at[i], fs, tp)

    tok_hop = tk_copy(0, tok_ref.at[mine_q], ptok.at[mine_q], zp, b)
    cot_hop = tk_copy(1, cot_ref.at[mine_q], pcot.at[mine_q], zp, sib)

    def spread(i, buf, q, tp):
        return tk_copy(i, buf.at[rows_of(q)], buf.at[rows_of(q)], z, tp)

    give = tk_copy(8, pcot.at[far_rows], pcot.at[far_rows], z, sib)

    @pl.when(home)
    def _():
        tok_hop.start()
        for c, kind in every:
            w_copy(own(c, kind), c, z, kind, 0, zs).start()
            sib_copy(own(c, kind), c, z, kind).start()
            local_copy(c, kind).start()
        tok[...] = tok_ref[...].T
        cot[...] = cot_ref[...].T

    @pl.when(away)
    def _():
        cot_hop.start()
        for c, kind in every:
            w_copy(own(c, kind), c, z, kind, jnp.where(near, 1, 2), zn).start()
        tok_hop.wait_recv()
        spread(2, ptok, col, bx).start()
        spread(3, ptok, col, by).start()
        cot_hop.wait_recv()
        spread(4, pcot, col, bx).start()
        spread(5, pcot, col, by).start()
        spread(2, ptok, col_x, bx).wait_recv()
        spread(6, ptok, col_x, by).start()
        spread(5, pcot, col_y, by).wait_recv()
        spread(7, pcot, col_y, bx).start()
        spread(3, ptok, col_y, by).wait_recv()
        spread(6, ptok, col_d, by).wait_recv()
        tok[...] = ptok[...].T
        spread(4, pcot, col_x, bx).wait_recv()
        spread(7, pcot, col_d, bx).wait_recv()
        give.start()
        cot[...] = pcot[...].T

    others = (zs, zn, zf)

    def gather(c):
        @pl.when(home)
        def _():
            for kind in range(3):
                for i, k in enumerate(others):
                    w_copy(slot(c, k, kind), c, k, kind, i, zs).wait_recv()
                    if i:
                        @pl.when(near)
                        def _():
                            w_copy(slot(c, k, kind), c, k, kind, i, zs).start()
                    sib_copy(slot(c, k, kind), c, k, kind).start()
            if c == 0:
                drain(weights.at[rows_of(z)], local_sem.at[2])

        @pl.when(away)
        def _():
            drain(weights.at[:, pl.ds(3 * c * LANES, 3 * LANES)], w_recv.at[c, 0, 0])

    def hid_copy(c):
        return remote(hid.at[me, c], hid.at[me, c], sent.at[3], hid_recv.at[c], z, sib)

    def dg_home(c):
        return remote(dgs.at[c, 0], dgr.at[c, 0], sent.at[4], dg_recv.at[c], zs, b)

    def dg_away(c):
        return remote(dgs.at[c], dgr.at[c], sent.at[4], dg_recv.at[c], zs, b)

    def dg_far(c, i):
        return remote(dgs.at[c, i], dgf.at[c], sent.at[4], dgf_recv.at[c],
                      2 * (1 - side) + i, sib)

    def lanes_of(c):
        return pl.ds(c * LANES, LANES)

    def down_part(c):
        hid_copy(c).wait_recv()
        for i in range(2):
            k = rows_of(2 * core + i)
            value = (jnp.dot(cot_ref[k, :], hid[0, c], preferred_element_type=F32)
                     + jnp.dot(pcot[k, :], hid[1, c], preferred_element_type=F32))

            @pl.when(jnp.logical_and(home, zodd == i))
            def _():
                dgacc[:, lanes_of(c)] = value

            @pl.when(jnp.logical_and(home, zodd != i))
            def _():
                dgs[c, 0] = value.astype(BF16)

            @pl.when(jnp.logical_and(away, near))
            def _():
                dgp[c, i] = value

            @pl.when(jnp.logical_and(away, end))
            def _():
                dgs[c, i] = value.astype(BF16)

        @pl.when(home)
        def _():
            dg_home(c).start()

        @pl.when(jnp.logical_and(away, end))
        def _():
            dg_away(c).start()

    def down_mid(c):
        @pl.when(jnp.logical_and(away, near))
        def _():
            dg_away(c).wait_recv()
            for i in range(2):
                dgs[c, i] = (dgp[c, i] + dgr[c, i].astype(F32)).astype(BF16)
                dg_far(c, i).start()

    def down_final(c):
        @pl.when(home)
        def _():
            dg_home(c).wait_recv()
            dgacc[:, lanes_of(c)] += dgr[c, 0].astype(F32)

        @pl.when(away)
        def _():
            dg_far(c, 0).wait_recv()
            dgacc[:, lanes_of(c)] = dgf[c].astype(F32)

    low, high = slice(0, half_rows), slice(half_rows, rows)
    halves = (low, high)

    def t1_copy(i, step):
        return remote(t1s.at[i, step], t1r.at[i, step], sent.at[5], t1_recv.at[i, step],
                      z, bx if i == 0 else by)

    def t2_copy(i, q):
        return remote(t2s.at[i, q], t2r.at[i, q], sent.at[6], t2_recv.at[i, q],
                      z, by if i == 0 else bx)

    def t3_copy(q):
        return remote(t3s.at[q], t3r.at[q], sent.at[7], t3_recv.at[q], zp, last)

    def strip(k, q):
        return pl.ds(pl.multiple_of(k * shard + q * piece, SUB), piece)

    def own_copy(q):
        return remote(dxacc.at[strip(col, q)], ownr.at[q], sent.at[7], own_recv.at[q], z, sib)

    def y_copy(i, k, q, tp):
        ref = ybuf.at[strip(k, q)]
        return remote(ref, ref, sent.at[8], y_recv.at[i, q], z, tp)

    def y_sib(i, k, q):
        ref = ybuf.at[strip(k, q)]
        return remote(ref, ref, sent.at[9], y_recv.at[i, q], z, sib)

    def put(k, q):
        r = strip(k, q)
        return pltpu.make_async_copy(ybuf.at[r], dx_out.at[r], local_sem.at[3])

    dg_put = pltpu.make_async_copy(dgacc, dg_out, local_sem.at[4])

    for c in range(chunks):
        gather(c)
        w = weights[:, 3 * c * LANES:(3 * c + 2) * LANES]
        pre = jnp.dot(tok[...], w, preferred_element_type=F32)
        hg = jnp.dot(cot[...], weights[:, (3 * c + 2) * LANES:(3 * c + 3) * LANES],
                     preferred_element_type=F32)
        gate_pre, up_pre = pre[:, :LANES], pre[:, LANES:]
        sig = jax.nn.sigmoid(gate_pre)
        act = gate_pre * sig
        hid[me, c] = (act * up_pre).astype(BF16)
        hid_copy(c).start()
        dgu = jnp.concatenate(
            [(hg * up_pre * sig * (1.0 + gate_pre * (1.0 - sig))).astype(BF16),
             (hg * act).astype(BF16)], axis=1)
        if c == 0:
            dxacc[...] = contract_cols(w, dgu)
        elif c < chunks - 1:
            dxacc[...] += contract_cols(w, dgu)
        if c:
            @pl.when(end)
            def _():
                if c == 1:
                    @pl.when(home)
                    def _():
                        give.wait_recv()
                down_part(c - 1)
        if c == chunks - 1:
            for k, sends in ((col_d, ((0, 0), (1, 0))), (col_x, ((0, 1),)), (col_y, ((1, 1),)), (col, ())):
                r = rows_of(k)
                value = contract_cols(weights[r, 3 * c * LANES:(3 * c + 2) * LANES], dgu)
                if c:
                    value = value + dxacc[r, :]
                if k is not col_d:
                    dxacc[r, :] = value
                for i, step in sends:
                    t1s[i, step] = value[:, halves[i]].astype(BF16)
                    t1_copy(i, step).start()

    @pl.when(end)
    def _():
        if chunks == 1:
            @pl.when(home)
            def _():
                give.wait_recv()
        down_part(chunks - 1)

    @pl.when(near)
    def _():
        @pl.when(home)
        def _():
            give.wait_recv()
        for c in range(chunks):
            down_part(c)
    t1_copy(0, 0).wait_recv()
    t1_copy(1, 0).wait_recv()
    for q in range(parts):
        inner = slice(q * piece, (q + 1) * piece)
        for i, k in ((0, col_y), (1, col_x)):
            t2s[i, q] = (dxacc[strip(k, q), halves[i]] + t1r[i, 0, inner].astype(F32)).astype(BF16)
            t2_copy(i, q).start()
    t1_copy(0, 1).wait_recv()
    t1_copy(1, 1).wait_recv()
    for q in range(parts):
        inner = slice(q * piece, (q + 1) * piece)
        for i in range(2):
            dxacc[strip(col, q), halves[i]] += t1r[i, 1, inner].astype(F32)
    for q in range(parts):
        for i in range(2):
            t2_copy(i, q).wait_recv()
            dxacc[strip(col, q), halves[i]] += t2r[i, q].astype(F32)

        @pl.when(away)
        def _():
            t3s[q] = dxacc[strip(col, q), :].astype(BF16)
            t3_copy(q).start()

        @pl.when(jnp.logical_and(home, core == 0))
        def _():
            own_copy(q).start()

    for c in range(chunks):
        down_mid(c)

    places = (col, col_x, col_y, col_d)

    @pl.when(lead)
    def _():
        for q in range(parts):
            t3_copy(q).wait_recv()

            @pl.when(home)
            def _():
                ybuf[strip(col, q), :] = (dxacc[strip(col, q), :] + t3r[q].astype(F32)).astype(BF16)

            @pl.when(away)
            def _():
                own_copy(q).wait_recv()
                ybuf[strip(col, q), :] = (ownr[q] + t3r[q].astype(F32)).astype(BF16)

            y_copy(2, col, q, bd).start()
            y_copy(0, col, q, bx).start()
            y_copy(1, col, q, by).start()
            y_sib(0, col, q).start()
            put(col, q).start()
        for q in range(parts):
            for i, k, tp in ((0, col_x, bx), (1, col_y, by), (2, col_d, bd)):
                y_copy(i, k, q, tp).wait_recv()
                y_sib(i + 1, k, q).start()
                put(k, q).start()

    for c in range(chunks):
        down_final(c)
    dg_put.start()

    @pl.when(core == 0)
    def _():
        for q in range(parts):
            for i, k in enumerate(places):
                y_sib(i, k, q).wait_recv()
                put(k, q).start()

    @pl.when(lead)
    def _():
        drain(ybuf.at[pl.ds(0, 3 * shard)], sent.at[8])
        drain(ybuf, sent.at[9])

    @pl.when(home)
    def _():
        drain(ybuf.at[pl.ds(0, shard)], sent.at[2])
        drain(weights, sent.at[1])
        drain(dgs.at[:, 0], sent.at[4])

        @pl.when(near)
        def _():
            drain(weights.at[pl.ds(0, 3 * shard)], sent.at[0])

        @pl.when(end)
        def _():
            drain(weights.at[pl.ds(0, shard)], sent.at[0])

        @pl.when(core == 0)
        def _():
            drain(ownr, sent.at[7])

    @pl.when(away)
    def _():
        drain(weights.at[pl.ds(0, shard)], sent.at[0])
        drain(tally, sent.at[2])
        drain(dgs, sent.at[4])
        drain(t3s, sent.at[7])

    drain(hid.at[0], sent.at[3])
    drain(t1s, sent.at[5])
    drain(t2s, sent.at[6])
    drain(ybuf, local_sem.at[3])
    dg_put.wait()


def per_device_kernel(n, tokens, cotangent, gate_weight, up_weight, down_weight):
    rows, depth = tokens.shape
    shard, ff = gate_weight.shape
    chunks = ff // LANES
    parts = next(p for p in (3, 2, 1) if shard % (p * SUB) == 0)
    piece = shard // parts
    vmem = pl.BlockSpec(memory_space=pltpu.VMEM)
    dma = pltpu.SemaphoreType.DMA
    dx, dg = pl.pallas_call(
        functools.partial(kernel, n),
        out_shape=(pltpu.VMEM((depth, rows), BF16), pltpu.VMEM((shard, ff), F32)),
        in_specs=[pl.BlockSpec(memory_space=pltpu.HBM)] * 5,
        out_specs=[pl.BlockSpec(memory_space=pl.ANY)] * 2,
        scratch_shapes=[
            pltpu.VMEM((depth, rows), BF16),
            pltpu.VMEM((depth, rows), BF16),
            pltpu.VMEM((shard, ff), BF16),
            pltpu.VMEM((shard, ff), BF16),
            pltpu.VMEM((shard, ff), BF16),
            pltpu.VMEM((shard, ff), F32),
            pltpu.VMEM((depth, 3 * ff), BF16),
            pltpu.VMEM((rows, depth), BF16),
            pltpu.VMEM((rows, depth), BF16),
            pltpu.VMEM((depth, rows), BF16),
            pltpu.VMEM((depth, rows), BF16),
            pltpu.VMEM((depth, rows), F32),
            pltpu.VMEM((2, chunks, rows, LANES), BF16),
            pltpu.VMEM((chunks, 2, shard, LANES), F32),
            pltpu.VMEM((chunks, 2, shard, LANES), BF16),
            pltpu.VMEM((chunks, 2, shard, LANES), BF16),
            pltpu.VMEM((chunks, shard, LANES), BF16),
            pltpu.VMEM((2, 2, shard, rows // 2), BF16),
            pltpu.VMEM((2, 2, shard, rows // 2), BF16),
            pltpu.VMEM((2, parts, piece, rows // 2), BF16),
            pltpu.VMEM((2, parts, piece, rows // 2), BF16),
            pltpu.VMEM((parts, piece, rows), BF16),
            pltpu.VMEM((parts, piece, rows), BF16),
            pltpu.VMEM((parts, piece, rows), F32),
            pltpu.VMEM((depth, rows), BF16),
            pltpu.VMEM((9 * shard, rows), BF16),
            dma((10,)), dma((chunks, 3, 3)), dma((9,)), dma((chunks,)), dma((chunks,)),
            dma((chunks,)), dma((2, 2)), dma((2, parts)), dma((parts,)), dma((parts,)),
            dma((4, parts)), dma((5,)),
        ],
        compiler_params=pltpu.CompilerParams(
            collective_id=0, has_side_effects=True, vmem_limit_bytes=28 * 2**20),
    )(*(pltpu.with_memory_space_constraint(a, pltpu.HBM) for a in (
        tokens.T, cotangent.T, gate_weight, up_weight, down_weight.T)))
    return dx.T, dg.T


def solution(mesh):
    n, tp = mesh.shape["fs"], mesh.shape["tp"]

    def per_device(tokens, cotangent, gate_weight, up_weight, down_weight):
        rows, depth = tokens.shape
        shard, ff = gate_weight.shape
        args = (tokens, cotangent, gate_weight, up_weight, down_weight)
        fits = (tp == 8 and n == 4 and rows % (2 * LANES) == 0 and rows <= 512
                and depth == n * shard and shard % SUB == 0 and ff % LANES == 0 and ff <= 512)
        return per_device_kernel(n, *args) if fits else per_device_plain(*args)

    placed = (P("fs", None), P("fs", None), P("fs", "tp"), P("fs", "tp"), P("tp", "fs"))
    return jax.shard_map(
        per_device,
        mesh=mesh,
        in_specs=placed,
        out_specs=(P("fs", None), P("tp", "fs")),
        check_vma=False,
    )
```

```python
import functools

import jax
import jax.numpy as jnp
from jax import lax
from jax.experimental import pallas as pl
from jax.experimental.pallas import tpu as pltpu
from jax.sharding import PartitionSpec as P

LANES = 128
SUB = 16
BF16 = jnp.bfloat16
F32 = jnp.float32


def contract_rows(left, right):
    return lax.dot_general(
        left, right, (((0,), (0,)), ((), ())), preferred_element_type=jnp.float32
    )


def contract_cols(left, right):
    return lax.dot_general(
        left, right, (((1,), (1,)), ((), ())), preferred_element_type=jnp.float32
    )


def send_down(hidden, cotangent):
    return lax.psum_scatter(
        contract_rows(cotangent, hidden), "fs", scatter_dimension=0, tiled=True
    ).T


def per_device_plain(tokens, cotangent, gate_weight, up_weight, down_weight):
    whole_gate, whole_up, whole_down = (
        lax.all_gather(gate_weight, "fs", axis=0, tiled=True),
        lax.all_gather(up_weight, "fs", axis=0, tiled=True),
        lax.all_gather(down_weight, "fs", axis=1, tiled=True),
    )
    gate_pre = jnp.dot(tokens, whole_gate, preferred_element_type=jnp.float32)
    up_pre = jnp.dot(tokens, whole_up, preferred_element_type=jnp.float32)
    hidden_grad = contract_cols(cotangent, whole_down)
    sigmoid_gate = jax.nn.sigmoid(gate_pre)
    activated = gate_pre * sigmoid_gate
    hidden = (activated * up_pre).astype(jnp.bfloat16)
    gate_pre_grad = (
        hidden_grad * up_pre * sigmoid_gate * (1.0 + gate_pre * (1.0 - sigmoid_gate))
    ).astype(jnp.bfloat16)
    up_pre_grad = (hidden_grad * activated).astype(jnp.bfloat16)
    partial_value = contract_cols(gate_pre_grad, whole_gate) + contract_cols(up_pre_grad, whole_up)
    input_grad = lax.psum(partial_value.astype(jnp.bfloat16), "tp")
    down_grad = send_down(hidden, cotangent)
    return (input_grad, down_grad)


def kernel(n, tok_hbm, cot_hbm, gate_hbm, up_hbm, down_hbm, dx_out, dg_out,
           tok_ref, cot_ref, gate_ref, up_ref, down_ref, weights, tok, cot,
           ptok, pcot, etok, ecot, dxacc, hid, dgacc, dgs, dgr,
           t1s, t1r, t2s, t2r, t3s, t3r, ownr, ybuf, tally,
           sent, w_recv, tk_recv, hid_recv, dg_recv, t1_recv, t2_recv,
           t3_recv, own_recv, y_recv, local_sem):
    z = lax.axis_index("fs")
    b = lax.axis_index("tp")
    depth, rows = tok_ref.shape
    shard, ff = gate_ref.shape
    chunks = ff // LANES
    parts, piece = t2s.shape[2], t2s.shape[3]
    half_rows = rows // 2
    core = lax.rem(b, 2)
    col = lax.div(b, 2)
    cx = lax.rem(col, 2)
    cy = lax.div(col, 2)
    side = lax.div(z, 2)
    zodd = lax.rem(z, 2)
    home = core == side
    away = core != side
    near = side != zodd
    end = side == zodd
    lead = core == 1
    sib = b + 1 - 2 * core
    bx = b + 2 * (1 - 2 * cx)
    by = b + 4 * (1 - 2 * cy)
    bd = bx + by - b
    last = 2 * col + 1
    zs = z + 1 - 2 * zodd
    zn = 2 - side
    zf = 3 - 3 * side
    me = jnp.where(home, 0, 1)
    col_x = 2 * cy + 1 - cx
    col_y = 2 * (1 - cy) + cx
    col_d = 2 * (1 - cy) + 1 - cx
    for src, dst, i in ((tok_hbm, tok_ref, 0), (cot_hbm, cot_ref, 0), (gate_hbm, gate_ref, 1),
                        (up_hbm, up_ref, 1), (down_hbm, down_ref, 1)):
        pltpu.make_async_copy(src, dst, local_sem.at[i]).start()

    def drain(ref, sem):
        pltpu.make_async_copy(ref, ref, sem).wait()

    barrier = pltpu.get_barrier_semaphore()

    def greet(fs, tp):
        pl.semaphore_signal(barrier, inc=1, device_id={"fs": fs, "tp": tp},
                            device_id_type=pl.DeviceIdType.MESH)

    greet(z, sib)
    greet(z, bx)
    greet(z, by)
    greet(z, bd)
    for step in range(1, n):
        greet(lax.rem(z + step, n), b)
        greet(lax.rem(z + step, n), sib)
    pl.semaphore_wait(barrier, 4 + 2 * (n - 1))
    drain(tally.at[pl.ds(0, 2 * depth)], local_sem.at[0])
    drain(weights.at[pl.ds(0, shard)], local_sem.at[1])

    def remote(src, dst, send, recv, fs, tp):
        return pltpu.make_async_remote_copy(
            src_ref=src, dst_ref=dst, send_sem=send, recv_sem=recv,
            device_id={"fs": fs, "tp": tp}, device_id_type=pl.DeviceIdType.MESH)

    def rows_of(k, count=1):
        return pl.ds(pl.multiple_of(k * shard, SUB), count * shard)

    def lanes_of(c, count=1):
        return pl.ds(c * LANES, count * LANES)

    def slot(c, k, kind):
        return weights.at[rows_of(k), lanes_of(3 * c + kind)]

    def own(c, kind):
        return (gate_ref, up_ref, down_ref)[kind].at[:, lanes_of(c)]

    def w_copy(c, k, kind, i, fs):
        return remote(own(c, kind), slot(c, k, kind), sent.at[0], w_recv.at[c, i, kind], fs, b)

    def sib_copy(src, c, k, kind):
        return remote(src, slot(c, k, kind), sent.at[1], w_recv.at[c, 0, 0], z, sib)

    every = [(c, kind) for c in range(chunks) for kind in range(3)]
    others = (zs, zn, zf)
    mine_q = rows_of(col)

    def tk_copy(i, src, dst, fs, tp):
        return remote(src, dst, sent.at[2], tk_recv.at[i], fs, tp)

    def tok_buf(e):
        return etok if e else ptok

    def cot_buf(e):
        return ecot.at[me] if e else pcot

    def spread(i, e, q, tp):
        buf = cot_buf(e) if i in (1, 4, 5, 7) else tok_buf(e)
        ref = buf.at[rows_of(q)]
        return tk_copy(8 * e + i, ref, ref, z, tp)

    def spread_first(e):
        spread(0, e, col, bx).wait_recv()
        spread(2, e, col, bx).start()
        spread(3, e, col, by).start()
        spread(1, e, col, bx).wait_recv()
        spread(4, e, col, bx).start()
        spread(5, e, col, by).start()

    def spread_second(e):
        spread(2, e, col_x, bx).wait_recv()
        spread(6, e, col_x, by).start()
        spread(5, e, col_y, by).wait_recv()
        spread(7, e, col_y, bx).start()

    def spread_rest(e):
        spread(3, e, col_y, by).wait_recv()
        spread(6, e, col_d, by).wait_recv()
        spread(4, e, col_x, bx).wait_recv()
        spread(7, e, col_d, bx).wait_recv()

    far_rows = rows_of(2 * (1 - core), 2)
    give = tk_copy(16, pcot.at[far_rows], pcot.at[far_rows], z, sib)
    give_extra = tk_copy(17, ecot.at[me, far_rows], ecot.at[me, far_rows], z, sib)
    take_extra = tk_copy(17, ecot.at[1 - me, far_rows], ecot.at[1 - me, far_rows], z, sib)
    @pl.when(jnp.logical_and(end, home))
    def _():
        tk_copy(8, tok_ref.at[mine_q], etok.at[mine_q], zn, b).start()
        tk_copy(8, tok_ref.at[mine_q], etok.at[mine_q], zs, b).start()
        for c, kind in every:
            w_copy(c, z, kind, 0, zs).start()

    @pl.when(jnp.logical_and(end, away))
    def _():
        tk_copy(9, cot_ref.at[mine_q], ecot.at[1, mine_q], zn, sib).start()
        tk_copy(9, cot_ref.at[mine_q], ecot.at[0, mine_q], zs, sib).start()
        for c, kind in every:
            w_copy(c, z, kind, 2, zn).start()

    @pl.when(jnp.logical_and(near, home))
    def _():
        tk_copy(0, tok_ref.at[mine_q], ptok.at[mine_q], zn, b).start()
        for c, kind in every:
            sib_copy(own(c, kind), c, z, kind).start()
            pltpu.make_async_copy(own(c, kind), slot(c, z, kind), local_sem.at[2]).start()
        tok[0] = tok_ref[...].T
        cot[0] = cot_ref[...].T
        spread_first(1)
        spread_second(1)

    @pl.when(jnp.logical_and(near, away))
    def _():
        tk_copy(1, cot_ref.at[mine_q], pcot.at[mine_q], zn, sib).start()
        for c, kind in every:
            w_copy(c, z, kind, 1, zn).start()
        spread_first(0)
        spread_first(1)
        spread_second(0)
        spread_second(1)
        spread_rest(0)
        give.start()
        tok[0] = ptok[...].T
        cot[0] = pcot[...].T

    def gather(c):
        @pl.when(home)
        def _():
            for kind in range(3):
                for i, k in enumerate(others):
                    w_copy(c, k, kind, i, zs).wait_recv()
                    sib_copy(slot(c, k, kind), c, k, kind).start()
            if c == 0:
                drain(weights.at[rows_of(z)], local_sem.at[2])

        @pl.when(away)
        def _():
            drain(weights.at[:, lanes_of(3 * c, 3)], w_recv.at[c, 0, 0])

    def hid_copy(e, c):
        ref = hid.at[e, me, :, lanes_of(c)]
        return remote(ref, ref, sent.at[3], hid_recv.at[e, c], z, sib)

    def activate(e, c):
        pre = jnp.dot(tok[e], weights[:, 3 * c * LANES:(3 * c + 2) * LANES],
                      preferred_element_type=F32)
        hg = jnp.dot(cot[e], weights[:, (3 * c + 2) * LANES:(3 * c + 3) * LANES],
                     preferred_element_type=F32)
        gate_pre, up_pre = pre[:, :LANES], pre[:, LANES:]
        sig = jax.nn.sigmoid(gate_pre)
        act = gate_pre * sig
        hid[e, me, :, lanes_of(c)] = (act * up_pre).astype(BF16)
        hid_copy(e, c).start()
        return jnp.concatenate(
            [(hg * up_pre * sig * (1.0 + gate_pre * (1.0 - sig))).astype(BF16),
             (hg * act).astype(BF16)], axis=1)

    def work(e, c):
        dgu = activate(e, c)
        value = contract_cols(weights[:, 3 * c * LANES:(3 * c + 2) * LANES], dgu)
        if c == 0:
            dxacc[e] = value
        else:
            dxacc[e] += value

    halves = (slice(0, half_rows), slice(half_rows, rows))

    def t1_copy(e, i, step):
        return remote(t1s.at[e, i, step], t1r.at[e, i, step], sent.at[5], t1_recv.at[e, i, step],
                      z, bx if i == 0 else by)

    def t2_copy(e, i, q):
        return remote(t2s.at[e, i, q], t2r.at[e, i, q], sent.at[6], t2_recv.at[e, i, q],
                      z, by if i == 0 else bx)

    def t3_copy(e, i, q, fs):
        return remote(t3s.at[e, q], t3r.at[i, q], sent.at[7], t3_recv.at[i, q], fs, last)

    def strip(k, q):
        return pl.ds(pl.multiple_of(k * shard + q * piece, SUB), piece)

    def own_copy(q):
        return remote(dxacc.at[0, strip(col, q)], ownr.at[q], sent.at[10], own_recv.at[q], z, sib)

    def work_last(e, c, at_once):
        dgu = activate(e, c)
        for k, sends in ((col_d, ((0, 0), (1, 0))), (col_x, ((0, 1),)), (col_y, ((1, 1),)), (col, ())):
            r = rows_of(k)
            value = contract_cols(weights[r, 3 * c * LANES:(3 * c + 2) * LANES], dgu)
            if c:
                value = value + dxacc[e, r, :]
            if k is not col_d:
                dxacc[e, r, :] = value
            for i, step in sends:
                t1s[e, i, step] = value[:, halves[i]].astype(BF16)
                if at_once:
                    t1_copy(e, i, step).start()

    def second_step(e):
        t1_copy(e, 0, 0).wait_recv()
        t1_copy(e, 1, 0).wait_recv()
        for q in range(parts):
            inner = slice(q * piece, (q + 1) * piece)
            for i, k in ((0, col_y), (1, col_x)):
                t2s[e, i, q] = (dxacc[e, strip(k, q), halves[i]]
                                + t1r[e, i, 0, inner].astype(F32)).astype(BF16)
                t2_copy(e, i, q).start()

    def collect(e):
        t1_copy(e, 0, 1).wait_recv()
        t1_copy(e, 1, 1).wait_recv()
        for q in range(parts):
            inner = slice(q * piece, (q + 1) * piece)
            for i in range(2):
                dxacc[e, strip(col, q), halves[i]] += t1r[e, i, 1, inner].astype(F32)

    def arrive(e, q):
        for i in range(2):
            t2_copy(e, i, q).wait_recv()
            dxacc[e, strip(col, q), halves[i]] += t2r[e, i, q].astype(F32)

    def dg_send(i, fs, tp):
        return remote(dgs.at[i], dgr, sent.at[4], dg_recv.at[0], fs, tp)

    def down_parts():
        @pl.when(home)
        def _():
            give.wait_recv()
        take_extra.wait_recv()
        for e in range(2):
            for c in range(chunks):
                remote(hid.at[e, 1 - me, :, lanes_of(c)], hid.at[e, 1 - me, :, lanes_of(c)],
                       sent.at[3], hid_recv.at[e, c], z, sib).wait_recv()
        for i in range(2):
            k = rows_of(2 * core + i)
            value = (jnp.dot(cot_ref[k, :], hid[0, 0], preferred_element_type=F32)
                     + jnp.dot(pcot[k, :], hid[0, 1], preferred_element_type=F32)
                     + jnp.dot(ecot[0, k, :], hid[1, 0], preferred_element_type=F32)
                     + jnp.dot(ecot[1, k, :], hid[1, 1], preferred_element_type=F32))

            @pl.when(jnp.logical_and(home, zodd == i))
            def _():
                dgacc[...] = value

            @pl.when(jnp.logical_and(home, zodd != i))
            def _():
                dgs[0] = value.astype(BF16)

            @pl.when(away)
            def _():
                dgs[i] = value.astype(BF16)

    def down_sends():
        @pl.when(home)
        def _():
            dg_send(0, zs, b).start()

        @pl.when(away)
        def _():
            for i in range(2):
                dg_send(i, 2 * (1 - side) + i, sib).start()
    @pl.when(near)
    def _():
        for c in range(chunks - 1):
            gather(c)
            work(0, c)
        spread_rest(1)
        give_extra.start()
        tok[1] = etok[...].T
        cot[1] = ecot[me].T
        for c in range(chunks - 1):
            work(1, c)
        gather(chunks - 1)
        work_last(1, chunks - 1, True)
        work_last(0, chunks - 1, False)
        down_parts()
        second_step(1)
        for i, step in ((0, 0), (1, 0), (0, 1), (1, 1)):
            t1_copy(0, i, step).start()
        collect(1)
        for q in range(parts):
            arrive(1, q)
            t3s[1, q] = dxacc[1, strip(col, q), :].astype(BF16)

            @pl.when(home)
            def _():
                t3_copy(1, 0, q, zs).start()

            @pl.when(away)
            def _():
                t3_copy(1, 1, q, zf).start()
        down_sends()
        second_step(0)
        collect(0)
        for q in range(parts):
            arrive(0, q)

            @pl.when(away)
            def _():
                t3s[0, q] = dxacc[0, strip(col, q), :].astype(BF16)
                t3_copy(0, 0, q, zn).start()

            @pl.when(jnp.logical_and(home, core == 0))
            def _():
                own_copy(q).start()

    def y_copy(i, k, q, tp):
        ref = ybuf.at[strip(k, q)]
        return remote(ref, ref, sent.at[8], y_recv.at[i, q], z, tp)

    def y_sib(i, k, q):
        ref = ybuf.at[strip(k, q)]
        return remote(ref, ref, sent.at[9], y_recv.at[i, q], z, sib)

    def put(k, q):
        r = strip(k, q)
        return pltpu.make_async_copy(ybuf.at[r], dx_out.at[r], local_sem.at[3])

    dg_put = pltpu.make_async_copy(dgacc, dg_out, local_sem.at[4])

    def result(q, value):
        ybuf[strip(col, q), :] = value.astype(BF16)
    @pl.when(lead)
    def _():
        for q in range(parts):
            t3_copy(0, 0, q, zn).wait_recv()

            @pl.when(end)
            def _():
                t3_copy(1, 1, q, zn).wait_recv()
                result(q, t3r[0, q].astype(F32) + t3r[1, q].astype(F32))

            @pl.when(jnp.logical_and(near, home))
            def _():
                result(q, dxacc[0, strip(col, q), :] + t3r[0, q].astype(F32))

            @pl.when(jnp.logical_and(near, away))
            def _():
                own_copy(q).wait_recv()
                result(q, ownr[q] + t3r[0, q].astype(F32))

            y_copy(2, col, q, bd).start()
            y_copy(0, col, q, bx).start()
            y_copy(1, col, q, by).start()
            y_sib(0, col, q).start()
            put(col, q).start()
        for q in range(parts):
            for i, k, tp in ((0, col_x, bx), (1, col_y, by), (2, col_d, bd)):
                y_copy(i, k, q, tp).wait_recv()
                y_sib(i + 1, k, q).start()
                put(k, q).start()
    @pl.when(jnp.logical_or(end, away))
    def _():
        dg_send(0, zs, b).wait_recv()
        dgacc[...] = dgr[...].astype(F32)

    dg_put.start()
    @pl.when(core == 0)
    def _():
        for q in range(parts):
            for i, k in enumerate((col, col_x, col_y, col_d)):
                y_sib(i, k, q).wait_recv()
                put(k, q).start()
    @pl.when(lead)
    def _():
        drain(ybuf.at[pl.ds(0, 3 * shard)], sent.at[8])
        drain(ybuf, sent.at[9])

    @pl.when(jnp.logical_or(end, away))
    def _():
        drain(weights.at[pl.ds(0, shard)], sent.at[0])

    @pl.when(end)
    def _():
        drain(tally.at[pl.ds(0, 2 * shard)], sent.at[2])

    @pl.when(near)
    def _():
        drain(hid.at[:, 0], sent.at[3])
        drain(t1s, sent.at[5])
        drain(t2s, sent.at[6])

        @pl.when(home)
        def _():
            drain(weights, sent.at[1])
            drain(tally.at[pl.ds(0, 9 * shard)], sent.at[2])
            drain(dgs.at[0], sent.at[4])
            drain(t3s.at[0], sent.at[7])

            @pl.when(core == 0)
            def _():
                drain(ownr, sent.at[10])

        @pl.when(away)
        def _():
            drain(tally, sent.at[2])
            drain(dgs, sent.at[4])
            drain(t3s, sent.at[7])

    drain(ybuf, local_sem.at[3])
    dg_put.wait()


def per_device_kernel(n, tokens, cotangent, gate_weight, up_weight, down_weight):
    rows, depth = tokens.shape
    shard, ff = gate_weight.shape
    chunks = ff // LANES
    parts = next(p for p in (3, 2, 1) if shard % (p * SUB) == 0)
    piece = shard // parts
    vmem, dma = pltpu.VMEM, pltpu.SemaphoreType.DMA
    dx, dg = pl.pallas_call(
        functools.partial(kernel, n),
        out_shape=(vmem((depth, rows), BF16), vmem((shard, ff), F32)),
        in_specs=[pl.BlockSpec(memory_space=pltpu.HBM)] * 5,
        out_specs=[pl.BlockSpec(memory_space=pl.ANY)] * 2,
        scratch_shapes=[
            vmem((depth, rows), BF16), vmem((depth, rows), BF16),
            vmem((shard, ff), BF16), vmem((shard, ff), BF16), vmem((shard, ff), BF16),
            vmem((depth, 3 * ff), BF16),
            vmem((2, rows, depth), BF16), vmem((2, rows, depth), BF16),
            vmem((depth, rows), BF16), vmem((depth, rows), BF16),
            vmem((depth, rows), BF16), vmem((2, depth, rows), BF16),
            vmem((2, depth, rows), F32),
            vmem((2, 2, rows, ff), BF16),
            vmem((shard, ff), F32), vmem((2, shard, ff), BF16), vmem((shard, ff), BF16),
            vmem((2, 2, 2, shard, rows // 2), BF16), vmem((2, 2, 2, shard, rows // 2), BF16),
            vmem((2, 2, parts, piece, rows // 2), BF16), vmem((2, 2, parts, piece, rows // 2), BF16),
            vmem((2, parts, piece, rows), BF16), vmem((2, parts, piece, rows), BF16),
            vmem((parts, piece, rows), F32),
            vmem((depth, rows), BF16),
            vmem((17 * shard, rows), BF16),
            dma((11,)), dma((chunks, 3, 3)), dma((18,)), dma((2, chunks)), dma((1,)),
            dma((2, 2, 2)), dma((2, 2, parts)), dma((2, parts)), dma((parts,)),
            dma((4, parts)), dma((5,)),
        ],
        compiler_params=pltpu.CompilerParams(
            collective_id=0, has_side_effects=True, vmem_limit_bytes=40 * 2**20),
    )(*(pltpu.with_memory_space_constraint(a, pltpu.HBM) for a in (
        tokens.T, cotangent.T, gate_weight, up_weight, down_weight.T)))
    return dx.T, dg.T


def solution(mesh):
    n, tp = mesh.shape["fs"], mesh.shape["tp"]

    def per_device(tokens, cotangent, gate_weight, up_weight, down_weight):
        rows, depth = tokens.shape
        shard, ff = gate_weight.shape
        args = (tokens, cotangent, gate_weight, up_weight, down_weight)
        fits = (tp == 8 and n == 4 and rows % (2 * LANES) == 0 and rows <= 256
                and depth == n * shard and shard % SUB == 0 and ff % LANES == 0
                and LANES < ff <= 512 and depth <= 2048)
        return per_device_kernel(n, *args) if fits else per_device_plain(*args)

    placed = (P("fs", None), P("fs", None), P("fs", "tp"), P("fs", "tp"), P("tp", "fs"))
    return jax.shard_map(
        per_device,
        mesh=mesh,
        in_specs=placed,
        out_specs=(P("fs", None), P("tp", "fs")),
        check_vma=False,
    )
```

```python
import functools

import jax
import jax.numpy as jnp
from jax import lax
from jax.experimental import pallas as pl
from jax.experimental.pallas import tpu as pltpu
from jax.sharding import PartitionSpec as P

LANES = 128
SUB = 16
BF16 = jnp.bfloat16
F32 = jnp.float32


def contract_rows(left, right):
    return lax.dot_general(
        left, right, (((0,), (0,)), ((), ())), preferred_element_type=jnp.float32
    )


def contract_cols(left, right):
    return lax.dot_general(
        left, right, (((1,), (1,)), ((), ())), preferred_element_type=jnp.float32
    )


def send_down(hidden, cotangent):
    return lax.psum_scatter(
        contract_rows(cotangent, hidden), "fs", scatter_dimension=0, tiled=True
    ).T


def per_device_plain(tokens, cotangent, gate_weight, up_weight, down_weight):
    whole_gate, whole_up, whole_down = (
        lax.all_gather(gate_weight, "fs", axis=0, tiled=True),
        lax.all_gather(up_weight, "fs", axis=0, tiled=True),
        lax.all_gather(down_weight, "fs", axis=1, tiled=True),
    )
    gate_pre = jnp.dot(tokens, whole_gate, preferred_element_type=jnp.float32)
    up_pre = jnp.dot(tokens, whole_up, preferred_element_type=jnp.float32)
    hidden_grad = contract_cols(cotangent, whole_down)
    sigmoid_gate = jax.nn.sigmoid(gate_pre)
    activated = gate_pre * sigmoid_gate
    hidden = (activated * up_pre).astype(jnp.bfloat16)
    gate_pre_grad = (
        hidden_grad * up_pre * sigmoid_gate * (1.0 + gate_pre * (1.0 - sigmoid_gate))
    ).astype(jnp.bfloat16)
    up_pre_grad = (hidden_grad * activated).astype(jnp.bfloat16)
    partial_value = contract_cols(gate_pre_grad, whole_gate) + contract_cols(up_pre_grad, whole_up)
    input_grad = lax.psum(partial_value.astype(jnp.bfloat16), "tp")
    down_grad = send_down(hidden, cotangent)
    return (input_grad, down_grad)


def kernel(n, tok_hbm, cot_hbm, gate_hbm, up_hbm, down_hbm, dx_out, dg_out,
           tok_ref, cot_ref, gate_ref, up_ref, down_ref, weights, tok, cot,
           ptok, pcot, etok, ecot, dxacc, hid, dgacc, dgp, dgs, dgr, dgf,
           t1s, t1r, t2s, t2r, t3s, t3r, ownr, ybuf, tally,
           sent, w_recv, tk_recv, hid_recv, dg_recv, dgf_recv, t1_recv, t2_recv,
           t3_recv, own_recv, y_recv, local_sem):
    z = lax.axis_index("fs")
    b = lax.axis_index("tp")
    depth, rows = tok_ref.shape
    shard, ff = gate_ref.shape
    chunks = ff // LANES
    parts, piece = t2s.shape[2], t2s.shape[3]
    half_rows = rows // 2
    core = lax.rem(b, 2)
    col = lax.div(b, 2)
    cx = lax.rem(col, 2)
    cy = lax.div(col, 2)
    side = lax.div(z, 2)
    zodd = lax.rem(z, 2)
    home = core == side
    away = core != side
    near = side != zodd
    end = side == zodd
    lead = core == 1
    sib = b + 1 - 2 * core
    bx = b + 2 * (1 - 2 * cx)
    by = b + 4 * (1 - 2 * cy)
    bd = bx + by - b
    last = 2 * col + 1
    zs = z + 1 - 2 * zodd
    zn = 2 - side
    zf = 3 - 3 * side
    me = jnp.where(home, 0, 1)
    col_x = 2 * cy + 1 - cx
    col_y = 2 * (1 - cy) + cx
    col_d = 2 * (1 - cy) + 1 - cx
    for src, dst, i in ((tok_hbm, tok_ref, 0), (cot_hbm, cot_ref, 0), (gate_hbm, gate_ref, 1),
                        (up_hbm, up_ref, 1), (down_hbm, down_ref, 1)):
        pltpu.make_async_copy(src, dst, local_sem.at[i]).start()

    def drain(ref, sem):
        pltpu.make_async_copy(ref, ref, sem).wait()

    barrier = pltpu.get_barrier_semaphore()

    def greet(fs, tp):
        pl.semaphore_signal(barrier, inc=1, device_id={"fs": fs, "tp": tp},
                            device_id_type=pl.DeviceIdType.MESH)

    greet(z, sib)
    greet(z, bx)
    greet(z, by)
    greet(z, bd)
    for step in range(1, n):
        greet(lax.rem(z + step, n), b)
        greet(lax.rem(z + step, n), sib)
    pl.semaphore_wait(barrier, 4 + 2 * (n - 1))
    drain(tally.at[pl.ds(0, 2 * depth)], local_sem.at[0])
    drain(weights.at[pl.ds(0, shard)], local_sem.at[1])

    def remote(src, dst, send, recv, fs, tp):
        return pltpu.make_async_remote_copy(
            src_ref=src, dst_ref=dst, send_sem=send, recv_sem=recv,
            device_id={"fs": fs, "tp": tp}, device_id_type=pl.DeviceIdType.MESH)

    def rows_of(k, count=1):
        return pl.ds(pl.multiple_of(k * shard, SUB), count * shard)

    def lanes_of(c, count=1):
        return pl.ds(c * LANES, count * LANES)

    def slot(c, k, kind):
        return weights.at[rows_of(k), lanes_of(3 * c + kind)]

    def own(c, kind):
        return (gate_ref, up_ref, down_ref)[kind].at[:, lanes_of(c)]

    def w_copy(src, c, k, kind, i, fs):
        return remote(src, slot(c, k, kind), sent.at[0], w_recv.at[c, i, kind], fs, b)

    def sib_copy(src, c, k, kind):
        return remote(src, slot(c, k, kind), sent.at[1], w_recv.at[c, 0, 0], z, sib)

    every = [(c, kind) for c in range(chunks) for kind in range(3)]
    others = (zs, zn, zf)
    mine_q = rows_of(col)

    def tk_copy(i, src, dst, fs, tp):
        return remote(src, dst, sent.at[2], tk_recv.at[i], fs, tp)

    def tok_buf(e):
        return etok if e else ptok

    def cot_buf(e):
        return ecot if e else pcot

    def spread(i, e, q, tp):
        buf = cot_buf(e) if i in (1, 4, 5, 7) else tok_buf(e)
        ref = buf.at[rows_of(q)]
        return tk_copy(8 * e + i, ref, ref, z, tp)

    def spread_first(e):
        spread(0, e, col, bx).wait_recv()
        spread(2, e, col, bx).start()
        spread(3, e, col, by).start()
        spread(1, e, col, bx).wait_recv()
        spread(4, e, col, bx).start()
        spread(5, e, col, by).start()

    def spread_second(e):
        spread(2, e, col_x, bx).wait_recv()
        spread(6, e, col_x, by).start()
        spread(5, e, col_y, by).wait_recv()
        spread(7, e, col_y, bx).start()

    def spread_rest(e):
        spread(3, e, col_y, by).wait_recv()
        spread(6, e, col_d, by).wait_recv()
        spread(4, e, col_x, bx).wait_recv()
        spread(7, e, col_d, bx).wait_recv()

    far_rows = rows_of(2 * (1 - core), 2)
    give = tk_copy(16, pcot.at[far_rows], pcot.at[far_rows], z, sib)
    give_extra = tk_copy(17, ecot.at[far_rows], ecot.at[far_rows], z, sib)
    half_me = pl.ds(pl.multiple_of(me * half_rows, LANES), half_rows)
    @pl.when(end)
    def _():
        @pl.when(home)
        def _():
            tk_copy(8, tok_ref.at[mine_q], etok.at[mine_q], zn, sib).start()

        @pl.when(away)
        def _():
            tk_copy(9, cot_ref.at[mine_q], ecot.at[mine_q], zn, b).start()

    @pl.when(near)
    def _():
        @pl.when(home)
        def _():
            tk_copy(0, tok_ref.at[mine_q], ptok.at[mine_q], zn, b).start()

        @pl.when(away)
        def _():
            tk_copy(1, cot_ref.at[mine_q], pcot.at[mine_q], zn, sib).start()

    @pl.when(home)
    def _():
        for c, kind in every:
            w_copy(own(c, kind), c, z, kind, 0, zs).start()
            sib_copy(own(c, kind), c, z, kind).start()
            pltpu.make_async_copy(own(c, kind), slot(c, z, kind), local_sem.at[2]).start()

    @pl.when(away)
    def _():
        for c, kind in every:
            w_copy(own(c, kind), c, z, kind, jnp.where(near, 1, 2), zn).start()

    @pl.when(end)
    def _():
        tok[0, :half_rows] = tok_ref[:, half_me].T
        cot[0, :half_rows] = cot_ref[:, half_me].T

    @pl.when(jnp.logical_and(near, home))
    def _():
        tok[0] = tok_ref[...].T
        cot[0] = cot_ref[...].T
        spread_first(1)
        spread_second(1)

    @pl.when(jnp.logical_and(near, away))
    def _():
        spread_first(0)
        spread_second(0)
        spread_rest(0)
        give.start()
        tok[0] = ptok[...].T
        cot[0] = pcot[...].T

    def gather(c):
        @pl.when(home)
        def _():
            for kind in range(3):
                for i, k in enumerate(others):
                    there = slot(c, k, kind)
                    w_copy(there, c, k, kind, i, zs).wait_recv()
                    if i:
                        @pl.when(near)
                        def _():
                            w_copy(there, c, k, kind, i, zs).start()
                    sib_copy(there, c, k, kind).start()
            if c == 0:
                drain(weights.at[rows_of(z)], local_sem.at[2])

        @pl.when(away)
        def _():
            drain(weights.at[:, lanes_of(3 * c, 3)], w_recv.at[c, 0, 0])

    def hid_copy(e, c, ref):
        return remote(ref, ref, sent.at[3], hid_recv.at[e, c], z, sib)

    def hid_ref(e, c):
        return hid.at[2 if e else me, :, lanes_of(c)]

    def hid_half(c):
        return hid.at[0, pl.ds(pl.multiple_of(me * half_rows, SUB), half_rows), lanes_of(c)]

    def activate(x, y, c, out, e):
        pre = jnp.dot(x, weights[:, 3 * c * LANES:(3 * c + 2) * LANES],
                      preferred_element_type=F32)
        hg = jnp.dot(y, weights[:, (3 * c + 2) * LANES:(3 * c + 3) * LANES],
                     preferred_element_type=F32)
        gate_pre, up_pre = pre[:, :LANES], pre[:, LANES:]
        sig = jax.nn.sigmoid(gate_pre)
        act = gate_pre * sig
        out[...] = (act * up_pre).astype(BF16)
        hid_copy(e, c, out).start()
        return jnp.concatenate(
            [(hg * up_pre * sig * (1.0 + gate_pre * (1.0 - sig))).astype(BF16),
             (hg * act).astype(BF16)], axis=1)

    def work(e, c):
        dgu = activate(tok[e], cot[e], c, hid_ref(e, c), e)
        value = contract_cols(weights[:, 3 * c * LANES:(3 * c + 2) * LANES], dgu)
        if c == 0:
            dxacc[e] = value
        else:
            dxacc[e] += value

    def work_half(c):
        dgu = activate(tok[0, :half_rows], cot[0, :half_rows], c, hid_half(c), 0)
        value = contract_cols(weights[:, 3 * c * LANES:(3 * c + 2) * LANES], dgu)
        if c == 0:
            dxacc[0, :, half_me] = value
        else:
            dxacc[0, :, half_me] += value

    halves = (slice(0, half_rows), slice(half_rows, rows))

    def t1_copy(e, i, step):
        return remote(t1s.at[e, i, step], t1r.at[e, i, step], sent.at[5], t1_recv.at[e, i, step],
                      z, bx if i == 0 else by)

    def t2_copy(e, i, q):
        return remote(t2s.at[e, i, q], t2r.at[e, i, q], sent.at[6], t2_recv.at[e, i, q],
                      z, by if i == 0 else bx)

    def t3_copy(q, fs):
        return remote(t3s.at[q], t3r.at[q], sent.at[7], t3_recv.at[q], fs, last)

    def strip(k, q):
        return pl.ds(pl.multiple_of(k * shard + q * piece, SUB), piece)

    def own_copy(q):
        return remote(dxacc.at[0, strip(col, q)], ownr.at[q], sent.at[10], own_recv.at[q], z, sib)

    def work_last(e, c):
        dgu = activate(tok[e], cot[e], c, hid_ref(e, c), e)
        for k, sends in ((col_d, ((0, 0), (1, 0))), (col_x, ((0, 1),)), (col_y, ((1, 1),)), (col, ())):
            r = rows_of(k)
            value = contract_cols(weights[r, 3 * c * LANES:(3 * c + 2) * LANES], dgu) + dxacc[e, r, :]
            if k is not col_d:
                dxacc[e, r, :] = value
            for i, step in sends:
                t1s[e, i, step] = value[:, halves[i]].astype(BF16)
                t1_copy(e, i, step).start()

    first_tp = jnp.where(home, bx, by)
    second_tp = jnp.where(home, by, bx)
    first_col = jnp.where(home, col_x, col_y)
    second_col = jnp.where(home, col_y, col_x)

    def t1_half(step):
        return remote(t1s.at[0, me, step], t1r.at[0, me, step], sent.at[5], t1_recv.at[0, me, step],
                      z, first_tp)

    def t2_half(q):
        return remote(t2s.at[0, me, q], t2r.at[0, me, q], sent.at[6], t2_recv.at[0, me, q],
                      z, second_tp)

    def own_half(q):
        return remote(dxacc.at[0, strip(col, q), half_me], ownr.at[q, :, half_me],
                      sent.at[10], own_recv.at[q], z, sib)

    def last_half(c):
        dgu = activate(tok[0, :half_rows], cot[0, :half_rows], c, hid_half(c), 0)
        for k, step in ((col_d, 0), (first_col, 1), (second_col, 2), (col, 2)):
            r = rows_of(k)
            value = (contract_cols(weights[r, 3 * c * LANES:(3 * c + 2) * LANES], dgu)
                     + dxacc[0, r, half_me])
            if step:
                dxacc[0, r, half_me] = value
            if step < 2:
                t1s[0, me, step] = value.astype(BF16)
                t1_half(step).start()

    def reduce_half():
        t1_half(0).wait_recv()
        for q in range(parts):
            inner = slice(q * piece, (q + 1) * piece)
            t2s[0, me, q] = (dxacc[0, strip(second_col, q), half_me]
                             + t1r[0, me, 0, inner].astype(F32)).astype(BF16)
            t2_half(q).start()
        t1_half(1).wait_recv()
        for q in range(parts):
            inner = slice(q * piece, (q + 1) * piece)
            dxacc[0, strip(col, q), half_me] += t1r[0, me, 1, inner].astype(F32)
        for q in range(parts):
            t2_half(q).wait_recv()
            dxacc[0, strip(col, q), half_me] += t2r[0, me, q].astype(F32)

            @pl.when(core == 0)
            def _():
                own_half(q).start()

    def second_step(e):
        t1_copy(e, 0, 0).wait_recv()
        t1_copy(e, 1, 0).wait_recv()
        for q in range(parts):
            inner = slice(q * piece, (q + 1) * piece)
            for i, k in ((0, col_y), (1, col_x)):
                t2s[e, i, q] = (dxacc[e, strip(k, q), halves[i]]
                                + t1r[e, i, 0, inner].astype(F32)).astype(BF16)
                t2_copy(e, i, q).start()

    def collect(e):
        t1_copy(e, 0, 1).wait_recv()
        t1_copy(e, 1, 1).wait_recv()
        for q in range(parts):
            inner = slice(q * piece, (q + 1) * piece)
            for i in range(2):
                dxacc[e, strip(col, q), halves[i]] += t1r[e, i, 1, inner].astype(F32)

    def arrive(e, q):
        for i in range(2):
            t2_copy(e, i, q).wait_recv()
            dxacc[e, strip(col, q), halves[i]] += t2r[e, i, q].astype(F32)

    stages = (slice(0, ff - LANES), slice(ff - LANES, ff))

    def lanes_at(g):
        return pl.ds(stages[g].start, stages[g].stop - stages[g].start)

    def dg_home(g):
        lanes = lanes_at(g)
        return remote(dgs.at[0, :, lanes], dgr.at[0, :, lanes], sent.at[4], dg_recv.at[g], zs, b)

    def dg_away(g):
        lanes = lanes_at(g)
        return remote(dgs.at[:, :, lanes], dgr.at[:, :, lanes], sent.at[4], dg_recv.at[g], zs, b)

    def dg_far(g, i):
        lanes = lanes_at(g)
        return remote(dgs.at[i, :, lanes], dgf.at[:, lanes], sent.at[4], dgf_recv.at[g],
                      2 * (1 - side) + i, sib)

    def stage_chunks(g):
        return range(chunks - 1) if g == 0 else (chunks - 1,)

    def keep_part(g, i, value):
        lanes = stages[g]

        @pl.when(jnp.logical_and(home, zodd == i))
        def _():
            dgacc[:, lanes] = value

        @pl.when(jnp.logical_and(home, zodd != i))
        def _():
            dgs[0, :, lanes] = value.astype(BF16)

        @pl.when(jnp.logical_and(away, near))
        def _():
            dgp[i, :, lanes] = value

        @pl.when(jnp.logical_and(away, end))
        def _():
            dgs[i, :, lanes] = value.astype(BF16)

    def down_near(g):
        for c in stage_chunks(g):
            hid_copy(0, c, hid.at[1 - me, :, lanes_of(c)]).wait_recv()

            @pl.when(away)
            def _():
                hid_copy(1, c, hid.at[2, :, lanes_of(c)]).wait_recv()
        lanes = stages[g]
        for i in range(2):
            k = rows_of(2 * core + i)
            keep_part(g, i, jnp.dot(cot_ref[k, :], hid[0, :, lanes], preferred_element_type=F32)
                      + jnp.dot(pcot[k, :], hid[1, :, lanes], preferred_element_type=F32)
                      + jnp.dot(ecot[k, :], hid[2, :, lanes], preferred_element_type=F32))

        @pl.when(home)
        def _():
            dg_home(g).start()

    def down_end(g):
        for c in stage_chunks(g):
            other = hid.at[0, pl.ds(pl.multiple_of((1 - me) * half_rows, SUB), half_rows), lanes_of(c)]
            hid_copy(0, c, other).wait_recv()
        for i in range(2):
            k = rows_of(2 * core + i)
            keep_part(g, i, jnp.dot(cot_ref[k, :], hid[0, :, stages[g]], preferred_element_type=F32))

        @pl.when(home)
        def _():
            dg_home(g).start()

        @pl.when(away)
        def _():
            dg_away(g).start()

    def down_mid(g):
        lanes = stages[g]
        dg_away(g).wait_recv()
        for i in range(2):
            dgs[i, :, lanes] = (dgp[i, :, lanes] + dgr[i, :, lanes].astype(F32)).astype(BF16)
            dg_far(g, i).start()
    @pl.when(near)
    def _():
        for c in range(chunks - 1):
            gather(c)
            work(0, c)

        @pl.when(home)
        def _():
            spread_rest(1)
            give_extra.start()
            tok[1] = etok[...].T
            cot[1] = ecot[...].T
            for c in range(chunks - 1):
                work(1, c)
        gather(chunks - 1)

        @pl.when(home)
        def _():
            work_last(1, chunks - 1)
        work_last(0, chunks - 1)

        @pl.when(home)
        def _():
            give.wait_recv()

        @pl.when(away)
        def _():
            give_extra.wait_recv()

        down_near(0)

        @pl.when(away)
        def _():
            down_mid(0)

        down_near(1)

        @pl.when(home)
        def _():
            second_step(1)
            collect(1)
            for q in range(parts):
                arrive(1, q)
                t3s[q] = dxacc[1, strip(col, q), :].astype(BF16)
                t3_copy(q, zf).start()
        second_step(0)
        collect(0)
        for q in range(parts):
            arrive(0, q)

            @pl.when(away)
            def _():
                t3s[q] = dxacc[0, strip(col, q), :].astype(BF16)
                t3_copy(q, zn).start()

            @pl.when(jnp.logical_and(home, core == 0))
            def _():
                own_copy(q).start()

        @pl.when(away)
        def _():
            down_mid(1)

    @pl.when(end)
    def _():
        for c in range(chunks - 1):
            gather(c)
            work_half(c)
        down_end(0)
        gather(chunks - 1)
        last_half(chunks - 1)
        down_end(1)
        reduce_half()

    def y_copy(i, k, q, tp):
        ref = ybuf.at[strip(k, q)]
        return remote(ref, ref, sent.at[8], y_recv.at[i, q], z, tp)

    def y_sib(i, k, q):
        ref = ybuf.at[strip(k, q)]
        return remote(ref, ref, sent.at[9], y_recv.at[i, q], z, sib)

    def put(k, q):
        r = strip(k, q)
        return pltpu.make_async_copy(ybuf.at[r], dx_out.at[r], local_sem.at[3])

    dg_put = pltpu.make_async_copy(dgacc, dg_out, local_sem.at[4])

    def result(q, value):
        ybuf[strip(col, q), :] = value.astype(BF16)
    @pl.when(lead)
    def _():
        for q in range(parts):
            t3_copy(q, zn).wait_recv()

            @pl.when(end)
            def _():
                own_half(q).wait_recv()
                there = pl.ds(pl.multiple_of((1 - me) * half_rows, LANES), half_rows)
                r = strip(col, q)
                ybuf[r, half_me] = (dxacc[0, r, half_me] + t3r[q, :, half_me].astype(F32)).astype(BF16)
                ybuf[r, there] = (ownr[q, :, there] + t3r[q, :, there].astype(F32)).astype(BF16)

            @pl.when(jnp.logical_and(near, home))
            def _():
                result(q, dxacc[0, strip(col, q), :] + t3r[q].astype(F32))

            @pl.when(jnp.logical_and(near, away))
            def _():
                own_copy(q).wait_recv()
                result(q, ownr[q] + t3r[q].astype(F32))
            y_copy(2, col, q, bd).start()
            y_copy(0, col, q, bx).start()
            y_copy(1, col, q, by).start()
            y_sib(0, col, q).start()
            put(col, q).start()
        for q in range(parts):
            for i, k, tp in ((0, col_x, bx), (1, col_y, by), (2, col_d, bd)):
                y_copy(i, k, q, tp).wait_recv()
                y_sib(i + 1, k, q).start()
                put(k, q).start()
    @pl.when(home)
    def _():
        for g in range(2):
            dg_home(g).wait_recv()
        dgacc[...] += dgr[0].astype(F32)

    @pl.when(away)
    def _():
        for g in range(2):
            dg_far(g, 0).wait_recv()
        dgacc[...] = dgf[...].astype(F32)

    dg_put.start()
    @pl.when(core == 0)
    def _():
        for q in range(parts):
            for i, k in enumerate((col, col_x, col_y, col_d)):
                y_sib(i, k, q).wait_recv()
                put(k, q).start()
    @pl.when(lead)
    def _():
        drain(ybuf.at[pl.ds(0, 3 * shard)], sent.at[8])
        drain(ybuf, sent.at[9])

    @pl.when(home)
    def _():
        drain(weights, sent.at[1])
        drain(dgs.at[0], sent.at[4])

    @pl.when(away)
    def _():
        drain(weights.at[pl.ds(0, shard)], sent.at[0])
        drain(dgs, sent.at[4])

    @pl.when(end)
    def _():
        drain(tally.at[pl.ds(0, shard)], sent.at[2])
        drain(hid.at[0, pl.ds(0, half_rows)], sent.at[3])
        drain(t1s.at[0, 0], sent.at[5])
        drain(t2s.at[0, 0], sent.at[6])

        @pl.when(home)
        def _():
            drain(weights.at[pl.ds(0, shard)], sent.at[0])

        @pl.when(core == 0)
        def _():
            drain(ownr.at[:, :, pl.ds(0, half_rows)], sent.at[10])

    @pl.when(near)
    def _():
        drain(tally, sent.at[2])
        drain(t3s, sent.at[7])

        @pl.when(home)
        def _():
            drain(weights.at[pl.ds(0, 3 * shard)], sent.at[0])
            drain(hid.at[pl.ds(0, 2)], sent.at[3])
            drain(t1s, sent.at[5])
            drain(t2s, sent.at[6])

            @pl.when(core == 0)
            def _():
                drain(ownr, sent.at[10])

        @pl.when(away)
        def _():
            drain(hid.at[0], sent.at[3])
            drain(t1s.at[0], sent.at[5])
            drain(t2s.at[0], sent.at[6])

    drain(ybuf, local_sem.at[3])
    dg_put.wait()


def per_device_kernel(n, tokens, cotangent, gate_weight, up_weight, down_weight):
    rows, depth = tokens.shape
    shard, ff = gate_weight.shape
    chunks = ff // LANES
    parts = next(p for p in (3, 2, 1) if shard % (p * SUB) == 0)
    piece = shard // parts
    vmem, dma = pltpu.VMEM, pltpu.SemaphoreType.DMA
    dx, dg = pl.pallas_call(
        functools.partial(kernel, n),
        out_shape=(vmem((depth, rows), BF16), vmem((shard, ff), F32)),
        in_specs=[pl.BlockSpec(memory_space=pltpu.HBM)] * 5,
        out_specs=[pl.BlockSpec(memory_space=pl.ANY)] * 2,
        scratch_shapes=[
            vmem((depth, rows), BF16), vmem((depth, rows), BF16),
            vmem((shard, ff), BF16), vmem((shard, ff), BF16), vmem((shard, ff), BF16),
            vmem((depth, 3 * ff), BF16),
            vmem((2, rows, depth), BF16), vmem((2, rows, depth), BF16),
            vmem((depth, rows), BF16), vmem((depth, rows), BF16),
            vmem((depth, rows), BF16), vmem((depth, rows), BF16),
            vmem((2, depth, rows), F32),
            vmem((3, rows, ff), BF16),
            vmem((shard, ff), F32), vmem((2, shard, ff), F32), vmem((2, shard, ff), BF16),
            vmem((2, shard, ff), BF16), vmem((shard, ff), BF16),
            vmem((2, 2, 2, shard, rows // 2), BF16), vmem((2, 2, 2, shard, rows // 2), BF16),
            vmem((2, 2, parts, piece, rows // 2), BF16), vmem((2, 2, parts, piece, rows // 2), BF16),
            vmem((parts, piece, rows), BF16), vmem((parts, piece, rows), BF16),
            vmem((parts, piece, rows), F32),
            vmem((depth, rows), BF16),
            vmem((9 * shard, rows), BF16),
            dma((11,)), dma((chunks, 3, 3)), dma((18,)), dma((2, chunks)), dma((2,)), dma((2,)),
            dma((2, 2, 2)), dma((2, 2, parts)), dma((parts,)), dma((parts,)),
            dma((4, parts)), dma((5,)),
        ],
        compiler_params=pltpu.CompilerParams(
            collective_id=0, has_side_effects=True, vmem_limit_bytes=40 * 2**20),
    )(*(pltpu.with_memory_space_constraint(a, pltpu.HBM) for a in (
        tokens.T, cotangent.T, gate_weight, up_weight, down_weight.T)))
    return dx.T, dg.T


def solution(mesh):
    n, tp = mesh.shape["fs"], mesh.shape["tp"]

    def per_device(tokens, cotangent, gate_weight, up_weight, down_weight):
        rows, depth = tokens.shape
        shard, ff = gate_weight.shape
        args = (tokens, cotangent, gate_weight, up_weight, down_weight)
        fits = (tp == 8 and n == 4 and rows % (2 * LANES) == 0 and rows <= 256
                and depth == n * shard and shard % SUB == 0 and ff % LANES == 0
                and LANES < ff <= 512 and depth <= 2048)
        return per_device_kernel(n, *args) if fits else per_device_plain(*args)

    placed = (P("fs", None), P("fs", None), P("fs", "tp"), P("fs", "tp"), P("tp", "fs"))
    return jax.shard_map(
        per_device,
        mesh=mesh,
        in_specs=placed,
        out_specs=(P("fs", None), P("tp", "fs")),
        check_vma=False,
    )
```

```python
import functools

import jax
import jax.numpy as jnp
from jax import lax
from jax.experimental import pallas as pl
from jax.experimental.pallas import tpu as pltpu
from jax.sharding import PartitionSpec as P

LANES = 128
SUB = 16
BF16 = jnp.bfloat16
F32 = jnp.float32


def contract_rows(left, right):
    return lax.dot_general(
        left, right, (((0,), (0,)), ((), ())), preferred_element_type=jnp.float32
    )


def contract_cols(left, right):
    return lax.dot_general(
        left, right, (((1,), (1,)), ((), ())), preferred_element_type=jnp.float32
    )


def send_down(hidden, cotangent):
    return lax.psum_scatter(
        contract_rows(cotangent, hidden), "fs", scatter_dimension=0, tiled=True
    ).T


def per_device_plain(tokens, cotangent, gate_weight, up_weight, down_weight):
    whole_gate, whole_up, whole_down = (
        lax.all_gather(gate_weight, "fs", axis=0, tiled=True),
        lax.all_gather(up_weight, "fs", axis=0, tiled=True),
        lax.all_gather(down_weight, "fs", axis=1, tiled=True),
    )
    gate_pre = jnp.dot(tokens, whole_gate, preferred_element_type=jnp.float32)
    up_pre = jnp.dot(tokens, whole_up, preferred_element_type=jnp.float32)
    hidden_grad = contract_cols(cotangent, whole_down)
    sigmoid_gate = jax.nn.sigmoid(gate_pre)
    activated = gate_pre * sigmoid_gate
    hidden = (activated * up_pre).astype(jnp.bfloat16)
    gate_pre_grad = (
        hidden_grad * up_pre * sigmoid_gate * (1.0 + gate_pre * (1.0 - sigmoid_gate))
    ).astype(jnp.bfloat16)
    up_pre_grad = (hidden_grad * activated).astype(jnp.bfloat16)
    partial_value = contract_cols(gate_pre_grad, whole_gate) + contract_cols(up_pre_grad, whole_up)
    input_grad = lax.psum(partial_value.astype(jnp.bfloat16), "tp")
    down_grad = send_down(hidden, cotangent)
    return (input_grad, down_grad)


def kernel(n, tok_hbm, cot_hbm, gate_hbm, up_hbm, down_hbm, dx_out, dg_out,
           tok_ref, cot_ref, gate_ref, up_ref, down_ref, weights, tok, cot,
           ptok, pcot, etok, ecot, dxacc, hid, dgacc, dgp, dgs, dgr, dgf,
           t1s, t1r, t2s, t2r, t3s, t3r, ownr, ybuf, tally,
           sent, w_recv, tk_recv, hid_recv, dg_recv, dgf_recv, t1_recv, t2_recv,
           t3_recv, own_recv, y_recv, local_sem):
    z = lax.axis_index("fs")
    b = lax.axis_index("tp")
    depth, rows = tok_ref.shape
    shard, ff = gate_ref.shape
    chunks = ff // LANES
    parts, piece = t2s.shape[2], t2s.shape[3]
    half_rows = rows // 2
    core = lax.rem(b, 2)
    col = lax.div(b, 2)
    cx = lax.rem(col, 2)
    cy = lax.div(col, 2)
    side = lax.div(z, 2)
    zodd = lax.rem(z, 2)
    home = core == side
    away = core != side
    near = side != zodd
    end = side == zodd
    lead = core == 1
    sib = b + 1 - 2 * core
    bx = b + 2 * (1 - 2 * cx)
    by = b + 4 * (1 - 2 * cy)
    bd = bx + by - b
    last = 2 * col + 1
    zs = z + 1 - 2 * zodd
    zn = 2 - side
    zf = 3 - 3 * side
    me = jnp.where(home, 0, 1)
    col_x = 2 * cy + 1 - cx
    col_y = 2 * (1 - cy) + cx
    col_d = 2 * (1 - cy) + 1 - cx
    for src, dst, i in ((tok_hbm, tok_ref, 0), (cot_hbm, cot_ref, 0), (gate_hbm, gate_ref, 1),
                        (up_hbm, up_ref, 1), (down_hbm, down_ref, 1)):
        pltpu.make_async_copy(src, dst, local_sem.at[i]).start()

    def drain(ref, sem):
        pltpu.make_async_copy(ref, ref, sem).wait()

    barrier = pltpu.get_barrier_semaphore()

    def greet(fs, tp):
        pl.semaphore_signal(barrier, inc=1, device_id={"fs": fs, "tp": tp},
                            device_id_type=pl.DeviceIdType.MESH)

    greet(z, sib)
    greet(z, bx)
    greet(z, by)
    greet(z, bd)
    for step in range(1, n):
        greet(lax.rem(z + step, n), b)
        greet(lax.rem(z + step, n), sib)
    pl.semaphore_wait(barrier, 4 + 2 * (n - 1))
    drain(tally.at[pl.ds(0, 2 * depth)], local_sem.at[0])
    drain(weights.at[pl.ds(0, shard)], local_sem.at[1])

    def remote(src, dst, send, recv, fs, tp):
        return pltpu.make_async_remote_copy(
            src_ref=src, dst_ref=dst, send_sem=send, recv_sem=recv,
            device_id={"fs": fs, "tp": tp}, device_id_type=pl.DeviceIdType.MESH)

    def rows_of(k, count=1):
        return pl.ds(pl.multiple_of(k * shard, SUB), count * shard)

    def lanes_of(c, count=1):
        return pl.ds(c * LANES, count * LANES)

    def slot(c, k, kind):
        return weights.at[rows_of(k), lanes_of(3 * c + kind)]

    def own(c, kind):
        return (gate_ref, up_ref, down_ref)[kind].at[:, lanes_of(c)]

    def w_copy(src, c, k, kind, i, fs):
        return remote(src, slot(c, k, kind), sent.at[0], w_recv.at[c, i, kind], fs, b)

    def sib_copy(src, c, k, kind):
        return remote(src, slot(c, k, kind), sent.at[1], w_recv.at[c, 0, 0], z, sib)

    every = [(c, kind) for c in range(chunks) for kind in range(3)]
    others = (zs, zn, zf)
    mine_q = rows_of(col)

    def tk_copy(i, src, dst, fs, tp):
        return remote(src, dst, sent.at[2], tk_recv.at[i], fs, tp)

    def tok_buf(e):
        return etok if e else ptok

    def cot_buf(e):
        return ecot if e else pcot

    def spread(i, e, q, tp):
        buf = cot_buf(e) if i in (1, 4, 5, 7) else tok_buf(e)
        ref = buf.at[rows_of(q)]
        return tk_copy(8 * e + i, ref, ref, z, tp)

    def spread_first(e):
        spread(0, e, col, bx).wait_recv()
        spread(2, e, col, bx).start()
        spread(3, e, col, by).start()
        spread(1, e, col, bx).wait_recv()
        spread(4, e, col, bx).start()
        spread(5, e, col, by).start()

    def spread_second(e):
        spread(2, e, col_x, bx).wait_recv()
        spread(6, e, col_x, by).start()
        spread(5, e, col_y, by).wait_recv()
        spread(7, e, col_y, bx).start()

    def spread_rest(e):
        spread(3, e, col_y, by).wait_recv()
        spread(6, e, col_d, by).wait_recv()
        spread(4, e, col_x, bx).wait_recv()
        spread(7, e, col_d, bx).wait_recv()

    far_rows = rows_of(2 * (1 - core), 2)
    give = tk_copy(16, pcot.at[far_rows], pcot.at[far_rows], z, sib)
    give_extra = tk_copy(17, ecot.at[far_rows], ecot.at[far_rows], z, sib)
    half_me = pl.ds(pl.multiple_of(me * half_rows, LANES), half_rows)
    @pl.when(end)
    def _():
        @pl.when(home)
        def _():
            tk_copy(8, tok_ref.at[mine_q], etok.at[mine_q], zn, sib).start()

        @pl.when(away)
        def _():
            tk_copy(9, cot_ref.at[mine_q], ecot.at[mine_q], zn, b).start()

    @pl.when(near)
    def _():
        @pl.when(home)
        def _():
            tk_copy(0, tok_ref.at[mine_q], ptok.at[mine_q], zn, b).start()

        @pl.when(away)
        def _():
            tk_copy(1, cot_ref.at[mine_q], pcot.at[mine_q], zn, sib).start()

    @pl.when(home)
    def _():
        for c, kind in every:
            w_copy(own(c, kind), c, z, kind, 0, zs).start()
            sib_copy(own(c, kind), c, z, kind).start()
            pltpu.make_async_copy(own(c, kind), slot(c, z, kind), local_sem.at[2]).start()

    @pl.when(away)
    def _():
        for c, kind in every:
            w_copy(own(c, kind), c, z, kind, jnp.where(near, 1, 2), zn).start()

    @pl.when(end)
    def _():
        tok[0, :half_rows] = tok_ref[:, half_me].T
        cot[0, :half_rows] = cot_ref[:, half_me].T

    @pl.when(jnp.logical_and(near, home))
    def _():
        tok[0] = tok_ref[...].T
        cot[0] = cot_ref[...].T
        spread_first(1)
        spread_second(1)

    @pl.when(jnp.logical_and(near, away))
    def _():
        spread_first(0)
        spread_second(0)
        spread_rest(0)
        give.start()
        tok[0] = ptok[...].T
        cot[0] = pcot[...].T

    def gather(c):
        @pl.when(home)
        def _():
            for kind in range(3):
                for i, k in enumerate(others):
                    there = slot(c, k, kind)
                    w_copy(there, c, k, kind, i, zs).wait_recv()
                    if i:
                        @pl.when(near)
                        def _():
                            w_copy(there, c, k, kind, i, zs).start()
                    sib_copy(there, c, k, kind).start()
            if c == 0:
                drain(weights.at[rows_of(z)], local_sem.at[2])

        @pl.when(away)
        def _():
            drain(weights.at[:, lanes_of(3 * c, 3)], w_recv.at[c, 0, 0])

    def hid_copy(e, c, ref):
        return remote(ref, ref, sent.at[3], hid_recv.at[e, c], z, sib)

    def hid_ref(e, c):
        return hid.at[2 if e else me, :, lanes_of(c)]

    def hid_half(c):
        return hid.at[0, pl.ds(pl.multiple_of(me * half_rows, SUB), half_rows), lanes_of(c)]

    def activate(x, y, c, out, e):
        pre = jnp.dot(x, weights[:, 3 * c * LANES:(3 * c + 2) * LANES],
                      preferred_element_type=F32)
        hg = jnp.dot(y, weights[:, (3 * c + 2) * LANES:(3 * c + 3) * LANES],
                     preferred_element_type=F32)
        gate_pre, up_pre = pre[:, :LANES], pre[:, LANES:]
        sig = jax.nn.sigmoid(gate_pre)
        act = gate_pre * sig
        out[...] = (act * up_pre).astype(BF16)
        hid_copy(e, c, out).start()
        return jnp.concatenate(
            [(hg * up_pre * sig * (1.0 + gate_pre * (1.0 - sig))).astype(BF16),
             (hg * act).astype(BF16)], axis=1)

    def work(e, c):
        dgu = activate(tok[e], cot[e], c, hid_ref(e, c), e)
        value = contract_cols(weights[:, 3 * c * LANES:(3 * c + 2) * LANES], dgu)
        if c == 0:
            dxacc[e] = value
        else:
            dxacc[e] += value

    def work_half(c):
        dgu = activate(tok[0, :half_rows], cot[0, :half_rows], c, hid_half(c), 0)
        value = contract_cols(weights[:, 3 * c * LANES:(3 * c + 2) * LANES], dgu)
        if c == 0:
            dxacc[0, :, half_me] = value
        else:
            dxacc[0, :, half_me] += value

    halves = (slice(0, half_rows), slice(half_rows, rows))

    def t1_copy(e, i, step):
        return remote(t1s.at[e, i, step], t1r.at[e, i, step], sent.at[5], t1_recv.at[e, i, step],
                      z, bx if i == 0 else by)

    def t2_copy(e, i, q):
        return remote(t2s.at[e, i, q], t2r.at[e, i, q], sent.at[6], t2_recv.at[e, i, q],
                      z, by if i == 0 else bx)

    def t3_copy(q, fs):
        return remote(t3s.at[q], t3r.at[q], sent.at[7], t3_recv.at[q], fs, last)

    def strip(k, q):
        return pl.ds(pl.multiple_of(k * shard + q * piece, SUB), piece)

    def own_copy(q):
        return remote(dxacc.at[0, strip(col, q)], ownr.at[q], sent.at[10], own_recv.at[q], z, sib)

    def work_last(e, c):
        dgu = activate(tok[e], cot[e], c, hid_ref(e, c), e)
        for k, sends in ((col_d, ((0, 0), (1, 0))), (col_x, ((0, 1),)), (col_y, ((1, 1),)), (col, ())):
            r = rows_of(k)
            value = contract_cols(weights[r, 3 * c * LANES:(3 * c + 2) * LANES], dgu) + dxacc[e, r, :]
            if k is not col_d:
                dxacc[e, r, :] = value
            for i, step in sends:
                t1s[e, i, step] = value[:, halves[i]].astype(BF16)
                t1_copy(e, i, step).start()

    first_tp = jnp.where(home, bx, by)
    second_tp = jnp.where(home, by, bx)
    first_col = jnp.where(home, col_x, col_y)
    second_col = jnp.where(home, col_y, col_x)

    def t1_half(step):
        return remote(t1s.at[0, me, step], t1r.at[0, me, step], sent.at[5], t1_recv.at[0, me, step],
                      z, first_tp + 1 - core)

    def own_half(i, k):
        ref = dxacc.at[0, rows_of(k), half_me]
        return remote(ref, ref, sent.at[10], own_recv.at[i], z, sib)

    def take_half(i, k):
        there = pl.ds(pl.multiple_of((1 - me) * half_rows, LANES), half_rows)
        ref = dxacc.at[0, rows_of(k), there]
        return remote(ref, ref, sent.at[10], own_recv.at[i], z, sib)

    def last_half(c):
        dgu = activate(tok[0, :half_rows], cot[0, :half_rows], c, hid_half(c), 0)
        for k, step in ((col_d, 0), (first_col, 1), (second_col, 2), (col, 2)):
            r = rows_of(k)
            value = (contract_cols(weights[r, 3 * c * LANES:(3 * c + 2) * LANES], dgu)
                     + dxacc[0, r, half_me])
            if step:
                dxacc[0, r, half_me] = value
            if step < 2:
                t1s[0, me, step] = value.astype(BF16)
                t1_half(step).start()

    def reduce_half():
        @pl.when(core == 0)
        def _():
            own_half(0, second_col).start()
            own_half(1, col).start()

        @pl.when(lead)
        def _():
            take_half(0, first_col).wait_recv()
            second_step(0)
            take_half(1, col).wait_recv()
            collect(0)
            for q in range(parts):
                arrive(0, q)

    def second_step(e):
        t1_copy(e, 0, 0).wait_recv()
        t1_copy(e, 1, 0).wait_recv()
        for q in range(parts):
            inner = slice(q * piece, (q + 1) * piece)
            for i, k in ((0, col_y), (1, col_x)):
                t2s[e, i, q] = (dxacc[e, strip(k, q), halves[i]]
                                + t1r[e, i, 0, inner].astype(F32)).astype(BF16)
                t2_copy(e, i, q).start()

    def collect(e):
        t1_copy(e, 0, 1).wait_recv()
        t1_copy(e, 1, 1).wait_recv()
        for q in range(parts):
            inner = slice(q * piece, (q + 1) * piece)
            for i in range(2):
                dxacc[e, strip(col, q), halves[i]] += t1r[e, i, 1, inner].astype(F32)

    def arrive(e, q):
        for i in range(2):
            t2_copy(e, i, q).wait_recv()
            dxacc[e, strip(col, q), halves[i]] += t2r[e, i, q].astype(F32)

    stages = (slice(0, ff - LANES), slice(ff - LANES, ff))

    def lanes_at(g):
        return pl.ds(stages[g].start, stages[g].stop - stages[g].start)

    def dg_home(g):
        lanes = lanes_at(g)
        return remote(dgs.at[0, :, lanes], dgr.at[0, :, lanes], sent.at[4], dg_recv.at[g], zs, b)

    def dg_away(g):
        lanes = lanes_at(g)
        return remote(dgs.at[:, :, lanes], dgr.at[:, :, lanes], sent.at[4], dg_recv.at[g], zs, b)

    def dg_far(g, i):
        lanes = lanes_at(g)
        return remote(dgs.at[i, :, lanes], dgf.at[:, lanes], sent.at[4], dgf_recv.at[g],
                      2 * (1 - side) + i, sib)

    def stage_chunks(g):
        return range(chunks - 1) if g == 0 else (chunks - 1,)

    def keep_part(g, i, value):
        lanes = stages[g]

        @pl.when(jnp.logical_and(home, zodd == i))
        def _():
            dgacc[:, lanes] = value

        @pl.when(jnp.logical_and(home, zodd != i))
        def _():
            dgs[0, :, lanes] = value.astype(BF16)

        @pl.when(jnp.logical_and(away, near))
        def _():
            dgp[i, :, lanes] = value

        @pl.when(jnp.logical_and(away, end))
        def _():
            dgs[i, :, lanes] = value.astype(BF16)

    def down_near(g):
        for c in stage_chunks(g):
            hid_copy(0, c, hid.at[1 - me, :, lanes_of(c)]).wait_recv()

            @pl.when(away)
            def _():
                hid_copy(1, c, hid.at[2, :, lanes_of(c)]).wait_recv()
        lanes = stages[g]
        for i in range(2):
            k = rows_of(2 * core + i)
            keep_part(g, i, jnp.dot(cot_ref[k, :], hid[0, :, lanes], preferred_element_type=F32)
                      + jnp.dot(pcot[k, :], hid[1, :, lanes], preferred_element_type=F32)
                      + jnp.dot(ecot[k, :], hid[2, :, lanes], preferred_element_type=F32))

    def down_end(g):
        for c in stage_chunks(g):
            other = hid.at[0, pl.ds(pl.multiple_of((1 - me) * half_rows, SUB), half_rows), lanes_of(c)]
            hid_copy(0, c, other).wait_recv()
        for i in range(2):
            k = rows_of(2 * core + i)
            keep_part(g, i, jnp.dot(cot_ref[k, :], hid[0, :, stages[g]], preferred_element_type=F32))

        @pl.when(home)
        def _():
            dg_home(g).start()

        @pl.when(away)
        def _():
            dg_away(g).start()

    def down_mid(g):
        lanes = stages[g]
        dg_away(g).wait_recv()
        for i in range(2):
            dgs[i, :, lanes] = (dgp[i, :, lanes] + dgr[i, :, lanes].astype(F32)).astype(BF16)
            dg_far(g, i).start()
    @pl.when(near)
    def _():
        for c in range(chunks - 1):
            gather(c)
            work(0, c)
        gather(chunks - 1)

        @pl.when(home)
        def _():
            spread_rest(1)
            give_extra.start()
            tok[1] = etok[...].T
            cot[1] = ecot[...].T
            for c in range(chunks - 1):
                work(1, c)

        @pl.when(home)
        def _():
            work_last(1, chunks - 1)
        work_last(0, chunks - 1)

        @pl.when(home)
        def _():
            give.wait_recv()

        @pl.when(away)
        def _():
            give_extra.wait_recv()

        for g in range(2):
            down_near(g)

        @pl.when(home)
        def _():
            second_step(1)
            collect(1)
            for q in range(parts):
                arrive(1, q)
                t3s[q] = dxacc[1, strip(col, q), :].astype(BF16)
                t3_copy(q, zf).start()
            for g in range(2):
                dg_home(g).start()
        second_step(0)
        collect(0)
        for q in range(parts):
            arrive(0, q)

            @pl.when(away)
            def _():
                t3s[q] = dxacc[0, strip(col, q), :].astype(BF16)
                t3_copy(q, zn).start()

            @pl.when(jnp.logical_and(home, core == 0))
            def _():
                own_copy(q).start()

        @pl.when(away)
        def _():
            down_mid(0)

            @pl.when(core == 0)
            def _():
                down_mid(1)

    @pl.when(end)
    def _():
        for c in range(chunks - 1):
            gather(c)
            work_half(c)
        down_end(0)
        gather(chunks - 1)
        last_half(chunks - 1)
        down_end(1)
        reduce_half()

    def y_copy(i, k, q, tp):
        ref = ybuf.at[strip(k, q)]
        return remote(ref, ref, sent.at[8], y_recv.at[i, q], z, tp)

    def y_sib(i, k, q):
        ref = ybuf.at[strip(k, q)]
        return remote(ref, ref, sent.at[9], y_recv.at[i, q], z, sib)

    def put(k, q):
        r = strip(k, q)
        return pltpu.make_async_copy(ybuf.at[r], dx_out.at[r], local_sem.at[3])

    dg_put = pltpu.make_async_copy(dgacc, dg_out, local_sem.at[4])

    def result(q, value):
        ybuf[strip(col, q), :] = value.astype(BF16)
    @pl.when(lead)
    def _():
        for q in range(parts):
            t3_copy(q, zn).wait_recv()

            @pl.when(jnp.logical_or(end, home))
            def _():
                result(q, dxacc[0, strip(col, q), :] + t3r[q].astype(F32))

            @pl.when(jnp.logical_and(near, away))
            def _():
                own_copy(q).wait_recv()
                result(q, ownr[q] + t3r[q].astype(F32))
            y_copy(2, col, q, bd).start()
            y_copy(0, col, q, bx).start()
            y_copy(1, col, q, by).start()
            y_sib(0, col, q).start()
            put(col, q).start()

        @pl.when(jnp.logical_and(near, away))
        def _():
            down_mid(1)
        for q in range(parts):
            for i, k, tp in ((0, col_x, bx), (1, col_y, by), (2, col_d, bd)):
                y_copy(i, k, q, tp).wait_recv()
                y_sib(i + 1, k, q).start()
                put(k, q).start()
    @pl.when(home)
    def _():
        for g in range(2):
            dg_home(g).wait_recv()
        dgacc[...] += dgr[0].astype(F32)

    @pl.when(away)
    def _():
        for g in range(2):
            dg_far(g, 0).wait_recv()
        dgacc[...] = dgf[...].astype(F32)

    dg_put.start()
    @pl.when(core == 0)
    def _():
        for q in range(parts):
            for i, k in enumerate((col, col_x, col_y, col_d)):
                y_sib(i, k, q).wait_recv()
                put(k, q).start()
    @pl.when(lead)
    def _():
        drain(ybuf.at[pl.ds(0, 3 * shard)], sent.at[8])
        drain(ybuf, sent.at[9])

    @pl.when(home)
    def _():
        drain(weights, sent.at[1])
        drain(dgs.at[0], sent.at[4])

    @pl.when(away)
    def _():
        drain(weights.at[pl.ds(0, shard)], sent.at[0])
        drain(dgs, sent.at[4])

    @pl.when(end)
    def _():
        drain(tally.at[pl.ds(0, shard)], sent.at[2])
        drain(hid.at[0, pl.ds(0, half_rows)], sent.at[3])
        drain(t1s.at[0, 0], sent.at[5])

        @pl.when(lead)
        def _():
            drain(t2s.at[0], sent.at[6])

        @pl.when(home)
        def _():
            drain(weights.at[pl.ds(0, shard)], sent.at[0])

        @pl.when(core == 0)
        def _():
            drain(dxacc.at[0, pl.ds(0, 2 * shard), pl.ds(0, half_rows)], sent.at[10])

    @pl.when(near)
    def _():
        drain(tally, sent.at[2])
        drain(t3s, sent.at[7])

        @pl.when(home)
        def _():
            drain(weights.at[pl.ds(0, 3 * shard)], sent.at[0])
            drain(hid.at[pl.ds(0, 2)], sent.at[3])
            drain(t1s, sent.at[5])
            drain(t2s, sent.at[6])

            @pl.when(core == 0)
            def _():
                drain(ownr, sent.at[10])

        @pl.when(away)
        def _():
            drain(hid.at[0], sent.at[3])
            drain(t1s.at[0], sent.at[5])
            drain(t2s.at[0], sent.at[6])

    drain(ybuf, local_sem.at[3])
    dg_put.wait()


def per_device_kernel(n, tokens, cotangent, gate_weight, up_weight, down_weight):
    rows, depth = tokens.shape
    shard, ff = gate_weight.shape
    chunks = ff // LANES
    parts = next(p for p in (3, 2, 1) if shard % (p * SUB) == 0)
    piece = shard // parts
    vmem, dma = pltpu.VMEM, pltpu.SemaphoreType.DMA
    dx, dg = pl.pallas_call(
        functools.partial(kernel, n),
        out_shape=(vmem((depth, rows), BF16), vmem((shard, ff), F32)),
        in_specs=[pl.BlockSpec(memory_space=pltpu.HBM)] * 5,
        out_specs=[pl.BlockSpec(memory_space=pl.ANY)] * 2,
        scratch_shapes=[
            vmem((depth, rows), BF16), vmem((depth, rows), BF16),
            vmem((shard, ff), BF16), vmem((shard, ff), BF16), vmem((shard, ff), BF16),
            vmem((depth, 3 * ff), BF16),
            vmem((2, rows, depth), BF16), vmem((2, rows, depth), BF16),
            vmem((depth, rows), BF16), vmem((depth, rows), BF16),
            vmem((depth, rows), BF16), vmem((depth, rows), BF16),
            vmem((2, depth, rows), F32),
            vmem((3, rows, ff), BF16),
            vmem((shard, ff), F32), vmem((2, shard, ff), F32), vmem((2, shard, ff), BF16),
            vmem((2, shard, ff), BF16), vmem((shard, ff), BF16),
            vmem((2, 2, 2, shard, rows // 2), BF16), vmem((2, 2, 2, shard, rows // 2), BF16),
            vmem((2, 2, parts, piece, rows // 2), BF16), vmem((2, 2, parts, piece, rows // 2), BF16),
            vmem((parts, piece, rows), BF16), vmem((parts, piece, rows), BF16),
            vmem((parts, piece, rows), F32),
            vmem((depth, rows), BF16),
            vmem((9 * shard, rows), BF16),
            dma((11,)), dma((chunks, 3, 3)), dma((18,)), dma((2, chunks)), dma((2,)), dma((2,)),
            dma((2, 2, 2)), dma((2, 2, parts)), dma((parts,)), dma((parts,)),
            dma((4, parts)), dma((5,)),
        ],
        compiler_params=pltpu.CompilerParams(
            collective_id=0, has_side_effects=True, vmem_limit_bytes=40 * 2**20),
    )(*(pltpu.with_memory_space_constraint(a, pltpu.HBM) for a in (
        tokens.T, cotangent.T, gate_weight, up_weight, down_weight.T)))
    return dx.T, dg.T


def solution(mesh):
    n, tp = mesh.shape["fs"], mesh.shape["tp"]

    def per_device(tokens, cotangent, gate_weight, up_weight, down_weight):
        rows, depth = tokens.shape
        shard, ff = gate_weight.shape
        args = (tokens, cotangent, gate_weight, up_weight, down_weight)
        fits = (tp == 8 and n == 4 and rows % (2 * LANES) == 0 and rows <= 256
                and depth == n * shard and shard % SUB == 0 and ff % LANES == 0
                and LANES < ff <= 512 and depth <= 2048)
        return per_device_kernel(n, *args) if fits else per_device_plain(*args)

    placed = (P("fs", None), P("fs", None), P("fs", "tp"), P("fs", "tp"), P("tp", "fs"))
    return jax.shard_map(
        per_device,
        mesh=mesh,
        in_specs=placed,
        out_specs=(P("fs", None), P("tp", "fs")),
        check_vma=False,
    )
```

```python
import functools

import jax
import jax.numpy as jnp
from jax import lax
from jax.experimental import pallas as pl
from jax.experimental.pallas import tpu as pltpu
from jax.sharding import PartitionSpec as P

LANES = 128
SUB = 16
BF16 = jnp.bfloat16
F32 = jnp.float32


def contract_rows(left, right):
    return lax.dot_general(
        left, right, (((0,), (0,)), ((), ())), preferred_element_type=jnp.float32
    )


def contract_cols(left, right):
    return lax.dot_general(
        left, right, (((1,), (1,)), ((), ())), preferred_element_type=jnp.float32
    )


def send_down(hidden, cotangent):
    return lax.psum_scatter(
        contract_rows(cotangent, hidden), "fs", scatter_dimension=0, tiled=True
    ).T


def per_device_plain(tokens, cotangent, gate_weight, up_weight, down_weight):
    whole_gate, whole_up, whole_down = (
        lax.all_gather(gate_weight, "fs", axis=0, tiled=True),
        lax.all_gather(up_weight, "fs", axis=0, tiled=True),
        lax.all_gather(down_weight, "fs", axis=1, tiled=True),
    )
    gate_pre = jnp.dot(tokens, whole_gate, preferred_element_type=jnp.float32)
    up_pre = jnp.dot(tokens, whole_up, preferred_element_type=jnp.float32)
    hidden_grad = contract_cols(cotangent, whole_down)
    sigmoid_gate = jax.nn.sigmoid(gate_pre)
    activated = gate_pre * sigmoid_gate
    hidden = (activated * up_pre).astype(jnp.bfloat16)
    gate_pre_grad = (
        hidden_grad * up_pre * sigmoid_gate * (1.0 + gate_pre * (1.0 - sigmoid_gate))
    ).astype(jnp.bfloat16)
    up_pre_grad = (hidden_grad * activated).astype(jnp.bfloat16)
    partial_value = contract_cols(gate_pre_grad, whole_gate) + contract_cols(up_pre_grad, whole_up)
    input_grad = lax.psum(partial_value.astype(jnp.bfloat16), "tp")
    down_grad = send_down(hidden, cotangent)
    return (input_grad, down_grad)


def kernel(n, tok_hbm, cot_hbm, gate_hbm, up_hbm, down_hbm, dx_out, dg_out,
           tok_ref, cot_ref, gate_ref, up_ref, down_ref, weights, tok, cot,
           ptok, pcot, etok, ecot, dxacc, hid, dgacc, dgp, dgs, dgr, dgf, dge,
           t1s, t1r, t2s, t2r, t3s, t3r, es, er, ownr, ybuf, tally,
           sent, w_recv, tk_recv, hid_recv, dg_recv, dgf_recv, dge_recv, t1_recv, t2_recv,
           t3_recv, e_recv, own_recv, y_recv, local_sem):
    z = lax.axis_index("fs")
    b = lax.axis_index("tp")
    depth, rows = tok_ref.shape
    shard, ff = gate_ref.shape
    chunks = ff // LANES
    parts, piece = t2s.shape[2], t2s.shape[3]
    half_rows = rows // 2
    core = lax.rem(b, 2)
    col = lax.div(b, 2)
    cx = lax.rem(col, 2)
    cy = lax.div(col, 2)
    side = lax.div(z, 2)
    zodd = lax.rem(z, 2)
    home = core == side
    away = core != side
    near = side != zodd
    end = side == zodd
    lead = core == 1
    sib = b + 1 - 2 * core
    bx = b + 2 * (1 - 2 * cx)
    by = b + 4 * (1 - 2 * cy)
    bd = bx + by - b
    last = 2 * col + 1
    zs = z + 1 - 2 * zodd
    zn = 2 - side
    zf = 3 - 3 * side
    me = jnp.where(home, 0, 1)
    col_x = 2 * cy + 1 - cx
    col_y = 2 * (1 - cy) + cx
    col_d = 2 * (1 - cy) + 1 - cx
    for src, dst, i in ((tok_hbm, tok_ref, 0), (cot_hbm, cot_ref, 0), (gate_hbm, gate_ref, 1),
                        (up_hbm, up_ref, 1), (down_hbm, down_ref, 1)):
        pltpu.make_async_copy(src, dst, local_sem.at[i]).start()

    def drain(ref, sem):
        pltpu.make_async_copy(ref, ref, sem).wait()

    barrier = pltpu.get_barrier_semaphore()

    def greet(fs, tp):
        pl.semaphore_signal(barrier, inc=1, device_id={"fs": fs, "tp": tp},
                            device_id_type=pl.DeviceIdType.MESH)

    greet(z, sib)
    greet(z, bx)
    greet(z, by)
    greet(z, bd)
    for step in range(1, n):
        greet(lax.rem(z + step, n), b)
        greet(lax.rem(z + step, n), sib)
    pl.semaphore_wait(barrier, 4 + 2 * (n - 1))
    drain(tally.at[pl.ds(0, 2 * depth)], local_sem.at[0])
    drain(weights.at[pl.ds(0, shard)], local_sem.at[1])

    def remote(src, dst, send, recv, fs, tp):
        return pltpu.make_async_remote_copy(
            src_ref=src, dst_ref=dst, send_sem=send, recv_sem=recv,
            device_id={"fs": fs, "tp": tp}, device_id_type=pl.DeviceIdType.MESH)

    def rows_of(k, count=1):
        return pl.ds(pl.multiple_of(k * shard, SUB), count * shard)

    def lanes_of(c, count=1):
        return pl.ds(c * LANES, count * LANES)

    def slot(c, k, kind):
        return weights.at[rows_of(k), lanes_of(3 * c + kind)]

    def own(c, kind):
        return (gate_ref, up_ref, down_ref)[kind].at[:, lanes_of(c)]

    def w_copy(src, c, k, kind, i, fs):
        return remote(src, slot(c, k, kind), sent.at[0], w_recv.at[c, i, kind], fs, b)

    def sib_copy(src, c, k, kind):
        return remote(src, slot(c, k, kind), sent.at[1], w_recv.at[c, 0, 0], z, sib)

    every = [(c, kind) for c in range(chunks) for kind in range(3)]
    others = (zs, zn, zf)
    mine_q = rows_of(col)

    def tk_copy(i, src, dst, fs, tp):
        return remote(src, dst, sent.at[2], tk_recv.at[i], fs, tp)

    def tok_buf(e):
        return etok if e else ptok

    def cot_buf(e):
        return ecot if e else pcot

    def spread(i, e, q, tp):
        buf = cot_buf(e) if i in (1, 4, 5, 7) else tok_buf(e)
        ref = buf.at[rows_of(q)]
        return tk_copy(8 * e + i, ref, ref, z, tp)

    def spread_first(e):
        spread(0, e, col, bx).wait_recv()
        spread(2, e, col, bx).start()
        spread(3, e, col, by).start()
        spread(1, e, col, bx).wait_recv()
        spread(4, e, col, bx).start()
        spread(5, e, col, by).start()

    def spread_second(e):
        spread(2, e, col_x, bx).wait_recv()
        spread(6, e, col_x, by).start()
        spread(5, e, col_y, by).wait_recv()
        spread(7, e, col_y, bx).start()

    def spread_rest(e):
        spread(3, e, col_y, by).wait_recv()
        spread(6, e, col_d, by).wait_recv()
        spread(4, e, col_x, bx).wait_recv()
        spread(7, e, col_d, bx).wait_recv()

    far_rows = rows_of(2 * (1 - core), 2)
    give = tk_copy(16, pcot.at[far_rows], pcot.at[far_rows], z, sib)
    give_extra = tk_copy(17, ecot.at[far_rows], ecot.at[far_rows], z, sib)
    half_me = pl.ds(pl.multiple_of(me * half_rows, LANES), half_rows)
    @pl.when(end)
    def _():
        @pl.when(home)
        def _():
            tk_copy(8, tok_ref.at[mine_q], etok.at[mine_q], zn, sib).start()

        @pl.when(away)
        def _():
            tk_copy(9, cot_ref.at[mine_q], ecot.at[mine_q], zn, b).start()

    @pl.when(near)
    def _():
        @pl.when(home)
        def _():
            tk_copy(0, tok_ref.at[mine_q], ptok.at[mine_q], zn, b).start()

        @pl.when(away)
        def _():
            tk_copy(1, cot_ref.at[mine_q], pcot.at[mine_q], zn, sib).start()

    @pl.when(home)
    def _():
        for c, kind in every:
            w_copy(own(c, kind), c, z, kind, 0, zs).start()
            sib_copy(own(c, kind), c, z, kind).start()
            pltpu.make_async_copy(own(c, kind), slot(c, z, kind), local_sem.at[2]).start()

    @pl.when(away)
    def _():
        for c, kind in every:
            w_copy(own(c, kind), c, z, kind, jnp.where(near, 1, 2), zn).start()

    @pl.when(end)
    def _():
        tok[0, :half_rows] = tok_ref[:, half_me].T
        cot[0, :half_rows] = cot_ref[:, half_me].T

    @pl.when(jnp.logical_and(near, home))
    def _():
        tok[0] = tok_ref[...].T
        cot[0] = cot_ref[...].T
        spread_first(1)
        spread_second(1)

    @pl.when(jnp.logical_and(near, away))
    def _():
        spread_first(0)
        spread_second(0)
        spread_rest(0)
        give.start()
        tok[0] = ptok[...].T
        cot[0] = pcot[...].T

    def relay(c, kind):
        for i, k in enumerate(others):
            there = slot(c, k, kind)
            w_copy(there, c, k, kind, i, zs).wait_recv()
            if i:
                @pl.when(near)
                def _():
                    w_copy(there, c, k, kind, i, zs).start()
            sib_copy(there, c, k, kind).start()

    def relay_all(c):
        for kind in range(3):
            relay(c, kind)
        if c == 0:
            drain(weights.at[rows_of(z)], local_sem.at[2])

    def gather_sib(c):
        drain(weights.at[:, lanes_of(3 * c, 3)], w_recv.at[c, 0, 0])

    def gather(c):
        @pl.when(home)
        def _():
            relay_all(c)

        @pl.when(away)
        def _():
            gather_sib(c)

    def hid_copy(e, c, ref):
        return remote(ref, ref, sent.at[3], hid_recv.at[e, c], z, sib)

    def hid_ref(e, c):
        return hid.at[2 if e else me, :, lanes_of(c)]

    def hid_half(c):
        return hid.at[0, pl.ds(pl.multiple_of(me * half_rows, SUB), half_rows), lanes_of(c)]

    def activate(x, y, c, out, e):
        pre = jnp.dot(x, weights[:, 3 * c * LANES:(3 * c + 2) * LANES],
                      preferred_element_type=F32)
        hg = jnp.dot(y, weights[:, (3 * c + 2) * LANES:(3 * c + 3) * LANES],
                     preferred_element_type=F32)
        gate_pre, up_pre = pre[:, :LANES], pre[:, LANES:]
        sig = jax.nn.sigmoid(gate_pre)
        act = gate_pre * sig
        out[...] = (act * up_pre).astype(BF16)
        hid_copy(e, c, out).start()
        return jnp.concatenate(
            [(hg * up_pre * sig * (1.0 + gate_pre * (1.0 - sig))).astype(BF16),
             (hg * act).astype(BF16)], axis=1)

    def begin(e, c):
        return activate(tok[e], cot[e], c, hid_ref(e, c), e)

    def finish(e, c, dgu):
        value = contract_cols(weights[:, 3 * c * LANES:(3 * c + 2) * LANES], dgu)
        if c == 0:
            dxacc[e] = value
        else:
            dxacc[e] += value

    def take_tokens():
        spread_rest(1)
        give_extra.start()
        tok[1] = etok[...].T
        cot[1] = ecot[...].T

    def work_half(c):
        dgu = activate(tok[0, :half_rows], cot[0, :half_rows], c, hid_half(c), 0)
        value = contract_cols(weights[:, 3 * c * LANES:(3 * c + 2) * LANES], dgu)
        if c == 0:
            dxacc[0, :, half_me] = value
        else:
            dxacc[0, :, half_me] += value

    halves = (slice(0, half_rows), slice(half_rows, rows))

    def t1_copy(e, i, step):
        return remote(t1s.at[e, i, step], t1r.at[e, i, step], sent.at[5], t1_recv.at[e, i, step],
                      z, bx if i == 0 else by)

    def t2_copy(e, i, q):
        return remote(t2s.at[e, i, q], t2r.at[e, i, q], sent.at[6], t2_recv.at[e, i, q],
                      z, by if i == 0 else bx)

    def t3_copy(q, fs):
        return remote(t3s.at[q], t3r.at[q], sent.at[7], t3_recv.at[q], fs, last)

    def strip(k, q):
        return pl.ds(pl.multiple_of(k * shard + q * piece, SUB), piece)

    def own_copy(q):
        return remote(dxacc.at[0, strip(col, q)], ownr.at[q], sent.at[10], own_recv.at[q], z, sib)

    def work_last(e, c):
        dgu = activate(tok[e], cot[e], c, hid_ref(e, c), e)
        for k, sends in ((col_d, ((0, 0), (1, 0))), (col_x, ((0, 1),)), (col_y, ((1, 1),)), (col, ())):
            r = rows_of(k)
            value = contract_cols(weights[r, 3 * c * LANES:(3 * c + 2) * LANES], dgu) + dxacc[e, r, :]
            if k is not col_d:
                dxacc[e, r, :] = value
            for i, step in sends:
                t1s[e, i, step] = value[:, halves[i]].astype(BF16)
                t1_copy(e, i, step).start()

    there = pl.ds(pl.multiple_of((1 - me) * half_rows, LANES), half_rows)

    def e_copy(i, q, tp):
        return remote(es.at[i, q], er.at[q, me, i], sent.at[5], e_recv.at[q], z, tp + 1 - core)

    def own_half():
        ref = dxacc.at[0, rows_of(col), half_me]
        return remote(ref, ref, sent.at[10], own_recv.at[0], z, sib)

    def take_half():
        ref = dxacc.at[0, rows_of(col), there]
        return remote(ref, ref, sent.at[10], own_recv.at[0], z, sib)

    def last_half(c):
        dgu = activate(tok[0, :half_rows], cot[0, :half_rows], c, hid_half(c), 0)
        columns = pl.ds(3 * c * LANES, 2 * LANES)
        for q in range(parts):
            for i, (k, tp) in enumerate(((col_d, bd), (col_x, bx), (col_y, by))):
                r = strip(k, q)
                es[i, q] = (contract_cols(weights[r, columns], dgu) + dxacc[0, r, half_me]).astype(BF16)
                e_copy(i, q, tp).start()
        r = rows_of(col)
        dxacc[0, r, half_me] += contract_cols(weights[r, columns], dgu)

        @pl.when(core == 0)
        def _():
            own_half().start()

    def end_result(q):
        drain(er.at[q], e_recv.at[q])
        r = strip(col, q)
        for i in range(2):
            total = dxacc[0, r, halves[i]] + t3r[q, :, halves[i]].astype(F32)
            for k in range(3):
                total = total + er[q, i, k].astype(F32)
            ybuf[r, halves[i]] = total.astype(BF16)

    def second_step(e):
        t1_copy(e, 0, 0).wait_recv()
        t1_copy(e, 1, 0).wait_recv()
        for q in range(parts):
            inner = slice(q * piece, (q + 1) * piece)
            for i, k in ((0, col_y), (1, col_x)):
                t2s[e, i, q] = (dxacc[e, strip(k, q), halves[i]]
                                + t1r[e, i, 0, inner].astype(F32)).astype(BF16)
                t2_copy(e, i, q).start()

    def collect(e):
        t1_copy(e, 0, 1).wait_recv()
        t1_copy(e, 1, 1).wait_recv()
        for q in range(parts):
            inner = slice(q * piece, (q + 1) * piece)
            for i in range(2):
                dxacc[e, strip(col, q), halves[i]] += t1r[e, i, 1, inner].astype(F32)

    def arrive(e, q):
        for i in range(2):
            t2_copy(e, i, q).wait_recv()
            dxacc[e, strip(col, q), halves[i]] += t2r[e, i, q].astype(F32)

    def span(c):
        return slice(c * LANES, (c + 1) * LANES)

    def dg_home(g):
        lanes = lanes_of(g)
        return remote(dgs.at[0, :, lanes], dgr.at[0, :, lanes], sent.at[4], dg_recv.at[g], zs, b)

    def dg_away(g):
        lanes = lanes_of(g)
        return remote(dgs.at[:, :, lanes], dgr.at[:, :, lanes], sent.at[4], dg_recv.at[g], zs, b)

    def dg_far(g, i):
        lanes = lanes_of(g)
        return remote(dgs.at[i, :, lanes], dgf.at[:, lanes], sent.at[4], dgf_recv.at[g],
                      2 * (1 - side) + i, sib)

    def dg_direct(i):
        return remote(dgs.at[i, :, lanes_of(chunks - 1)], dge, sent.at[4], dge_recv.at[0],
                      2 * (1 - side) + i, sib)

    def keep_part(g, i, value):
        lanes = span(g)

        @pl.when(jnp.logical_and(home, zodd == i))
        def _():
            dgacc[:, lanes] = value

        @pl.when(jnp.logical_and(home, zodd != i))
        def _():
            dgs[0, :, lanes] = value.astype(BF16)

        if g == chunks - 1:
            @pl.when(away)
            def _():
                dgs[i, :, lanes] = value.astype(BF16)

                @pl.when(near)
                def _():
                    dg_far(g, i).start()

                @pl.when(end)
                def _():
                    dg_direct(i).start()
        else:
            @pl.when(jnp.logical_and(away, near))
            def _():
                dgp[i, :, lanes] = value

            @pl.when(jnp.logical_and(away, end))
            def _():
                dgs[i, :, lanes] = value.astype(BF16)

    def down_near(g):
        hid_copy(0, g, hid.at[1 - me, :, lanes_of(g)]).wait_recv()

        @pl.when(away)
        def _():
            hid_copy(1, g, hid.at[2, :, lanes_of(g)]).wait_recv()

        lanes = span(g)
        for i in range(2):
            k = rows_of(2 * core + i)
            keep_part(g, i, jnp.dot(cot_ref[k, :], hid[0, :, lanes], preferred_element_type=F32)
                      + jnp.dot(pcot[k, :], hid[1, :, lanes], preferred_element_type=F32)
                      + jnp.dot(ecot[k, :], hid[2, :, lanes], preferred_element_type=F32))

    def down_end(g):
        other = hid.at[0, pl.ds(pl.multiple_of((1 - me) * half_rows, SUB), half_rows), lanes_of(g)]
        hid_copy(0, g, other).wait_recv()
        for i in range(2):
            k = rows_of(2 * core + i)
            keep_part(g, i, jnp.dot(cot_ref[k, :], hid[0, :, span(g)], preferred_element_type=F32))

        @pl.when(home)
        def _():
            dg_home(g).start()

        if g < chunks - 1:
            @pl.when(away)
            def _():
                dg_away(g).start()

    def down_mid(g):
        lanes = span(g)
        dg_away(g).wait_recv()
        for i in range(2):
            dgs[i, :, lanes] = (dgp[i, :, lanes] + dgr[i, :, lanes].astype(F32)).astype(BF16)
            dg_far(g, i).start()
    @pl.when(near)
    def _():

        @pl.when(home)
        def _():
            relay_all(0)
            for c in range(chunks - 1):
                dgu = begin(0, c)
                relay(c + 1, 0)
                finish(0, c, dgu)
                if c == 0:
                    take_tokens()
                relay(c + 1, 1)
                finish(1, c, begin(1, c))
                relay(c + 1, 2)

        @pl.when(away)
        def _():
            for c in range(chunks - 1):
                gather_sib(c)
                finish(0, c, begin(0, c))
            gather_sib(chunks - 1)

        @pl.when(home)
        def _():
            work_last(1, chunks - 1)
        work_last(0, chunks - 1)

        @pl.when(home)
        def _():
            second_step(1)
            collect(1)

        @pl.when(home)
        def _():
            give.wait_recv()

        @pl.when(away)
        def _():
            give_extra.wait_recv()

        for c in range(chunks):
            down_near(c)

            @pl.when(home)
            def _():
                dg_home(c).start()

            if c == 0 and chunks > 2:
                @pl.when(away)
                def _():
                    down_mid(0)
        second_step(0)

        @pl.when(home)
        def _():
            for q in range(parts):
                arrive(1, q)
                t3s[q] = dxacc[1, strip(col, q), :].astype(BF16)
                t3_copy(q, zf).start()
        collect(0)
        for q in range(parts):
            arrive(0, q)

            @pl.when(away)
            def _():
                t3s[q] = dxacc[0, strip(col, q), :].astype(BF16)
                t3_copy(q, zn).start()

            @pl.when(jnp.logical_and(home, core == 0))
            def _():
                own_copy(q).start()

        @pl.when(away)
        def _():
            for c in range(0 if chunks == 2 else 1, chunks - 1):
                down_mid(c)

    @pl.when(end)
    def _():
        for c in range(chunks - 1):
            gather(c)
            work_half(c)
            down_end(c)
        gather(chunks - 1)
        last_half(chunks - 1)
        down_end(chunks - 1)

        @pl.when(lead)
        def _():
            take_half().wait_recv()

    def y_copy(i, k, q, tp):
        ref = ybuf.at[strip(k, q)]
        return remote(ref, ref, sent.at[8], y_recv.at[i, q], z, tp)

    def y_sib(i, k, q):
        ref = ybuf.at[strip(k, q)]
        return remote(ref, ref, sent.at[9], y_recv.at[i, q], z, sib)

    def put(k, q):
        r = strip(k, q)
        return pltpu.make_async_copy(ybuf.at[r], dx_out.at[r], local_sem.at[3])

    dg_put = pltpu.make_async_copy(dgacc, dg_out, local_sem.at[4])

    def result(q, value):
        ybuf[strip(col, q), :] = value.astype(BF16)

    def down_final():
        @pl.when(home)
        def _():
            for g in range(chunks):
                dg_home(g).wait_recv()
            dgacc[...] += dgr[0].astype(F32)

        @pl.when(away)
        def _():
            for g in range(chunks):
                dg_far(g, 0).wait_recv()
            dg_direct(0).wait_recv()
            dgacc[...] = dgf[...].astype(F32)
            dgacc[:, span(chunks - 1)] += dge[...].astype(F32)

        dg_put.start()
    @pl.when(lead)
    def _():
        for q in range(parts):
            t3_copy(q, zn).wait_recv()

            @pl.when(end)
            def _():
                end_result(q)

            @pl.when(jnp.logical_and(near, home))
            def _():
                result(q, dxacc[0, strip(col, q), :] + t3r[q].astype(F32))

            @pl.when(jnp.logical_and(near, away))
            def _():
                own_copy(q).wait_recv()
                result(q, ownr[q] + t3r[q].astype(F32))
            y_copy(2, col, q, bd).start()
            y_copy(0, col, q, bx).start()
            y_copy(1, col, q, by).start()
            y_sib(0, col, q).start()
            put(col, q).start()
        down_final()
        for q in range(parts):
            for i, k, tp in ((0, col_x, bx), (1, col_y, by), (2, col_d, bd)):
                y_copy(i, k, q, tp).wait_recv()
                y_sib(i + 1, k, q).start()
                put(k, q).start()
    @pl.when(core == 0)
    def _():
        down_final()
        for q in range(parts):
            for i, k in enumerate((col, col_x, col_y, col_d)):
                y_sib(i, k, q).wait_recv()
                put(k, q).start()
    @pl.when(lead)
    def _():
        drain(ybuf.at[pl.ds(0, 3 * shard)], sent.at[8])
        drain(ybuf, sent.at[9])

    @pl.when(home)
    def _():
        drain(weights, sent.at[1])
        drain(dgs.at[0], sent.at[4])

    @pl.when(away)
    def _():
        drain(weights.at[pl.ds(0, shard)], sent.at[0])
        drain(dgs, sent.at[4])

    @pl.when(end)
    def _():
        drain(tally.at[pl.ds(0, shard)], sent.at[2])
        drain(hid.at[0, pl.ds(0, half_rows)], sent.at[3])
        drain(es, sent.at[5])

        @pl.when(home)
        def _():
            drain(weights.at[pl.ds(0, shard)], sent.at[0])

        @pl.when(core == 0)
        def _():
            drain(dxacc.at[0, pl.ds(0, shard), pl.ds(0, half_rows)], sent.at[10])

    @pl.when(near)
    def _():
        drain(tally, sent.at[2])
        drain(t3s, sent.at[7])

        @pl.when(home)
        def _():
            drain(weights.at[pl.ds(0, 3 * shard)], sent.at[0])
            drain(hid.at[pl.ds(0, 2)], sent.at[3])
            drain(t1s, sent.at[5])
            drain(t2s, sent.at[6])

            @pl.when(core == 0)
            def _():
                drain(ownr, sent.at[10])

        @pl.when(away)
        def _():
            drain(hid.at[0], sent.at[3])
            drain(t1s.at[0], sent.at[5])
            drain(t2s.at[0], sent.at[6])

    drain(ybuf, local_sem.at[3])
    dg_put.wait()


def per_device_kernel(n, tokens, cotangent, gate_weight, up_weight, down_weight):
    rows, depth = tokens.shape
    shard, ff = gate_weight.shape
    chunks = ff // LANES
    parts = next(p for p in (3, 2, 1) if shard % (p * SUB) == 0)
    piece = shard // parts
    vmem, dma = pltpu.VMEM, pltpu.SemaphoreType.DMA
    dx, dg = pl.pallas_call(
        functools.partial(kernel, n),
        out_shape=(vmem((depth, rows), BF16), vmem((shard, ff), F32)),
        in_specs=[pl.BlockSpec(memory_space=pltpu.HBM)] * 5,
        out_specs=[pl.BlockSpec(memory_space=pl.ANY)] * 2,
        scratch_shapes=[
            vmem((depth, rows), BF16), vmem((depth, rows), BF16),
            vmem((shard, ff), BF16), vmem((shard, ff), BF16), vmem((shard, ff), BF16),
            vmem((depth, 3 * ff), BF16),
            vmem((2, rows, depth), BF16), vmem((2, rows, depth), BF16),
            vmem((depth, rows), BF16), vmem((depth, rows), BF16),
            vmem((depth, rows), BF16), vmem((depth, rows), BF16),
            vmem((2, depth, rows), F32),
            vmem((3, rows, ff), BF16),
            vmem((shard, ff), F32), vmem((2, shard, ff), F32), vmem((2, shard, ff), BF16),
            vmem((2, shard, ff), BF16), vmem((shard, ff), BF16), vmem((shard, LANES), BF16),
            vmem((2, 2, 2, shard, rows // 2), BF16), vmem((2, 2, 2, shard, rows // 2), BF16),
            vmem((2, 2, parts, piece, rows // 2), BF16), vmem((2, 2, parts, piece, rows // 2), BF16),
            vmem((parts, piece, rows), BF16), vmem((parts, piece, rows), BF16),
            vmem((3, parts, piece, rows // 2), BF16), vmem((parts, 2, 3, piece, rows // 2), BF16),
            vmem((parts, piece, rows), F32),
            vmem((depth, rows), BF16),
            vmem((9 * shard, rows), BF16),
            dma((11,)), dma((chunks, 3, 3)), dma((18,)), dma((2, chunks)), dma((chunks,)), dma((chunks,)), dma((1,)),
            dma((2, 2, 2)), dma((2, 2, parts)), dma((parts,)), dma((parts,)), dma((parts,)),
            dma((4, parts)), dma((5,)),
        ],
        compiler_params=pltpu.CompilerParams(
            collective_id=0, has_side_effects=True, vmem_limit_bytes=40 * 2**20),
    )(*(pltpu.with_memory_space_constraint(a, pltpu.HBM) for a in (
        tokens.T, cotangent.T, gate_weight, up_weight, down_weight.T)))
    return dx.T, dg.T


def solution(mesh):
    n, tp = mesh.shape["fs"], mesh.shape["tp"]

    def per_device(tokens, cotangent, gate_weight, up_weight, down_weight):
        rows, depth = tokens.shape
        shard, ff = gate_weight.shape
        args = (tokens, cotangent, gate_weight, up_weight, down_weight)
        fits = (tp == 8 and n == 4 and rows % (2 * LANES) == 0 and rows <= 256
                and depth == n * shard and shard % SUB == 0 and ff % LANES == 0
                and LANES < ff <= 512 and depth <= 2048)
        return per_device_kernel(n, *args) if fits else per_device_plain(*args)

    placed = (P("fs", None), P("fs", None), P("fs", "tp"), P("fs", "tp"), P("tp", "fs"))
    return jax.shard_map(
        per_device,
        mesh=mesh,
        in_specs=placed,
        out_specs=(P("fs", None), P("tp", "fs")),
        check_vma=False,
    )
```

```python
import functools

import jax
import jax.numpy as jnp
from jax import lax
from jax.experimental import pallas as pl
from jax.experimental.pallas import tpu as pltpu
from jax.sharding import PartitionSpec as P

LANES = 128
SUB = 16
BF16 = jnp.bfloat16
F32 = jnp.float32


def contract_rows(left, right):
    return lax.dot_general(
        left, right, (((0,), (0,)), ((), ())), preferred_element_type=jnp.float32
    )


def contract_cols(left, right):
    return lax.dot_general(
        left, right, (((1,), (1,)), ((), ())), preferred_element_type=jnp.float32
    )


def send_down(hidden, cotangent):
    return lax.psum_scatter(
        contract_rows(cotangent, hidden), "fs", scatter_dimension=0, tiled=True
    ).T


def per_device_plain(tokens, cotangent, gate_weight, up_weight, down_weight):
    whole_gate, whole_up, whole_down = (
        lax.all_gather(gate_weight, "fs", axis=0, tiled=True),
        lax.all_gather(up_weight, "fs", axis=0, tiled=True),
        lax.all_gather(down_weight, "fs", axis=1, tiled=True),
    )
    gate_pre = jnp.dot(tokens, whole_gate, preferred_element_type=jnp.float32)
    up_pre = jnp.dot(tokens, whole_up, preferred_element_type=jnp.float32)
    hidden_grad = contract_cols(cotangent, whole_down)
    sigmoid_gate = jax.nn.sigmoid(gate_pre)
    activated = gate_pre * sigmoid_gate
    hidden = (activated * up_pre).astype(jnp.bfloat16)
    gate_pre_grad = (
        hidden_grad * up_pre * sigmoid_gate * (1.0 + gate_pre * (1.0 - sigmoid_gate))
    ).astype(jnp.bfloat16)
    up_pre_grad = (hidden_grad * activated).astype(jnp.bfloat16)
    partial_value = contract_cols(gate_pre_grad, whole_gate) + contract_cols(up_pre_grad, whole_up)
    input_grad = lax.psum(partial_value.astype(jnp.bfloat16), "tp")
    down_grad = send_down(hidden, cotangent)
    return (input_grad, down_grad)


def kernel(n, tok_hbm, cot_hbm, gate_hbm, up_hbm, down_hbm, ybuf, dgacc,
           tok_ref, cot_ref, gate_ref, up_ref, down_ref, weights, tok, cot,
           ptok, pcot, etok, ecot, dxacc, hid, dgp, dgs, dgr, dgf, dge,
           t1s, t1r, t2s, t2r, t3s, t3r, es, er, ownr, tally,
           sent, w_recv, tk_recv, hid_recv, dg_recv, dgf_recv, dge_recv, t1_recv, t2_recv,
           t3_recv, e_recv, own_recv, y_recv, local_sem):
    z = lax.axis_index("fs")
    b = lax.axis_index("tp")
    depth, rows = tok_ref.shape
    shard, ff = gate_ref.shape
    chunks = ff // LANES
    parts, piece = t2s.shape[2], t2s.shape[3]
    half_rows = rows // 2
    core = lax.rem(b, 2)
    col = lax.div(b, 2)
    cx = lax.rem(col, 2)
    cy = lax.div(col, 2)
    side = lax.div(z, 2)
    zodd = lax.rem(z, 2)
    home = core == side
    away = core != side
    near = side != zodd
    end = side == zodd
    lead = core == 1
    sib = b + 1 - 2 * core
    bx = b + 2 * (1 - 2 * cx)
    by = b + 4 * (1 - 2 * cy)
    bd = bx + by - b
    last = 2 * col + 1
    zs = z + 1 - 2 * zodd
    zn = 2 - side
    zf = 3 - 3 * side
    me = jnp.where(home, 0, 1)
    col_x = 2 * cy + 1 - cx
    col_y = 2 * (1 - cy) + cx
    col_d = 2 * (1 - cy) + 1 - cx
    for src, dst, i in ((tok_hbm, tok_ref, 0), (cot_hbm, cot_ref, 0), (gate_hbm, gate_ref, 1),
                        (up_hbm, up_ref, 1), (down_hbm, down_ref, 1)):
        pltpu.make_async_copy(src, dst, local_sem.at[i]).start()

    def drain(ref, sem):
        pltpu.make_async_copy(ref, ref, sem).wait()

    barrier = pltpu.get_barrier_semaphore()

    def greet(fs, tp):
        pl.semaphore_signal(barrier, inc=1, device_id={"fs": fs, "tp": tp},
                            device_id_type=pl.DeviceIdType.MESH)

    greet(z, sib)
    greet(z, bx)
    greet(z, by)
    greet(z, bd)
    for step in range(1, n):
        greet(lax.rem(z + step, n), b)
        greet(lax.rem(z + step, n), sib)
    pl.semaphore_wait(barrier, 4 + 2 * (n - 1))
    drain(tally.at[pl.ds(0, 2 * depth)], local_sem.at[0])
    drain(weights.at[pl.ds(0, shard)], local_sem.at[1])

    def remote(src, dst, send, recv, fs, tp):
        return pltpu.make_async_remote_copy(
            src_ref=src, dst_ref=dst, send_sem=send, recv_sem=recv,
            device_id={"fs": fs, "tp": tp}, device_id_type=pl.DeviceIdType.MESH)

    def rows_of(k, count=1):
        return pl.ds(pl.multiple_of(k * shard, SUB), count * shard)

    def lanes_of(c, count=1):
        return pl.ds(c * LANES, count * LANES)

    def slot(c, k, kind):
        return weights.at[rows_of(k), lanes_of(3 * c + kind)]

    def own(c, kind):
        return (gate_ref, up_ref, down_ref)[kind].at[:, lanes_of(c)]

    def w_copy(src, c, k, kind, i, fs):
        return remote(src, slot(c, k, kind), sent.at[0], w_recv.at[c, i, kind], fs, b)

    def sib_copy(src, c, k, kind):
        return remote(src, slot(c, k, kind), sent.at[1], w_recv.at[c, 0, 0], z, sib)

    every = [(c, kind) for c in range(chunks) for kind in range(3)]
    others = (zs, zn, zf)
    mine_q = rows_of(col)

    def tk_copy(i, src, dst, fs, tp):
        return remote(src, dst, sent.at[2], tk_recv.at[i], fs, tp)

    def tok_buf(e):
        return etok if e else ptok

    def cot_buf(e):
        return ecot if e else pcot

    def spread(i, e, q, tp):
        buf = cot_buf(e) if i in (1, 4, 5, 7) else tok_buf(e)
        ref = buf.at[rows_of(q)]
        return tk_copy(8 * e + (3 if i in (4, 6, 7) else i), ref, ref, z, tp)

    def spread_first(e):
        spread(0, e, col, bx).wait_recv()
        spread(2, e, col, bx).start()
        spread(3, e, col, by).start()
        spread(1, e, col, bx).wait_recv()
        spread(4, e, col, bx).start()
        spread(5, e, col, by).start()

    def spread_second(e):
        spread(2, e, col_x, bx).wait_recv()
        spread(6, e, col_x, by).start()
        spread(5, e, col_y, by).wait_recv()
        spread(7, e, col_y, bx).start()

    def spread_rest(e):
        drain(tally.at[pl.ds(0, 4 * shard)], tk_recv.at[8 * e + 3])

    far_rows = rows_of(2 * (1 - core), 2)
    give = tk_copy(16, pcot.at[far_rows], pcot.at[far_rows], z, sib)
    give_extra = tk_copy(17, ecot.at[far_rows], ecot.at[far_rows], z, sib)
    half_me = pl.ds(pl.multiple_of(me * half_rows, LANES), half_rows)
    @pl.when(end)
    def _():
        @pl.when(home)
        def _():
            tk_copy(8, tok_ref.at[mine_q], etok.at[mine_q], zn, sib).start()

        @pl.when(away)
        def _():
            tk_copy(9, cot_ref.at[mine_q], ecot.at[mine_q], zn, b).start()

    @pl.when(near)
    def _():
        @pl.when(home)
        def _():
            tk_copy(0, tok_ref.at[mine_q], ptok.at[mine_q], zn, b).start()

        @pl.when(away)
        def _():
            tk_copy(1, cot_ref.at[mine_q], pcot.at[mine_q], zn, sib).start()

    @pl.when(home)
    def _():
        for c, kind in every:
            w_copy(own(c, kind), c, z, kind, 0, zs).start()
            sib_copy(own(c, kind), c, z, kind).start()
            pltpu.make_async_copy(own(c, kind), slot(c, z, kind), local_sem.at[2]).start()

    @pl.when(away)
    def _():
        for c, kind in every:
            w_copy(own(c, kind), c, z, kind, jnp.where(near, 1, 2), zn).start()

    @pl.when(end)
    def _():
        tok[0, :half_rows] = tok_ref[:, half_me].T
        cot[0, :half_rows] = cot_ref[:, half_me].T

    @pl.when(jnp.logical_and(near, home))
    def _():
        tok[0] = tok_ref[...].T
        cot[0] = cot_ref[...].T
        spread_first(1)
        spread_second(1)

    @pl.when(jnp.logical_and(near, away))
    def _():
        spread_first(0)
        spread_second(0)
        spread_rest(0)
        give.start()
        tok[0] = ptok[...].T
        cot[0] = pcot[...].T

    def relay(c, kind):
        for i, k in enumerate(others):
            there = slot(c, k, kind)
            w_copy(there, c, k, kind, i, zs).wait_recv()
            if i:
                @pl.when(near)
                def _():
                    w_copy(there, c, k, kind, i, zs).start()
            sib_copy(there, c, k, kind).start()

    def relay_all(c):
        for kind in range(3):
            relay(c, kind)
        if c == 0:
            drain(weights.at[rows_of(z)], local_sem.at[2])

    def gather_sib(c):
        drain(weights.at[:, lanes_of(3 * c, 3)], w_recv.at[c, 0, 0])

    def gather(c):
        @pl.when(home)
        def _():
            relay_all(c)

        @pl.when(away)
        def _():
            gather_sib(c)

    def hid_copy(e, c, ref):
        return remote(ref, ref, sent.at[3], hid_recv.at[e, c], z, sib)

    def hid_ref(e, c):
        return hid.at[2 if e else me, :, lanes_of(c)]

    def hid_half(c):
        return hid.at[0, pl.ds(pl.multiple_of(me * half_rows, SUB), half_rows), lanes_of(c)]

    def activate(x, y, c, out, e):
        pre = jnp.dot(x, weights[:, 3 * c * LANES:(3 * c + 2) * LANES],
                      preferred_element_type=F32)
        hg = jnp.dot(y, weights[:, (3 * c + 2) * LANES:(3 * c + 3) * LANES],
                     preferred_element_type=F32)
        gate_pre, up_pre = pre[:, :LANES], pre[:, LANES:]
        sig = jax.nn.sigmoid(gate_pre)
        act = gate_pre * sig
        out[...] = (act * up_pre).astype(BF16)
        hid_copy(e, c, out).start()
        return jnp.concatenate(
            [(hg * up_pre * sig * (1.0 + gate_pre * (1.0 - sig))).astype(BF16),
             (hg * act).astype(BF16)], axis=1)

    def begin(e, c):
        return activate(tok[e], cot[e], c, hid_ref(e, c), e)

    def finish(e, c, dgu):
        value = contract_cols(weights[:, 3 * c * LANES:(3 * c + 2) * LANES], dgu)
        if c == 0:
            dxacc[e] = value
        else:
            dxacc[e] += value

    def take_tokens():
        spread_rest(1)
        give_extra.start()
        tok[1] = etok[...].T
        cot[1] = ecot[...].T

    def work_half(c):
        dgu = activate(tok[0, :half_rows], cot[0, :half_rows], c, hid_half(c), 0)
        value = contract_cols(weights[:, 3 * c * LANES:(3 * c + 2) * LANES], dgu)
        if c == 0:
            dxacc[0, :, half_me] = value
        else:
            dxacc[0, :, half_me] += value

    halves = (slice(0, half_rows), slice(half_rows, rows))

    def t1_copy(e, i, step):
        return remote(t1s.at[e, i, step], t1r.at[e, i, step], sent.at[5], t1_recv.at[e, step],
                      z, bx if i == 0 else by)

    def t2_copy(e, i, q):
        return remote(t2s.at[e, i, q], t2r.at[e, i, q], sent.at[6], t2_recv.at[e, q],
                      z, by if i == 0 else bx)

    def t3_copy(q, fs):
        return remote(t3s.at[q], t3r.at[q], sent.at[7], t3_recv.at[q], fs, last)

    def strip(k, q):
        return pl.ds(pl.multiple_of(k * shard + q * piece, SUB), piece)

    def own_copy(q):
        return remote(dxacc.at[0, strip(col, q)], ownr.at[q], sent.at[10], own_recv.at[q], z, sib)

    def work_last(e, c):
        dgu = activate(tok[e], cot[e], c, hid_ref(e, c), e)
        for k, sends in ((col_d, ((0, 0), (1, 0))), (col_x, ((0, 1),)), (col_y, ((1, 1),)), (col, ())):
            r = rows_of(k)
            value = contract_cols(weights[r, 3 * c * LANES:(3 * c + 2) * LANES], dgu) + dxacc[e, r, :]
            if k is not col_d:
                dxacc[e, r, :] = value
            for i, step in sends:
                t1s[e, i, step] = value[:, halves[i]].astype(BF16)
                t1_copy(e, i, step).start()

    there = pl.ds(pl.multiple_of((1 - me) * half_rows, LANES), half_rows)

    def e_copy(i, q, tp):
        return remote(es.at[i, q], er.at[q, me, i], sent.at[5], e_recv.at[q], z, tp + 1 - core)

    def own_half():
        ref = dxacc.at[0, rows_of(col), half_me]
        return remote(ref, ref, sent.at[10], own_recv.at[0], z, sib)

    def take_half():
        ref = dxacc.at[0, rows_of(col), there]
        return remote(ref, ref, sent.at[10], own_recv.at[0], z, sib)

    def last_half(c):
        dgu = activate(tok[0, :half_rows], cot[0, :half_rows], c, hid_half(c), 0)
        columns = pl.ds(3 * c * LANES, 2 * LANES)
        for q in range(parts):
            for i, (k, tp) in enumerate(((col_d, bd), (col_x, bx), (col_y, by))):
                r = strip(k, q)
                es[i, q] = (contract_cols(weights[r, columns], dgu) + dxacc[0, r, half_me]).astype(BF16)
                e_copy(i, q, tp).start()
        r = rows_of(col)
        dxacc[0, r, half_me] += contract_cols(weights[r, columns], dgu)

        @pl.when(core == 0)
        def _():
            own_half().start()

    def end_result(q):
        drain(er.at[q], e_recv.at[q])
        r = strip(col, q)
        for i in range(2):
            total = dxacc[0, r, halves[i]] + t3r[q, :, halves[i]].astype(F32)
            for k in range(3):
                total = total + er[q, i, k].astype(F32)
            ybuf[r, halves[i]] = total.astype(BF16)

    def second_step(e):
        drain(t1r.at[e, :, 0], t1_recv.at[e, 0])
        for q in range(parts):
            inner = slice(q * piece, (q + 1) * piece)
            for i, k in ((0, col_y), (1, col_x)):
                t2s[e, i, q] = (dxacc[e, strip(k, q), halves[i]]
                                + t1r[e, i, 0, inner].astype(F32)).astype(BF16)
                t2_copy(e, i, q).start()

    def collect(e):
        drain(t1r.at[e, :, 1], t1_recv.at[e, 1])
        for q in range(parts):
            inner = slice(q * piece, (q + 1) * piece)
            for i in range(2):
                dxacc[e, strip(col, q), halves[i]] += t1r[e, i, 1, inner].astype(F32)

    def arrive(e, q):
        drain(t2r.at[e, :, q], t2_recv.at[e, q])
        for i in range(2):
            dxacc[e, strip(col, q), halves[i]] += t2r[e, i, q].astype(F32)

    def span(c):
        return slice(c * LANES, (c + 1) * LANES)

    def dg_home(g):
        lanes = lanes_of(g)
        return remote(dgs.at[0, :, lanes], dgr.at[0, :, lanes], sent.at[4], dg_recv.at[g], zs, b)

    def dg_away(g):
        lanes = lanes_of(g)
        return remote(dgs.at[:, :, lanes], dgr.at[:, :, lanes], sent.at[4], dg_recv.at[g], zs, b)

    def dg_far(g, i):
        lanes = lanes_of(g)
        return remote(dgs.at[i, :, lanes], dgf.at[:, lanes], sent.at[4], dgf_recv.at[g],
                      2 * (1 - side) + i, sib)

    def dg_direct(i):
        return remote(dgs.at[i, :, lanes_of(chunks - 1)], dge, sent.at[4], dge_recv.at[0],
                      2 * (1 - side) + i, sib)

    def keep_part(g, i, value):
        lanes = span(g)

        @pl.when(jnp.logical_and(home, zodd == i))
        def _():
            dgacc[:, lanes] = value

        @pl.when(jnp.logical_and(home, zodd != i))
        def _():
            dgs[0, :, lanes] = value.astype(BF16)

        if g == chunks - 1:
            @pl.when(away)
            def _():
                dgs[i, :, lanes] = value.astype(BF16)

                @pl.when(near)
                def _():
                    dg_far(g, i).start()

                @pl.when(end)
                def _():
                    dg_direct(i).start()
        else:
            @pl.when(jnp.logical_and(away, near))
            def _():
                dgp[i, :, lanes] = value

            @pl.when(jnp.logical_and(away, end))
            def _():
                dgs[i, :, lanes] = value.astype(BF16)

    def down_near(g):
        hid_copy(0, g, hid.at[1 - me, :, lanes_of(g)]).wait_recv()

        @pl.when(away)
        def _():
            hid_copy(1, g, hid.at[2, :, lanes_of(g)]).wait_recv()

        lanes = span(g)
        for i in range(2):
            k = rows_of(2 * core + i)
            keep_part(g, i, jnp.dot(cot_ref[k, :], hid[0, :, lanes], preferred_element_type=F32)
                      + jnp.dot(pcot[k, :], hid[1, :, lanes], preferred_element_type=F32)
                      + jnp.dot(ecot[k, :], hid[2, :, lanes], preferred_element_type=F32))

    def down_end(g):
        other = hid.at[0, pl.ds(pl.multiple_of((1 - me) * half_rows, SUB), half_rows), lanes_of(g)]
        hid_copy(0, g, other).wait_recv()
        for i in range(2):
            k = rows_of(2 * core + i)
            keep_part(g, i, jnp.dot(cot_ref[k, :], hid[0, :, span(g)], preferred_element_type=F32))

        @pl.when(home)
        def _():
            dg_home(g).start()

        if g < chunks - 1:
            @pl.when(away)
            def _():
                dg_away(g).start()

    def down_mid(g):
        lanes = span(g)
        dg_away(g).wait_recv()
        for i in range(2):
            dgs[i, :, lanes] = (dgp[i, :, lanes] + dgr[i, :, lanes].astype(F32)).astype(BF16)
            dg_far(g, i).start()
    @pl.when(near)
    def _():

        @pl.when(home)
        def _():
            relay_all(0)
            for c in range(chunks - 1):
                dgu = begin(0, c)
                relay(c + 1, 0)
                finish(0, c, dgu)
                if c == 0:
                    take_tokens()
                relay(c + 1, 1)
                finish(1, c, begin(1, c))
                relay(c + 1, 2)

        @pl.when(away)
        def _():
            for c in range(chunks - 1):
                gather_sib(c)
                finish(0, c, begin(0, c))
            gather_sib(chunks - 1)

        @pl.when(home)
        def _():
            work_last(1, chunks - 1)
        work_last(0, chunks - 1)

        @pl.when(home)
        def _():
            second_step(1)
            collect(1)

        @pl.when(home)
        def _():
            give.wait_recv()

        @pl.when(away)
        def _():
            give_extra.wait_recv()

        for c in range(chunks):
            down_near(c)

            @pl.when(home)
            def _():
                dg_home(c).start()

            if c == 0 and chunks > 2:
                @pl.when(away)
                def _():
                    down_mid(0)
        second_step(0)

        @pl.when(home)
        def _():
            for q in range(parts):
                arrive(1, q)
                t3s[q] = dxacc[1, strip(col, q), :].astype(BF16)
                t3_copy(q, zf).start()
        collect(0)
        for q in range(parts):
            arrive(0, q)

            @pl.when(away)
            def _():
                t3s[q] = dxacc[0, strip(col, q), :].astype(BF16)
                t3_copy(q, zn).start()

            @pl.when(jnp.logical_and(home, core == 0))
            def _():
                own_copy(q).start()

        @pl.when(away)
        def _():
            for c in range(0 if chunks == 2 else 1, chunks - 1):
                down_mid(c)

    @pl.when(end)
    def _():
        for c in range(chunks - 1):
            gather(c)
            work_half(c)
            down_end(c)
        gather(chunks - 1)
        last_half(chunks - 1)
        down_end(chunks - 1)

        @pl.when(lead)
        def _():
            take_half().wait_recv()

    def y_copy(i, k, q, tp):
        ref = ybuf.at[strip(k, q)]
        return remote(ref, ref, sent.at[8], y_recv.at[q], z, tp)

    def y_sib(i, k, q):
        ref = ybuf.at[strip(k, q)]
        return remote(ref, ref, sent.at[9], y_recv.at[q], z, sib)

    def result(q, value):
        ybuf[strip(col, q), :] = value.astype(BF16)

    def down_final():
        @pl.when(home)
        def _():
            for g in range(chunks):
                dg_home(g).wait_recv()
            dgacc[...] += dgr[0].astype(F32)

        @pl.when(away)
        def _():
            for g in range(chunks):
                dg_far(g, 0).wait_recv()
            dg_direct(0).wait_recv()
            dgacc[...] = dgf[...].astype(F32)
            dgacc[:, span(chunks - 1)] += dge[...].astype(F32)
    @pl.when(lead)
    def _():
        for q in range(parts):
            t3_copy(q, zn).wait_recv()

            @pl.when(end)
            def _():
                end_result(q)

            @pl.when(jnp.logical_and(near, home))
            def _():
                result(q, dxacc[0, strip(col, q), :] + t3r[q].astype(F32))

            @pl.when(jnp.logical_and(near, away))
            def _():
                own_copy(q).wait_recv()
                result(q, ownr[q] + t3r[q].astype(F32))
            y_copy(2, col, q, bd).start()
            y_copy(0, col, q, bx).start()
            y_copy(1, col, q, by).start()
            y_sib(0, col, q).start()
        down_final()
        for q in range(parts):
            drain(tally.at[pl.ds(0, 3 * piece)], y_recv.at[q])
            for i, k in enumerate((col_x, col_y, col_d)):
                y_sib(i + 1, k, q).start()
    @pl.when(core == 0)
    def _():
        down_final()
        for q in range(parts):
            drain(tally.at[pl.ds(0, 4 * piece)], y_recv.at[q])
    @pl.when(lead)
    def _():
        drain(ybuf.at[pl.ds(0, 3 * shard)], sent.at[8])
        drain(ybuf, sent.at[9])

    @pl.when(home)
    def _():
        drain(weights, sent.at[1])
        drain(dgs.at[0], sent.at[4])

    @pl.when(away)
    def _():
        drain(weights.at[pl.ds(0, shard)], sent.at[0])
        drain(dgs, sent.at[4])

    @pl.when(end)
    def _():
        drain(tally.at[pl.ds(0, shard)], sent.at[2])
        drain(hid.at[0, pl.ds(0, half_rows)], sent.at[3])
        drain(es, sent.at[5])

        @pl.when(home)
        def _():
            drain(weights.at[pl.ds(0, shard)], sent.at[0])

        @pl.when(core == 0)
        def _():
            drain(dxacc.at[0, pl.ds(0, shard), pl.ds(0, half_rows)], sent.at[10])

    @pl.when(near)
    def _():
        drain(tally, sent.at[2])
        drain(t3s, sent.at[7])

        @pl.when(home)
        def _():
            drain(weights.at[pl.ds(0, 3 * shard)], sent.at[0])
            drain(hid.at[pl.ds(0, 2)], sent.at[3])
            drain(t1s, sent.at[5])
            drain(t2s, sent.at[6])

            @pl.when(core == 0)
            def _():
                drain(ownr, sent.at[10])

        @pl.when(away)
        def _():
            drain(hid.at[0], sent.at[3])
            drain(t1s.at[0], sent.at[5])
            drain(t2s.at[0], sent.at[6])


def store_kernel(dx_in, dg_in, dx_out, dg_out, sem):
    copies = [pltpu.make_async_copy(src, dst, sem.at[i])
              for i, (src, dst) in enumerate(((dx_in, dx_out), (dg_in, dg_out)))]
    for copy in copies:
        copy.start()
    for copy in copies:
        copy.wait()


def per_device_kernel(n, tokens, cotangent, gate_weight, up_weight, down_weight):
    rows, depth = tokens.shape
    shard, ff = gate_weight.shape
    chunks = ff // LANES
    parts = next(p for p in (3, 2, 1) if shard % (p * SUB) == 0)
    piece = shard // parts
    vmem, dma = pltpu.VMEM, pltpu.SemaphoreType.DMA
    dx, dg = pl.pallas_call(
        functools.partial(kernel, n),
        out_shape=(vmem((depth, rows), BF16), vmem((shard, ff), F32)),
        in_specs=[pl.BlockSpec(memory_space=pltpu.HBM)] * 5,
        out_specs=[pl.BlockSpec(memory_space=vmem)] * 2,
        scratch_shapes=[
            vmem((depth, rows), BF16), vmem((depth, rows), BF16),
            vmem((shard, ff), BF16), vmem((shard, ff), BF16), vmem((shard, ff), BF16),
            vmem((depth, 3 * ff), BF16),
            vmem((2, rows, depth), BF16), vmem((2, rows, depth), BF16),
            vmem((depth, rows), BF16), vmem((depth, rows), BF16),
            vmem((depth, rows), BF16), vmem((depth, rows), BF16),
            vmem((2, depth, rows), F32),
            vmem((3, rows, ff), BF16),
            vmem((2, shard, ff), F32), vmem((2, shard, ff), BF16),
            vmem((2, shard, ff), BF16), vmem((shard, ff), BF16), vmem((shard, LANES), BF16),
            vmem((2, 2, 2, shard, rows // 2), BF16), vmem((2, 2, 2, shard, rows // 2), BF16),
            vmem((2, 2, parts, piece, rows // 2), BF16), vmem((2, 2, parts, piece, rows // 2), BF16),
            vmem((parts, piece, rows), BF16), vmem((parts, piece, rows), BF16),
            vmem((3, parts, piece, rows // 2), BF16), vmem((parts, 2, 3, piece, rows // 2), BF16),
            vmem((parts, piece, rows), F32),
            vmem((9 * shard, rows), BF16),
            dma((11,)), dma((chunks, 3, 3)), dma((18,)), dma((2, chunks)), dma((chunks,)), dma((chunks,)), dma((1,)),
            dma((2, 2)), dma((2, parts)), dma((parts,)), dma((parts,)), dma((parts,)),
            dma((parts,)), dma((3,)),
        ],
        compiler_params=pltpu.CompilerParams(
            collective_id=0, has_side_effects=True, vmem_limit_bytes=40 * 2**20),
    )(*(pltpu.with_memory_space_constraint(a, pltpu.HBM) for a in (
        tokens.T, cotangent.T, gate_weight, up_weight, down_weight.T)))
    dx, dg = pl.pallas_call(
        store_kernel,
        out_shape=(pltpu.HBM((depth, rows), BF16), pltpu.HBM((shard, ff), F32)),
        in_specs=[pl.BlockSpec(memory_space=pl.ANY)] * 2,
        out_specs=[pl.BlockSpec(memory_space=pl.ANY)] * 2,
        scratch_shapes=[dma((2,))],
        compiler_params=pltpu.CompilerParams(vmem_limit_bytes=2**20),
    )(dx, dg)
    return dx.T, dg.T


def solution(mesh):
    n, tp = mesh.shape["fs"], mesh.shape["tp"]

    def per_device(tokens, cotangent, gate_weight, up_weight, down_weight):
        rows, depth = tokens.shape
        shard, ff = gate_weight.shape
        args = (tokens, cotangent, gate_weight, up_weight, down_weight)
        fits = (tp == 8 and n == 4 and rows % (2 * LANES) == 0 and rows <= 256
                and depth == n * shard and shard % SUB == 0 and ff % LANES == 0
                and LANES < ff <= 512 and depth <= 2048)
        return per_device_kernel(n, *args) if fits else per_device_plain(*args)

    placed = (P("fs", None), P("fs", None), P("fs", "tp"), P("fs", "tp"), P("tp", "fs"))
    return jax.shard_map(
        per_device,
        mesh=mesh,
        in_specs=placed,
        out_specs=(P("fs", None), P("tp", "fs")),
        check_vma=False,
    )
```

```python
import functools

import jax
import jax.numpy as jnp
from jax import lax
from jax.experimental import pallas as pl
from jax.experimental.pallas import tpu as pltpu
from jax.sharding import PartitionSpec as P

LANES = 128
SUB = 16
BF16 = jnp.bfloat16
F32 = jnp.float32


def contract_rows(left, right):
    return lax.dot_general(
        left, right, (((0,), (0,)), ((), ())), preferred_element_type=jnp.float32
    )


def contract_cols(left, right):
    return lax.dot_general(
        left, right, (((1,), (1,)), ((), ())), preferred_element_type=jnp.float32
    )


def send_down(hidden, cotangent):
    return lax.psum_scatter(
        contract_rows(cotangent, hidden), "fs", scatter_dimension=0, tiled=True
    ).T


def per_device_plain(tokens, cotangent, gate_weight, up_weight, down_weight):
    whole_gate, whole_up, whole_down = (
        lax.all_gather(gate_weight, "fs", axis=0, tiled=True),
        lax.all_gather(up_weight, "fs", axis=0, tiled=True),
        lax.all_gather(down_weight, "fs", axis=1, tiled=True),
    )
    gate_pre = jnp.dot(tokens, whole_gate, preferred_element_type=jnp.float32)
    up_pre = jnp.dot(tokens, whole_up, preferred_element_type=jnp.float32)
    hidden_grad = contract_cols(cotangent, whole_down)
    sigmoid_gate = jax.nn.sigmoid(gate_pre)
    activated = gate_pre * sigmoid_gate
    hidden = (activated * up_pre).astype(jnp.bfloat16)
    gate_pre_grad = (
        hidden_grad * up_pre * sigmoid_gate * (1.0 + gate_pre * (1.0 - sigmoid_gate))
    ).astype(jnp.bfloat16)
    up_pre_grad = (hidden_grad * activated).astype(jnp.bfloat16)
    partial_value = contract_cols(gate_pre_grad, whole_gate) + contract_cols(up_pre_grad, whole_up)
    input_grad = lax.psum(partial_value.astype(jnp.bfloat16), "tp")
    down_grad = send_down(hidden, cotangent)
    return (input_grad, down_grad)


def kernel(n, tok_hbm, cot_hbm, gate_hbm, up_hbm, down_hbm, ybuf, dgacc,
           tok_ref, cot_ref, gate_ref, up_ref, down_ref, weights, tok, cot,
           ptok, pcot, etok, ecot, dxacc, hid, dgp, dgs, dgr, dgf, dge,
           t1s, t1r, t2s, t2r, t3s, t3r, es, er, ownr, tally,
           sent, w_recv, tk_recv, hid_recv, dg_recv, dgf_recv, dge_recv, t1_recv, t2_recv,
           t3_recv, e_recv, own_recv, y_recv, local_sem):
    z = lax.axis_index("fs")
    b = lax.axis_index("tp")
    depth, rows = tok_ref.shape
    shard, ff = gate_ref.shape
    chunks = ff // LANES
    parts, piece = t2s.shape[2], t2s.shape[3]
    half_rows = rows // 2
    core = lax.rem(b, 2)
    col = lax.div(b, 2)
    cx = lax.rem(col, 2)
    cy = lax.div(col, 2)
    side = lax.div(z, 2)
    zodd = lax.rem(z, 2)
    home = core == side
    away = core != side
    near = side != zodd
    end = side == zodd
    lead = core == 1
    sib = b + 1 - 2 * core
    bx = b + 2 * (1 - 2 * cx)
    by = b + 4 * (1 - 2 * cy)
    bd = bx + by - b
    last = 2 * col + 1
    zs = z + 1 - 2 * zodd
    zn = 2 - side
    zf = 3 - 3 * side
    me = jnp.where(home, 0, 1)
    col_x = 2 * cy + 1 - cx
    col_y = 2 * (1 - cy) + cx
    col_d = 2 * (1 - cy) + 1 - cx
    for src, dst, i in ((tok_hbm, tok_ref, 0), (cot_hbm, cot_ref, 0), (gate_hbm, gate_ref, 1),
                        (up_hbm, up_ref, 1), (down_hbm, down_ref, 1)):
        pltpu.make_async_copy(src, dst, local_sem.at[i]).start()

    def drain(ref, sem):
        pltpu.make_async_copy(ref, ref, sem).wait()

    barrier = pltpu.get_barrier_semaphore()

    def greet(fs, tp):
        pl.semaphore_signal(barrier, inc=1, device_id={"fs": fs, "tp": tp},
                            device_id_type=pl.DeviceIdType.MESH)

    greet(z, sib)
    greet(z, bx)
    greet(z, by)
    greet(z, bd)
    for step in range(1, n):
        greet(lax.rem(z + step, n), b)
        greet(lax.rem(z + step, n), sib)
    pl.semaphore_wait(barrier, 4 + 2 * (n - 1))
    drain(tally.at[pl.ds(0, 2 * depth)], local_sem.at[0])
    drain(weights.at[pl.ds(0, shard)], local_sem.at[1])

    def remote(src, dst, send, recv, fs, tp):
        return pltpu.make_async_remote_copy(
            src_ref=src, dst_ref=dst, send_sem=send, recv_sem=recv,
            device_id={"fs": fs, "tp": tp}, device_id_type=pl.DeviceIdType.MESH)

    def rows_of(k, count=1):
        return pl.ds(pl.multiple_of(k * shard, SUB), count * shard)

    def lanes_of(c, count=1):
        return pl.ds(c * LANES, count * LANES)

    def slot(c, k, kind):
        return weights.at[rows_of(k), lanes_of(3 * c + kind)]

    def own(c, kind):
        return (gate_ref, up_ref, down_ref)[kind].at[:, lanes_of(c)]

    def w_copy(src, c, k, kind, i, fs):
        return remote(src, slot(c, k, kind), sent.at[0], w_recv.at[c, i, kind], fs, b)

    def sib_copy(src, c, k, kind):
        return remote(src, slot(c, k, kind), sent.at[1], w_recv.at[c, 0, int(c == chunks - 1 and kind == 2)], z, sib)

    every = [(c, kind) for c in range(chunks) for kind in range(3)]
    others = (zs, zn, zf)
    mine_q = rows_of(col)

    def tk_copy(i, src, dst, fs, tp):
        return remote(src, dst, sent.at[2], tk_recv.at[i], fs, tp)

    def tok_buf(e):
        return etok if e else ptok

    def cot_buf(e):
        return ecot if e else pcot

    def spread(i, e, q, tp):
        buf = cot_buf(e) if i in (1, 4, 5, 7) else tok_buf(e)
        ref = buf.at[rows_of(q)]
        return tk_copy(8 * e + (3 if i in (4, 6, 7) else i), ref, ref, z, tp)

    def spread_first(e):
        spread(0, e, col, bx).wait_recv()
        spread(2, e, col, bx).start()
        spread(3, e, col, by).start()
        spread(1, e, col, bx).wait_recv()
        spread(4, e, col, bx).start()
        spread(5, e, col, by).start()

    def spread_second(e):
        spread(2, e, col_x, bx).wait_recv()
        spread(6, e, col_x, by).start()
        spread(5, e, col_y, by).wait_recv()
        spread(7, e, col_y, bx).start()

    def spread_rest(e):
        drain(tally.at[pl.ds(0, 4 * shard)], tk_recv.at[8 * e + 3])

    far_rows = rows_of(2 * (1 - core), 2)
    give = tk_copy(16, pcot.at[far_rows], pcot.at[far_rows], z, sib)
    give_extra = tk_copy(17, ecot.at[far_rows], ecot.at[far_rows], z, sib)
    half_me = pl.ds(pl.multiple_of(me * half_rows, LANES), half_rows)
    @pl.when(end)
    def _():
        @pl.when(home)
        def _():
            tk_copy(8, tok_ref.at[mine_q], etok.at[mine_q], zn, sib).start()

        @pl.when(away)
        def _():
            tk_copy(9, cot_ref.at[mine_q], ecot.at[mine_q], zn, b).start()

    @pl.when(near)
    def _():
        @pl.when(home)
        def _():
            tk_copy(0, tok_ref.at[mine_q], ptok.at[mine_q], zn, b).start()

        @pl.when(away)
        def _():
            tk_copy(1, cot_ref.at[mine_q], pcot.at[mine_q], zn, sib).start()

    @pl.when(home)
    def _():
        for c, kind in every:
            w_copy(own(c, kind), c, z, kind, 0, zs).start()
            sib_copy(own(c, kind), c, z, kind).start()
            pltpu.make_async_copy(own(c, kind), slot(c, z, kind), local_sem.at[2]).start()

    @pl.when(away)
    def _():
        for c, kind in every:
            w_copy(own(c, kind), c, z, kind, jnp.where(near, 1, 2), zn).start()

    @pl.when(end)
    def _():
        tok[0, :half_rows] = tok_ref[:, half_me].T
        cot[0, :half_rows] = cot_ref[:, half_me].T

    @pl.when(jnp.logical_and(near, home))
    def _():
        tok[0] = tok_ref[...].T
        cot[0] = cot_ref[...].T
        spread_first(1)
        spread_second(1)

    @pl.when(jnp.logical_and(near, away))
    def _():
        spread_first(0)
        spread_second(0)
        spread_rest(0)
        give.start()
        tok[0] = ptok[...].T
        cot[0] = pcot[...].T

    def relay(c, kind):
        for i, k in enumerate(others):
            there = slot(c, k, kind)
            w_copy(there, c, k, kind, i, zs).wait_recv()
            if i:
                @pl.when(near)
                def _():
                    w_copy(there, c, k, kind, i, zs).start()
            sib_copy(there, c, k, kind).start()

    def relay_all(c):
        for kind in range(3):
            relay(c, kind)
        if c == 0:
            drain(weights.at[rows_of(z)], local_sem.at[2])

    def gather_sib(c):
        if c < chunks - 1:
            drain(weights.at[:, lanes_of(3 * c, 3)], w_recv.at[c, 0, 0])
        else:
            drain(weights.at[:, lanes_of(3 * c, 2)], w_recv.at[c, 0, 0])
            drain(weights.at[:, lanes_of(3 * c + 2)], w_recv.at[c, 0, 1])

    def gather(c):
        @pl.when(home)
        def _():
            relay_all(c)

        @pl.when(away)
        def _():
            gather_sib(c)

    def hid_copy(e, c, ref):
        return remote(ref, ref, sent.at[3], hid_recv.at[e, c], z, sib)

    def hid_ref(e, c):
        return hid.at[2 if e else me, :, lanes_of(c)]

    def hid_half(c):
        return hid.at[0, pl.ds(pl.multiple_of(me * half_rows, SUB), half_rows), lanes_of(c)]

    def gate_up(x, c):
        return jnp.dot(x, weights[:, 3 * c * LANES:(3 * c + 2) * LANES],
                       preferred_element_type=F32)

    def activate(x, y, c, out, e, pre=None):
        pre = gate_up(x, c) if pre is None else pre
        hg = jnp.dot(y, weights[:, (3 * c + 2) * LANES:(3 * c + 3) * LANES],
                     preferred_element_type=F32)
        gate_pre, up_pre = pre[:, :LANES], pre[:, LANES:]
        sig = jax.nn.sigmoid(gate_pre)
        act = gate_pre * sig
        out[...] = (act * up_pre).astype(BF16)
        hid_copy(e, c, out).start()
        return jnp.concatenate(
            [(hg * up_pre * sig * (1.0 + gate_pre * (1.0 - sig))).astype(BF16),
             (hg * act).astype(BF16)], axis=1)

    def begin(e, c):
        return activate(tok[e], cot[e], c, hid_ref(e, c), e)

    def finish(e, c, dgu):
        value = contract_cols(weights[:, 3 * c * LANES:(3 * c + 2) * LANES], dgu)
        if c == 0:
            dxacc[e] = value
        else:
            dxacc[e] += value

    def take_tokens():
        spread_rest(1)
        give_extra.start()
        tok[1] = etok[...].T
        cot[1] = ecot[...].T

    def work_half(c):
        dgu = activate(tok[0, :half_rows], cot[0, :half_rows], c, hid_half(c), 0)
        value = contract_cols(weights[:, 3 * c * LANES:(3 * c + 2) * LANES], dgu)
        if c == 0:
            dxacc[0, :, half_me] = value
        else:
            dxacc[0, :, half_me] += value

    halves = (slice(0, half_rows), slice(half_rows, rows))

    def t1_copy(e, i, step):
        return remote(t1s.at[e, i, step], t1r.at[e, i, step], sent.at[5], t1_recv.at[e, step],
                      z, bx if i == 0 else by)

    def t2_copy(e, i, q):
        return remote(t2s.at[e, i, q], t2r.at[e, i, q], sent.at[6], t2_recv.at[e, q],
                      z, by if i == 0 else bx)

    def t3_copy(q, fs):
        return remote(t3s.at[q], t3r.at[q], sent.at[7], t3_recv.at[q], fs, last)

    def strip(k, q):
        return pl.ds(pl.multiple_of(k * shard + q * piece, SUB), piece)

    def own_copy(q):
        return remote(dxacc.at[0, strip(col, q)], ownr.at[q], sent.at[10], own_recv.at[q], z, sib)

    def work_last(e, c):
        dgu = activate(tok[e], cot[e], c, hid_ref(e, c), e)
        for k, sends in ((col_d, ((0, 0), (1, 0))), (col_x, ((0, 1),)), (col_y, ((1, 1),)), (col, ())):
            r = rows_of(k)
            value = contract_cols(weights[r, 3 * c * LANES:(3 * c + 2) * LANES], dgu) + dxacc[e, r, :]
            if k is not col_d:
                dxacc[e, r, :] = value
            for i, step in sends:
                t1s[e, i, step] = value[:, halves[i]].astype(BF16)
                if e:
                    t1_copy(e, i, step).start()
                else:
                    @pl.when(away)
                    def _():
                        t1_copy(e, i, step).start()


    there = pl.ds(pl.multiple_of((1 - me) * half_rows, LANES), half_rows)

    def e_copy(i, q, tp):
        return remote(es.at[i, q], er.at[q, me, i], sent.at[5], e_recv.at[q], z, tp + 1 - core)

    def own_half():
        ref = dxacc.at[0, rows_of(col), half_me]
        return remote(ref, ref, sent.at[10], own_recv.at[0], z, sib)

    def take_half():
        ref = dxacc.at[0, rows_of(col), there]
        return remote(ref, ref, sent.at[10], own_recv.at[0], z, sib)

    def last_half(c):
        @pl.when(home)
        def _():
            relay(c, 0)
            relay(c, 1)

        @pl.when(away)
        def _():
            drain(weights.at[:, lanes_of(3 * c, 2)], w_recv.at[c, 0, 0])

        pre = gate_up(tok[0, :half_rows], c)

        @pl.when(home)
        def _():
            relay(c, 2)

        @pl.when(away)
        def _():
            drain(weights.at[:, lanes_of(3 * c + 2)], w_recv.at[c, 0, 1])
        dgu = activate(tok[0, :half_rows], cot[0, :half_rows], c, hid_half(c), 0, pre)
        columns = pl.ds(3 * c * LANES, 2 * LANES)
        for q in range(parts):
            for i, (k, tp) in enumerate(((col_d, bd), (col_x, bx), (col_y, by))):
                r = strip(k, q)
                es[i, q] = (contract_cols(weights[r, columns], dgu) + dxacc[0, r, half_me]).astype(BF16)
                e_copy(i, q, tp).start()
        r = rows_of(col)
        dxacc[0, r, half_me] += contract_cols(weights[r, columns], dgu)
        @pl.when(core == 0)
        def _():
            own_half().start()

    def end_result(q):
        drain(er.at[q], e_recv.at[q])
        r = strip(col, q)
        for i in range(2):
            total = dxacc[0, r, halves[i]] + t3r[q, :, halves[i]].astype(F32)
            for k in range(3):
                total = total + er[q, i, k].astype(F32)
            ybuf[r, halves[i]] = total.astype(BF16)

    def second_step(e):
        drain(t1r.at[e, :, 0], t1_recv.at[e, 0])
        for q in range(parts):
            inner = slice(q * piece, (q + 1) * piece)
            for i, k in ((0, col_y), (1, col_x)):
                t2s[e, i, q] = (dxacc[e, strip(k, q), halves[i]]
                                + t1r[e, i, 0, inner].astype(F32)).astype(BF16)
                t2_copy(e, i, q).start()

    def collect(e):
        drain(t1r.at[e, :, 1], t1_recv.at[e, 1])
        for q in range(parts):
            inner = slice(q * piece, (q + 1) * piece)
            for i in range(2):
                dxacc[e, strip(col, q), halves[i]] += t1r[e, i, 1, inner].astype(F32)

    def arrive(e, q):
        drain(t2r.at[e, :, q], t2_recv.at[e, q])
        for i in range(2):
            dxacc[e, strip(col, q), halves[i]] += t2r[e, i, q].astype(F32)

    def span(c):
        return slice(c * LANES, (c + 1) * LANES)

    def dg_home(g):
        lanes = lanes_of(g)
        return remote(dgs.at[0, :, lanes], dgr.at[0, :, lanes], sent.at[4], dg_recv.at[g], zs, b)

    def dg_away(g):
        lanes = lanes_of(g)
        return remote(dgs.at[:, :, lanes], dgr.at[:, :, lanes], sent.at[4], dg_recv.at[g], zs, b)

    def dg_far(g, i):
        lanes = lanes_of(g)
        return remote(dgs.at[i, :, lanes], dgf.at[:, lanes], sent.at[4], dgf_recv.at[g],
                      2 * (1 - side) + i, sib)

    def dg_direct(i):
        return remote(dgs.at[i, :, lanes_of(chunks - 1)], dge, sent.at[4], dge_recv.at[0],
                      2 * (1 - side) + i, sib)

    def keep_part(g, i, value):
        lanes = span(g)

        @pl.when(jnp.logical_and(home, zodd == i))
        def _():
            dgacc[:, lanes] = value

        @pl.when(jnp.logical_and(home, zodd != i))
        def _():
            dgs[0, :, lanes] = value.astype(BF16)

        if g == chunks - 1:
            @pl.when(away)
            def _():
                dgs[i, :, lanes] = value.astype(BF16)

                @pl.when(near)
                def _():
                    dg_far(g, i).start()

                @pl.when(end)
                def _():
                    dg_direct(i).start()
        else:
            @pl.when(jnp.logical_and(away, near))
            def _():
                dgp[i, :, lanes] = value

            @pl.when(jnp.logical_and(away, end))
            def _():
                dgs[i, :, lanes] = value.astype(BF16)

    def down_near(g):
        hid_copy(0, g, hid.at[1 - me, :, lanes_of(g)]).wait_recv()

        @pl.when(away)
        def _():
            hid_copy(1, g, hid.at[2, :, lanes_of(g)]).wait_recv()

        lanes = span(g)
        for i in range(2):
            k = rows_of(2 * core + i)
            keep_part(g, i, jnp.dot(cot_ref[k, :], hid[0, :, lanes], preferred_element_type=F32)
                      + jnp.dot(pcot[k, :], hid[1, :, lanes], preferred_element_type=F32)
                      + jnp.dot(ecot[k, :], hid[2, :, lanes], preferred_element_type=F32))

    def down_end(g):
        other = hid.at[0, pl.ds(pl.multiple_of((1 - me) * half_rows, SUB), half_rows), lanes_of(g)]
        hid_copy(0, g, other).wait_recv()
        for i in range(2):
            k = rows_of(2 * core + i)
            keep_part(g, i, jnp.dot(cot_ref[k, :], hid[0, :, span(g)], preferred_element_type=F32))

        @pl.when(home)
        def _():
            dg_home(g).start()

        if g < chunks - 1:
            @pl.when(away)
            def _():
                dg_away(g).start()

    def down_mid(g):
        lanes = span(g)
        dg_away(g).wait_recv()
        for i in range(2):
            dgs[i, :, lanes] = (dgp[i, :, lanes] + dgr[i, :, lanes].astype(F32)).astype(BF16)
            dg_far(g, i).start()
    @pl.when(near)
    def _():

        @pl.when(home)
        def _():
            relay_all(0)
            for c in range(chunks - 1):
                dgu = begin(0, c)
                relay(c + 1, 0)
                finish(0, c, dgu)
                if c == 0:
                    take_tokens()
                relay(c + 1, 1)
                finish(1, c, begin(1, c))
                relay(c + 1, 2)

        @pl.when(away)
        def _():
            for c in range(chunks - 1):
                gather_sib(c)
                finish(0, c, begin(0, c))
            gather_sib(chunks - 1)

        @pl.when(home)
        def _():
            work_last(1, chunks - 1)
        work_last(0, chunks - 1)

        @pl.when(home)
        def _():
            second_step(1)
            for step in range(2):
                for i in range(2):
                    t1_copy(0, i, step).start()
            collect(1)

        @pl.when(home)
        def _():
            give.wait_recv()

        @pl.when(away)
        def _():
            give_extra.wait_recv()

        @pl.when(away)
        def _():
            for c in range(chunks):
                down_near(c)
                if c == 0 and chunks > 2:
                    down_mid(0)
            second_step(0)

        @pl.when(home)
        def _():
            down_near(0)
            dg_home(0).start()
            for q in range(parts):
                arrive(1, q)
                t3s[q] = dxacc[1, strip(col, q), :].astype(BF16)
                t3_copy(q, zf).start()
            second_step(0)
            for c in range(1, chunks):
                down_near(c)
                dg_home(c).start()

        collect(0)
        for q in range(parts):
            arrive(0, q)

            @pl.when(away)
            def _():
                t3s[q] = dxacc[0, strip(col, q), :].astype(BF16)
                t3_copy(q, zn).start()

            @pl.when(jnp.logical_and(home, core == 0))
            def _():
                own_copy(q).start()

        @pl.when(away)
        def _():
            for c in range(0 if chunks == 2 else 1, chunks - 1):
                down_mid(c)

    @pl.when(end)
    def _():
        for c in range(chunks - 1):
            gather(c)
            work_half(c)
            down_end(c)
        last_half(chunks - 1)
        down_end(chunks - 1)

        @pl.when(lead)
        def _():
            take_half().wait_recv()

    def y_copy(i, k, q, tp):
        ref = ybuf.at[strip(k, q)]
        return remote(ref, ref, sent.at[8], y_recv.at[q], z, tp)

    def y_sib(i, k, q):
        ref = ybuf.at[strip(k, q)]
        return remote(ref, ref, sent.at[9], y_recv.at[q], z, sib)

    def result(q, value):
        ybuf[strip(col, q), :] = value.astype(BF16)

    def down_final():
        @pl.when(home)
        def _():
            for g in range(chunks):
                dg_home(g).wait_recv()
            dgacc[...] += dgr[0].astype(F32)

        @pl.when(away)
        def _():
            for g in range(chunks):
                dg_far(g, 0).wait_recv()
            dg_direct(0).wait_recv()
            dgacc[...] = dgf[...].astype(F32)
            dgacc[:, span(chunks - 1)] += dge[...].astype(F32)
    @pl.when(lead)
    def _():
        for q in range(parts):
            t3_copy(q, zn).wait_recv()

            @pl.when(end)
            def _():
                end_result(q)

            @pl.when(jnp.logical_and(near, home))
            def _():
                result(q, dxacc[0, strip(col, q), :] + t3r[q].astype(F32))

            @pl.when(jnp.logical_and(near, away))
            def _():
                own_copy(q).wait_recv()
                result(q, ownr[q] + t3r[q].astype(F32))
            y_copy(2, col, q, bd).start()
            y_copy(0, col, q, bx).start()
            y_copy(1, col, q, by).start()
            y_sib(0, col, q).start()
        down_final()
        for q in range(parts):
            drain(tally.at[pl.ds(0, 3 * piece)], y_recv.at[q])
            for i, k in enumerate((col_x, col_y, col_d)):
                y_sib(i + 1, k, q).start()
    @pl.when(core == 0)
    def _():
        down_final()
        for q in range(parts):
            drain(tally.at[pl.ds(0, 4 * piece)], y_recv.at[q])
    @pl.when(lead)
    def _():
        drain(ybuf.at[pl.ds(0, 3 * shard)], sent.at[8])
        drain(ybuf, sent.at[9])

    @pl.when(home)
    def _():
        drain(weights, sent.at[1])
        drain(dgs.at[0], sent.at[4])

    @pl.when(away)
    def _():
        drain(weights.at[pl.ds(0, shard)], sent.at[0])
        drain(dgs, sent.at[4])

    @pl.when(end)
    def _():
        drain(tally.at[pl.ds(0, shard)], sent.at[2])
        drain(hid.at[0, pl.ds(0, half_rows)], sent.at[3])
        drain(es, sent.at[5])

        @pl.when(home)
        def _():
            drain(weights.at[pl.ds(0, shard)], sent.at[0])

        @pl.when(core == 0)
        def _():
            drain(dxacc.at[0, pl.ds(0, shard), pl.ds(0, half_rows)], sent.at[10])

    @pl.when(near)
    def _():
        drain(tally, sent.at[2])
        drain(t3s, sent.at[7])

        @pl.when(home)
        def _():
            drain(weights.at[pl.ds(0, 3 * shard)], sent.at[0])
            drain(hid.at[pl.ds(0, 2)], sent.at[3])
            drain(t1s, sent.at[5])
            drain(t2s, sent.at[6])

            @pl.when(core == 0)
            def _():
                drain(ownr, sent.at[10])

        @pl.when(away)
        def _():
            drain(hid.at[0], sent.at[3])
            drain(t1s.at[0], sent.at[5])
            drain(t2s.at[0], sent.at[6])


def store_kernel(dx_in, dg_in, dx_out, dg_out, sem):
    copies = [pltpu.make_async_copy(src, dst, sem.at[i])
              for i, (src, dst) in enumerate(((dx_in, dx_out), (dg_in, dg_out)))]
    for copy in copies:
        copy.start()
    for copy in copies:
        copy.wait()


def per_device_kernel(n, tokens, cotangent, gate_weight, up_weight, down_weight):
    rows, depth = tokens.shape
    shard, ff = gate_weight.shape
    chunks = ff // LANES
    parts = next(p for p in (3, 2, 1) if shard % (p * SUB) == 0)
    piece = shard // parts
    vmem, dma = pltpu.VMEM, pltpu.SemaphoreType.DMA
    dx, dg = pl.pallas_call(
        functools.partial(kernel, n),
        out_shape=(vmem((depth, rows), BF16), vmem((shard, ff), F32)),
        in_specs=[pl.BlockSpec(memory_space=pltpu.HBM)] * 5,
        out_specs=[pl.BlockSpec(memory_space=vmem)] * 2,
        scratch_shapes=[
            vmem((depth, rows), BF16), vmem((depth, rows), BF16),
            vmem((shard, ff), BF16), vmem((shard, ff), BF16), vmem((shard, ff), BF16),
            vmem((depth, 3 * ff), BF16),
            vmem((2, rows, depth), BF16), vmem((2, rows, depth), BF16),
            vmem((depth, rows), BF16), vmem((depth, rows), BF16),
            vmem((depth, rows), BF16), vmem((depth, rows), BF16),
            vmem((2, depth, rows), F32),
            vmem((3, rows, ff), BF16),
            vmem((2, shard, ff), F32), vmem((2, shard, ff), BF16),
            vmem((2, shard, ff), BF16), vmem((shard, ff), BF16), vmem((shard, LANES), BF16),
            vmem((2, 2, 2, shard, rows // 2), BF16), vmem((2, 2, 2, shard, rows // 2), BF16),
            vmem((2, 2, parts, piece, rows // 2), BF16), vmem((2, 2, parts, piece, rows // 2), BF16),
            vmem((parts, piece, rows), BF16), vmem((parts, piece, rows), BF16),
            vmem((3, parts, piece, rows // 2), BF16), vmem((parts, 2, 3, piece, rows // 2), BF16),
            vmem((parts, piece, rows), F32),
            vmem((9 * shard, rows), BF16),
            dma((11,)), dma((chunks, 3, 3)), dma((18,)), dma((2, chunks)), dma((chunks,)), dma((chunks,)), dma((1,)),
            dma((2, 2)), dma((2, parts)), dma((parts,)), dma((parts,)), dma((parts,)),
            dma((parts,)), dma((3,)),
        ],
        compiler_params=pltpu.CompilerParams(
            collective_id=0, has_side_effects=True, vmem_limit_bytes=40 * 2**20),
    )(*(pltpu.with_memory_space_constraint(a, pltpu.HBM) for a in (
        tokens.T, cotangent.T, gate_weight, up_weight, down_weight.T)))
    dx, dg = pl.pallas_call(
        store_kernel,
        out_shape=(pltpu.HBM((depth, rows), BF16), pltpu.HBM((shard, ff), F32)),
        in_specs=[pl.BlockSpec(memory_space=pl.ANY)] * 2,
        out_specs=[pl.BlockSpec(memory_space=pl.ANY)] * 2,
        scratch_shapes=[dma((2,))],
        compiler_params=pltpu.CompilerParams(vmem_limit_bytes=2**20),
    )(dx, dg)
    return dx.T, dg.T


def solution(mesh):
    n, tp = mesh.shape["fs"], mesh.shape["tp"]

    def per_device(tokens, cotangent, gate_weight, up_weight, down_weight):
        rows, depth = tokens.shape
        shard, ff = gate_weight.shape
        args = (tokens, cotangent, gate_weight, up_weight, down_weight)
        fits = (tp == 8 and n == 4 and rows % (2 * LANES) == 0 and rows <= 256
                and depth == n * shard and shard % SUB == 0 and ff % LANES == 0
                and LANES < ff <= 512 and depth <= 2048)
        return per_device_kernel(n, *args) if fits else per_device_plain(*args)

    placed = (P("fs", None), P("fs", None), P("fs", "tp"), P("fs", "tp"), P("tp", "fs"))
    return jax.shard_map(
        per_device,
        mesh=mesh,
        in_specs=placed,
        out_specs=(P("fs", None), P("tp", "fs")),
        check_vma=False,
    )
```

```python
import functools

import jax
import jax.numpy as jnp
from jax import lax
from jax.experimental import pallas as pl
from jax.experimental.pallas import tpu as pltpu
from jax.sharding import PartitionSpec as P

LANES = 128
SUB = 16
BF16 = jnp.bfloat16
F32 = jnp.float32


def contract_rows(left, right):
    return lax.dot_general(
        left, right, (((0,), (0,)), ((), ())), preferred_element_type=jnp.float32
    )


def contract_cols(left, right):
    return lax.dot_general(
        left, right, (((1,), (1,)), ((), ())), preferred_element_type=jnp.float32
    )


def send_down(hidden, cotangent):
    return lax.psum_scatter(
        contract_rows(cotangent, hidden), "fs", scatter_dimension=0, tiled=True
    ).T


def per_device_plain(tokens, cotangent, gate_weight, up_weight, down_weight):
    whole_gate, whole_up, whole_down = (
        lax.all_gather(gate_weight, "fs", axis=0, tiled=True),
        lax.all_gather(up_weight, "fs", axis=0, tiled=True),
        lax.all_gather(down_weight, "fs", axis=1, tiled=True),
    )
    gate_pre = jnp.dot(tokens, whole_gate, preferred_element_type=jnp.float32)
    up_pre = jnp.dot(tokens, whole_up, preferred_element_type=jnp.float32)
    hidden_grad = contract_cols(cotangent, whole_down)
    sigmoid_gate = jax.nn.sigmoid(gate_pre)
    activated = gate_pre * sigmoid_gate
    hidden = (activated * up_pre).astype(jnp.bfloat16)
    gate_pre_grad = (
        hidden_grad * up_pre * sigmoid_gate * (1.0 + gate_pre * (1.0 - sigmoid_gate))
    ).astype(jnp.bfloat16)
    up_pre_grad = (hidden_grad * activated).astype(jnp.bfloat16)
    partial_value = contract_cols(gate_pre_grad, whole_gate) + contract_cols(up_pre_grad, whole_up)
    input_grad = lax.psum(partial_value.astype(jnp.bfloat16), "tp")
    down_grad = send_down(hidden, cotangent)
    return (input_grad, down_grad)


def kernel(n, tok_hbm, cot_hbm, gate_hbm, up_hbm, down_hbm, ybuf, dgacc,
           tok_ref, cot_ref, gate_ref, up_ref, down_ref, weights, tok, cot,
           ptok, pcot, etok, ecot, dxacc, hid, dgp, dgs, dgr, dgf, dge,
           t1s, t1r, t2s, t2r, t3s, t3r, es, er, ownr, tally,
           sent, w_recv, tk_recv, hid_recv, dg_recv, dgf_recv, dge_recv, t1_recv, t2_recv,
           t3_recv, e_recv, own_recv, y_recv, local_sem):
    z = lax.axis_index("fs")
    b = lax.axis_index("tp")
    depth, rows = tok_ref.shape
    shard, ff = gate_ref.shape
    chunks = ff // LANES
    parts, piece = t2s.shape[2], t2s.shape[3]
    half_rows = rows // 2
    core = lax.rem(b, 2)
    col = lax.div(b, 2)
    cx = lax.rem(col, 2)
    cy = lax.div(col, 2)
    side = lax.div(z, 2)
    zodd = lax.rem(z, 2)
    home = core == side
    away = core != side
    near = side != zodd
    end = side == zodd
    lead = core == 1
    sib = b + 1 - 2 * core
    bx = b + 2 * (1 - 2 * cx)
    by = b + 4 * (1 - 2 * cy)
    bd = bx + by - b
    last = 2 * col + 1
    zs = z + 1 - 2 * zodd
    zn = 2 - side
    zf = 3 - 3 * side
    me = jnp.where(home, 0, 1)
    col_x = 2 * cy + 1 - cx
    col_y = 2 * (1 - cy) + cx
    col_d = 2 * (1 - cy) + 1 - cx
    for src, dst, i in ((tok_hbm, tok_ref, 0), (cot_hbm, cot_ref, 0), (gate_hbm, gate_ref, 1),
                        (up_hbm, up_ref, 1), (down_hbm, down_ref, 1)):
        pltpu.make_async_copy(src, dst, local_sem.at[i]).start()

    def drain(ref, sem):
        pltpu.make_async_copy(ref, ref, sem).wait()

    barrier = pltpu.get_barrier_semaphore()

    def greet(fs, tp):
        pl.semaphore_signal(barrier, inc=1, device_id={"fs": fs, "tp": tp},
                            device_id_type=pl.DeviceIdType.MESH)

    greet(z, sib)
    greet(z, bx)
    greet(z, by)
    greet(z, bd)
    for step in range(1, n):
        greet(lax.rem(z + step, n), b)
        greet(lax.rem(z + step, n), sib)
    pl.semaphore_wait(barrier, 4 + 2 * (n - 1))
    drain(tally.at[pl.ds(0, 2 * depth)], local_sem.at[0])
    drain(weights.at[pl.ds(0, shard)], local_sem.at[1])

    def remote(src, dst, send, recv, fs, tp):
        return pltpu.make_async_remote_copy(
            src_ref=src, dst_ref=dst, send_sem=send, recv_sem=recv,
            device_id={"fs": fs, "tp": tp}, device_id_type=pl.DeviceIdType.MESH)

    def rows_of(k, count=1):
        return pl.ds(pl.multiple_of(k * shard, SUB), count * shard)

    def lanes_of(c, count=1):
        return pl.ds(c * LANES, count * LANES)

    def slot(c, k, kind):
        return weights.at[rows_of(k), lanes_of(3 * c + kind)]

    def own(c, kind):
        return (gate_ref, up_ref, down_ref)[kind].at[:, lanes_of(c)]

    def w_copy(src, c, k, kind, i, fs):
        return remote(src, slot(c, k, kind), sent.at[0], w_recv.at[c, i, kind], fs, b)

    def sib_copy(src, c, k, kind):
        return remote(src, slot(c, k, kind), sent.at[1], w_recv.at[c, 0, int(c == chunks - 1 and kind == 2)], z, sib)

    every = [(c, kind) for c in range(chunks) for kind in range(3)]
    others = (zs, zn, zf)
    mine_q = rows_of(col)

    def tk_copy(i, src, dst, fs, tp):
        return remote(src, dst, sent.at[2], tk_recv.at[i], fs, tp)

    def tok_buf(e):
        return etok if e else ptok

    def cot_buf(e):
        return ecot if e else pcot

    def spread(i, e, q, tp):
        buf = cot_buf(e) if i in (1, 4, 5, 7) else tok_buf(e)
        ref = buf.at[rows_of(q)]
        return tk_copy(8 * e + (3 if i in (4, 6, 7) else i), ref, ref, z, tp)

    def spread_first(e):
        spread(0, e, col, bx).wait_recv()
        spread(2, e, col, bx).start()
        spread(3, e, col, by).start()
        spread(1, e, col, bx).wait_recv()
        spread(4, e, col, bx).start()
        spread(5, e, col, by).start()

    def spread_second(e):
        spread(2, e, col_x, bx).wait_recv()
        spread(6, e, col_x, by).start()
        spread(5, e, col_y, by).wait_recv()
        spread(7, e, col_y, bx).start()

    def spread_rest(e):
        drain(tally.at[pl.ds(0, 4 * shard)], tk_recv.at[8 * e + 3])

    far_rows = rows_of(2 * (1 - core), 2)
    give = tk_copy(16, pcot.at[far_rows], pcot.at[far_rows], z, sib)
    give_extra = tk_copy(17, ecot.at[far_rows], ecot.at[far_rows], z, sib)
    half_me = pl.ds(pl.multiple_of(me * half_rows, LANES), half_rows)
    @pl.when(end)
    def _():
        @pl.when(home)
        def _():
            tk_copy(8, tok_ref.at[mine_q], etok.at[mine_q], zn, sib).start()

        @pl.when(away)
        def _():
            tk_copy(9, cot_ref.at[mine_q], ecot.at[mine_q], zn, b).start()

    @pl.when(near)
    def _():
        @pl.when(home)
        def _():
            tk_copy(0, tok_ref.at[mine_q], ptok.at[mine_q], zn, b).start()

        @pl.when(away)
        def _():
            tk_copy(1, cot_ref.at[mine_q], pcot.at[mine_q], zn, sib).start()

    @pl.when(home)
    def _():
        for c, kind in every:
            w_copy(own(c, kind), c, z, kind, 0, zs).start()
            sib_copy(own(c, kind), c, z, kind).start()
            pltpu.make_async_copy(own(c, kind), slot(c, z, kind), local_sem.at[2]).start()

    @pl.when(away)
    def _():
        for c, kind in every:
            w_copy(own(c, kind), c, z, kind, jnp.where(near, 1, 2), zn).start()

    @pl.when(end)
    def _():
        tok[0, :half_rows] = tok_ref[:, half_me].T
        cot[0, :half_rows] = cot_ref[:, half_me].T

    @pl.when(jnp.logical_and(near, home))
    def _():
        tok[0] = tok_ref[...].T
        cot[0] = cot_ref[...].T
        spread_first(1)
        spread_second(1)

    @pl.when(jnp.logical_and(near, away))
    def _():
        spread_first(0)
        spread_second(0)
        spread_rest(0)
        give.start()
        tok[0] = ptok[...].T
        cot[0] = pcot[...].T

    def relay(c, kind):
        for i, k in enumerate(others):
            there = slot(c, k, kind)
            w_copy(there, c, k, kind, i, zs).wait_recv()
            if i:
                @pl.when(near)
                def _():
                    w_copy(there, c, k, kind, i, zs).start()
            sib_copy(there, c, k, kind).start()

    def relay_all(c):
        for kind in range(3):
            relay(c, kind)
        if c == 0:
            drain(weights.at[rows_of(z)], local_sem.at[2])

    def gather_sib(c):
        if c < chunks - 1:
            drain(weights.at[:, lanes_of(3 * c, 3)], w_recv.at[c, 0, 0])
        else:
            drain(weights.at[:, lanes_of(3 * c, 2)], w_recv.at[c, 0, 0])
            drain(weights.at[:, lanes_of(3 * c + 2)], w_recv.at[c, 0, 1])

    def gather(c):
        @pl.when(home)
        def _():
            relay_all(c)

        @pl.when(away)
        def _():
            gather_sib(c)

    def hid_copy(e, c, ref):
        return remote(ref, ref, sent.at[3], hid_recv.at[e, c], z, sib)

    def hid_ref(e, c):
        return hid.at[2 if e else me, :, lanes_of(c)]

    def hid_half(c):
        return hid.at[0, pl.ds(pl.multiple_of(me * half_rows, SUB), half_rows), lanes_of(c)]

    def gate_up(x, c):
        return jnp.dot(x, weights[:, 3 * c * LANES:(3 * c + 2) * LANES],
                       preferred_element_type=F32)

    def activate(x, y, c, out, e, pre=None):
        pre = gate_up(x, c) if pre is None else pre
        hg = jnp.dot(y, weights[:, (3 * c + 2) * LANES:(3 * c + 3) * LANES],
                     preferred_element_type=F32)
        gate_pre, up_pre = pre[:, :LANES], pre[:, LANES:]
        sig = jax.nn.sigmoid(gate_pre)
        act = gate_pre * sig
        out[...] = (act * up_pre).astype(BF16)
        hid_copy(e, c, out).start()
        return jnp.concatenate(
            [(hg * up_pre * sig * (1.0 + gate_pre * (1.0 - sig))).astype(BF16),
             (hg * act).astype(BF16)], axis=1)

    def begin(e, c):
        return activate(tok[e], cot[e], c, hid_ref(e, c), e)

    def finish(e, c, dgu):
        value = contract_cols(weights[:, 3 * c * LANES:(3 * c + 2) * LANES], dgu)
        if c == 0:
            dxacc[e] = value
        else:
            dxacc[e] += value

    def take_tokens():
        spread_rest(1)
        give_extra.start()
        tok[1] = etok[...].T
        cot[1] = ecot[...].T

    def work_half(c):
        dgu = activate(tok[0, :half_rows], cot[0, :half_rows], c, hid_half(c), 0)
        value = contract_cols(weights[:, 3 * c * LANES:(3 * c + 2) * LANES], dgu)
        if c == 0:
            dxacc[0, :, half_me] = value
        else:
            dxacc[0, :, half_me] += value

    halves = (slice(0, half_rows), slice(half_rows, rows))

    def t1_copy(e, i, step):
        return remote(t1s.at[e, i, step], t1r.at[e, i, step], sent.at[5], t1_recv.at[e, step],
                      z, bx if i == 0 else by)

    def t2_copy(e, i, q):
        return remote(t2s.at[e, i, q], t2r.at[e, i, q], sent.at[6], t2_recv.at[e, q],
                      z, by if i == 0 else bx)

    def t3_copy(q, fs):
        return remote(t3s.at[q], t3r.at[q], sent.at[7], t3_recv.at[q], fs, last)

    def strip(k, q):
        return pl.ds(pl.multiple_of(k * shard + q * piece, SUB), piece)

    def own_copy(q):
        return remote(dxacc.at[0, strip(col, q)], ownr.at[q], sent.at[10], own_recv.at[q], z, sib)

    def work_last(e, c):
        dgu = activate(tok[e], cot[e], c, hid_ref(e, c), e)
        for k, sends in ((col_d, ((0, 0), (1, 0))), (col_x, ((0, 1),)), (col_y, ((1, 1),)), (col, ())):
            r = rows_of(k)
            value = contract_cols(weights[r, 3 * c * LANES:(3 * c + 2) * LANES], dgu) + dxacc[e, r, :]
            if k is not col_d:
                dxacc[e, r, :] = value
            for i, step in sends:
                t1s[e, i, step] = value[:, halves[i]].astype(BF16)
                if e:
                    t1_copy(e, i, step).start()
                else:
                    @pl.when(away)
                    def _():
                        t1_copy(e, i, step).start()


    there = pl.ds(pl.multiple_of((1 - me) * half_rows, LANES), half_rows)

    def e_copy(i, q, tp):
        return remote(es.at[i, q], er.at[q, me, i], sent.at[5], e_recv.at[q], z, tp + 1 - core)

    def own_half():
        ref = dxacc.at[0, rows_of(col), half_me]
        return remote(ref, ref, sent.at[10], own_recv.at[0], z, sib)

    def take_half():
        ref = dxacc.at[0, rows_of(col), there]
        return remote(ref, ref, sent.at[10], own_recv.at[0], z, sib)

    def last_half(c):
        @pl.when(home)
        def _():
            relay(c, 0)
            relay(c, 1)

        @pl.when(away)
        def _():
            drain(weights.at[:, lanes_of(3 * c, 2)], w_recv.at[c, 0, 0])

        pre = gate_up(tok[0, :half_rows], c)

        @pl.when(home)
        def _():
            relay(c, 2)

        @pl.when(away)
        def _():
            drain(weights.at[:, lanes_of(3 * c + 2)], w_recv.at[c, 0, 1])
        dgu = activate(tok[0, :half_rows], cot[0, :half_rows], c, hid_half(c), 0, pre)
        columns = pl.ds(3 * c * LANES, 2 * LANES)
        for q in range(parts):
            for i, (k, tp) in enumerate(((col_d, bd), (col_x, bx), (col_y, by))):
                r = strip(k, q)
                es[i, q] = (contract_cols(weights[r, columns], dgu) + dxacc[0, r, half_me]).astype(BF16)
                e_copy(i, q, tp).start()
        r = rows_of(col)
        dxacc[0, r, half_me] += contract_cols(weights[r, columns], dgu)
        @pl.when(core == 0)
        def _():
            own_half().start()

    def end_result(q):
        drain(er.at[q], e_recv.at[q])
        r = strip(col, q)
        for i in range(2):
            total = dxacc[0, r, halves[i]] + t3r[q, :, halves[i]].astype(F32)
            for k in range(3):
                total = total + er[q, i, k].astype(F32)
            ybuf[r, halves[i]] = total.astype(BF16)

    def second_step(e):
        drain(t1r.at[e, :, 0], t1_recv.at[e, 0])
        for q in range(parts):
            inner = slice(q * piece, (q + 1) * piece)
            for i, k in ((0, col_y), (1, col_x)):
                t2s[e, i, q] = (dxacc[e, strip(k, q), halves[i]]
                                + t1r[e, i, 0, inner].astype(F32)).astype(BF16)
                t2_copy(e, i, q).start()

    def collect(e):
        drain(t1r.at[e, :, 1], t1_recv.at[e, 1])
        for q in range(parts):
            inner = slice(q * piece, (q + 1) * piece)
            for i in range(2):
                dxacc[e, strip(col, q), halves[i]] += t1r[e, i, 1, inner].astype(F32)

    def arrive(e, q):
        drain(t2r.at[e, :, q], t2_recv.at[e, q])
        for i in range(2):
            dxacc[e, strip(col, q), halves[i]] += t2r[e, i, q].astype(F32)

    def span(c):
        return slice(c * LANES, (c + 1) * LANES)

    def dg_home(g):
        lanes = lanes_of(g)
        return remote(dgs.at[0, :, lanes], dgr.at[0, :, lanes], sent.at[4], dg_recv.at[g], zs, b)

    def dg_away(g):
        lanes = lanes_of(g)
        return remote(dgs.at[:, :, lanes], dgr.at[:, :, lanes], sent.at[4], dg_recv.at[g], zs, b)

    def dg_far(g, i):
        lanes = lanes_of(g)
        return remote(dgs.at[i, :, lanes], dgf.at[:, lanes], sent.at[4], dgf_recv.at[g],
                      2 * (1 - side) + i, sib)

    def dg_direct(i):
        return remote(dgs.at[i, :, lanes_of(chunks - 1)], dge, sent.at[4], dge_recv.at[0],
                      2 * (1 - side) + i, sib)

    def keep_part(g, i, value):
        lanes = span(g)

        @pl.when(jnp.logical_and(home, zodd == i))
        def _():
            dgacc[:, lanes] = value

        @pl.when(jnp.logical_and(home, zodd != i))
        def _():
            dgs[0, :, lanes] = value.astype(BF16)

        if g == chunks - 1:
            @pl.when(away)
            def _():
                dgs[i, :, lanes] = value.astype(BF16)

                @pl.when(near)
                def _():
                    dg_far(g, i).start()

                @pl.when(end)
                def _():
                    dg_direct(i).start()
        else:
            @pl.when(jnp.logical_and(away, near))
            def _():
                dgp[i, :, lanes] = value

            @pl.when(jnp.logical_and(away, end))
            def _():
                dgs[i, :, lanes] = value.astype(BF16)

    def down_near(g):
        hid_copy(0, g, hid.at[1 - me, :, lanes_of(g)]).wait_recv()

        @pl.when(away)
        def _():
            hid_copy(1, g, hid.at[2, :, lanes_of(g)]).wait_recv()

        lanes = span(g)
        for i in range(2):
            k = rows_of(2 * core + i)
            keep_part(g, i, jnp.dot(cot_ref[k, :], hid[0, :, lanes], preferred_element_type=F32)
                      + jnp.dot(pcot[k, :], hid[1, :, lanes], preferred_element_type=F32)
                      + jnp.dot(ecot[k, :], hid[2, :, lanes], preferred_element_type=F32))

    def down_end(g):
        other = hid.at[0, pl.ds(pl.multiple_of((1 - me) * half_rows, SUB), half_rows), lanes_of(g)]
        hid_copy(0, g, other).wait_recv()
        for i in range(2):
            k = rows_of(2 * core + i)
            keep_part(g, i, jnp.dot(cot_ref[k, :], hid[0, :, span(g)], preferred_element_type=F32))

        @pl.when(home)
        def _():
            dg_home(g).start()

        if g < chunks - 1:
            @pl.when(away)
            def _():
                dg_away(g).start()

    def down_mid(g):
        lanes = span(g)
        dg_away(g).wait_recv()
        for i in range(2):
            dgs[i, :, lanes] = (dgp[i, :, lanes] + dgr[i, :, lanes].astype(F32)).astype(BF16)
            dg_far(g, i).start()
    @pl.when(near)
    def _():

        @pl.when(home)
        def _():
            relay_all(0)
            for c in range(chunks - 1):
                dgu = begin(0, c)
                relay(c + 1, 0)
                finish(0, c, dgu)
                if c == 0:
                    take_tokens()
                relay(c + 1, 1)
                finish(1, c, begin(1, c))
                relay(c + 1, 2)

        @pl.when(away)
        def _():
            for c in range(chunks - 1):
                gather_sib(c)
                finish(0, c, begin(0, c))
            gather_sib(chunks - 1)

        @pl.when(home)
        def _():
            work_last(1, chunks - 1)
        work_last(0, chunks - 1)

        @pl.when(home)
        def _():
            second_step(1)
            for step in range(2):
                for i in range(2):
                    t1_copy(0, i, step).start()
            collect(1)

        @pl.when(home)
        def _():
            give.wait_recv()

        @pl.when(away)
        def _():
            give_extra.wait_recv()

        @pl.when(away)
        def _():
            for c in range(chunks):
                down_near(c)
                if c == 0 and chunks > 2:
                    down_mid(0)
            second_step(0)

        @pl.when(home)
        def _():
            down_near(0)
            dg_home(0).start()
            for q in range(parts):
                arrive(1, q)
                t3s[q] = dxacc[1, strip(col, q), :].astype(BF16)
                t3_copy(q, zf).start()
            second_step(0)
            for c in range(1, chunks):
                down_near(c)
                dg_home(c).start()

        collect(0)
        for q in range(parts):
            arrive(0, q)

            @pl.when(away)
            def _():
                t3s[q] = dxacc[0, strip(col, q), :].astype(BF16)
                t3_copy(q, zn).start()

            @pl.when(jnp.logical_and(home, core == 0))
            def _():
                own_copy(q).start()

        @pl.when(away)
        def _():
            for c in range(0 if chunks == 2 else 1, chunks - 1):
                down_mid(c)

    @pl.when(end)
    def _():
        for c in range(chunks - 1):
            gather(c)
            work_half(c)
            down_end(c)
        last_half(chunks - 1)
        down_end(chunks - 1)

        @pl.when(lead)
        def _():
            take_half().wait_recv()

    def y_copy(i, k, q, tp):
        ref = ybuf.at[strip(k, q)]
        return remote(ref, ref, sent.at[8], y_recv.at[q], z, tp)

    def y_sib(i, k, q):
        ref = ybuf.at[strip(k, q)]
        return remote(ref, ref, sent.at[9], y_recv.at[q], z, sib)

    def result(q, value):
        ybuf[strip(col, q), :] = value.astype(BF16)

    def down_final():
        @pl.when(home)
        def _():
            for g in range(chunks):
                dg_home(g).wait_recv()
            dgacc[...] += dgr[0].astype(F32)

        @pl.when(away)
        def _():
            for g in range(chunks):
                dg_far(g, 0).wait_recv()
            dg_direct(0).wait_recv()
            dgacc[...] = dgf[...].astype(F32)
            dgacc[:, span(chunks - 1)] += dge[...].astype(F32)
    @pl.when(lead)
    def _():
        for q in range(parts):
            t3_copy(q, zn).wait_recv()

            @pl.when(end)
            def _():
                end_result(q)

            @pl.when(jnp.logical_and(near, home))
            def _():
                result(q, dxacc[0, strip(col, q), :] + t3r[q].astype(F32))

            @pl.when(jnp.logical_and(near, away))
            def _():
                own_copy(q).wait_recv()
                result(q, ownr[q] + t3r[q].astype(F32))
            y_copy(2, col, q, bd).start()
            y_copy(0, col, q, bx).start()
            y_copy(1, col, q, by).start()
            y_sib(0, col, q).start()
        down_final()
        for q in range(parts):
            drain(tally.at[pl.ds(0, 3 * piece)], y_recv.at[q])
            for i, k in enumerate((col_x, col_y, col_d)):
                y_sib(i + 1, k, q).start()
    @pl.when(core == 0)
    def _():
        down_final()
        for q in range(parts):
            drain(tally.at[pl.ds(0, 4 * piece)], y_recv.at[q])
    @pl.when(lead)
    def _():
        drain(ybuf.at[pl.ds(0, 3 * shard)], sent.at[8])
        drain(ybuf, sent.at[9])

    @pl.when(home)
    def _():
        drain(weights, sent.at[1])
        drain(dgs.at[0], sent.at[4])

    @pl.when(away)
    def _():
        drain(weights.at[pl.ds(0, shard)], sent.at[0])
        drain(dgs, sent.at[4])

    @pl.when(end)
    def _():
        drain(tally.at[pl.ds(0, shard)], sent.at[2])
        drain(hid.at[0, pl.ds(0, half_rows)], sent.at[3])
        drain(es, sent.at[5])

        @pl.when(home)
        def _():
            drain(weights.at[pl.ds(0, shard)], sent.at[0])

        @pl.when(core == 0)
        def _():
            drain(dxacc.at[0, pl.ds(0, shard), pl.ds(0, half_rows)], sent.at[10])

    @pl.when(near)
    def _():
        drain(tally, sent.at[2])
        drain(t3s, sent.at[7])

        @pl.when(home)
        def _():
            drain(weights.at[pl.ds(0, 3 * shard)], sent.at[0])
            drain(hid.at[pl.ds(0, 2)], sent.at[3])
            drain(t1s, sent.at[5])
            drain(t2s, sent.at[6])

            @pl.when(core == 0)
            def _():
                drain(ownr, sent.at[10])

        @pl.when(away)
        def _():
            drain(hid.at[0], sent.at[3])
            drain(t1s.at[0], sent.at[5])
            drain(t2s.at[0], sent.at[6])


def store_kernel(dx_in, dg_in, dx_out, dg_out, sem):
    copies = []
    for src, dst in ((dx_in, dx_out), (dg_in, dg_out)):
        step = src.shape[0] // 3
        for lo in range(0, 3 * step, step):
            r = pl.ds(lo, step)
            copies.append(pltpu.make_async_copy(src.at[r], dst.at[r], sem.at[len(copies)]))
    for copy in copies:
        copy.start()
    for copy in copies:
        copy.wait()


def per_device_kernel(n, tokens, cotangent, gate_weight, up_weight, down_weight):
    rows, depth = tokens.shape
    shard, ff = gate_weight.shape
    chunks = ff // LANES
    parts = next(p for p in (3, 2, 1) if shard % (p * SUB) == 0)
    piece = shard // parts
    vmem, dma = pltpu.VMEM, pltpu.SemaphoreType.DMA
    dx, dg = pl.pallas_call(
        functools.partial(kernel, n),
        out_shape=(vmem((depth, rows), BF16), vmem((shard, ff), F32)),
        in_specs=[pl.BlockSpec(memory_space=pltpu.HBM)] * 5,
        out_specs=[pl.BlockSpec(memory_space=vmem)] * 2,
        scratch_shapes=[
            vmem((depth, rows), BF16), vmem((depth, rows), BF16),
            vmem((shard, ff), BF16), vmem((shard, ff), BF16), vmem((shard, ff), BF16),
            vmem((depth, 3 * ff), BF16),
            vmem((2, rows, depth), BF16), vmem((2, rows, depth), BF16),
            vmem((depth, rows), BF16), vmem((depth, rows), BF16),
            vmem((depth, rows), BF16), vmem((depth, rows), BF16),
            vmem((2, depth, rows), F32),
            vmem((3, rows, ff), BF16),
            vmem((2, shard, ff), F32), vmem((2, shard, ff), BF16),
            vmem((2, shard, ff), BF16), vmem((shard, ff), BF16), vmem((shard, LANES), BF16),
            vmem((2, 2, 2, shard, rows // 2), BF16), vmem((2, 2, 2, shard, rows // 2), BF16),
            vmem((2, 2, parts, piece, rows // 2), BF16), vmem((2, 2, parts, piece, rows // 2), BF16),
            vmem((parts, piece, rows), BF16), vmem((parts, piece, rows), BF16),
            vmem((3, parts, piece, rows // 2), BF16), vmem((parts, 2, 3, piece, rows // 2), BF16),
            vmem((parts, piece, rows), F32),
            vmem((9 * shard, rows), BF16),
            dma((11,)), dma((chunks, 3, 3)), dma((18,)), dma((2, chunks)), dma((chunks,)), dma((chunks,)), dma((1,)),
            dma((2, 2)), dma((2, parts)), dma((parts,)), dma((parts,)), dma((parts,)),
            dma((parts,)), dma((3,)),
        ],
        compiler_params=pltpu.CompilerParams(
            collective_id=0, has_side_effects=True, vmem_limit_bytes=40 * 2**20),
    )(*(pltpu.with_memory_space_constraint(a, pltpu.HBM) for a in (
        tokens.T, cotangent.T, gate_weight, up_weight, down_weight.T)))
    dx, dg = pl.pallas_call(
        store_kernel,
        out_shape=(pltpu.HBM((depth, rows), BF16), pltpu.HBM((shard, ff), F32)),
        in_specs=[pl.BlockSpec(memory_space=pl.ANY)] * 2,
        out_specs=[pl.BlockSpec(memory_space=pl.ANY)] * 2,
        scratch_shapes=[dma((6,))],
        compiler_params=pltpu.CompilerParams(vmem_limit_bytes=2**20),
    )(dx, dg)
    return dx.T, dg.T


def solution(mesh):
    n, tp = mesh.shape["fs"], mesh.shape["tp"]

    def per_device(tokens, cotangent, gate_weight, up_weight, down_weight):
        rows, depth = tokens.shape
        shard, ff = gate_weight.shape
        args = (tokens, cotangent, gate_weight, up_weight, down_weight)
        fits = (tp == 8 and n == 4 and rows % (2 * LANES) == 0 and rows <= 256
                and depth == n * shard and shard % SUB == 0 and ff % LANES == 0
                and shard % 48 == 0 and LANES < ff <= 512 and depth <= 2048)
        return per_device_kernel(n, *args) if fits else per_device_plain(*args)

    placed = (P("fs", None), P("fs", None), P("fs", "tp"), P("fs", "tp"), P("tp", "fs"))
    return jax.shard_map(
        per_device,
        mesh=mesh,
        in_specs=placed,
        out_specs=(P("fs", None), P("tp", "fs")),
        check_vma=False,
    )
```
